32 devices in a mesh: sp: 8 (over z, x), tp: 4 (over y, core).
Axes of the slice: x: 2, y: 2, z: 4, core: 2. Of those that a mesh axis runs over, the one named last changes fastest.
Arguments:
- residual: bfloat16 [3072, 2048], P('sp', 'tp'), may hold values from -6 to 6
- query_nope: bfloat16 [3072, 4096], P('sp', 'tp'), may hold values from -9 to 9
- query_rope: bfloat16 [3072, 2048], P('sp', 'tp'), may hold values from -600 to 600
- latent: bfloat16 [3072, 512], P('sp'), may hold values from -6 to 6
- rope_key: bfloat16 [3072, 64], P('sp'), may hold values from -6 to 6
- doc_ids: int32 [3072], P('sp'), may hold values from 0 to 3, never falling along the last dimension, each value on 1 to 1152 neighbouring positions
- key_up: bfloat16 [512, 4096], P(None, 'tp'), may hold values from -0.25 to 0.25
- value_up: bfloat16 [512, 4096], P(None, 'tp'), may hold values from -0.25 to 0.25
- out_proj: bfloat16 [4096, 2048], P('tp'), may hold values from -0.375 to 0.375
- norm1_gain: bfloat16 [2048], P('tp'), may hold values from 0.099609375 to 1.8984375
- norm1_bias: bfloat16 [2048], P('tp'), may hold values from -3 to 3
- ffn_gate: bfloat16 [2048, 5632], P('sp', 'tp'), may hold values from -0.125 to 0.125
- ffn_value: bfloat16 [2048, 5632], P('sp', 'tp'), may hold values from -0.125 to 0.125
- conv_gate: bfloat16 [3, 5632], P(None, 'tp'), may hold values from -3.5 to 3.5
- conv_value: bfloat16 [3, 5632], P(None, 'tp'), may hold values from -3.5 to 3.5
- ffn_down: bfloat16 [5632, 2048], P('tp', 'sp'), may hold values from -0.15625 to 0.15625
- norm2_gain: bfloat16 [2048], P('tp'), may hold values from 0.099609375 to 1.8984375
- norm2_bias: bfloat16 [2048], P('tp'), may hold values from -3 to 3
Outputs:
- layer_out: bfloat16 [3072, 2048], P('sp', 'tp')
The draws below stay inside these ranges and needn't reach their ends.
Inputs may be any that keep to these rules, and one draw needn't show every extreme that they name: `doc_ids`: document numbers never fall along the positions; each document holds 1 to 1152 positions, and one holds exactly 1152.
All inputs are finite; a program needn't handle non-finite values.
Results may differ from the reference program's by a relative error of at most 0.014.
Values may be sent and summed in bfloat16 or wider, within the bound.
A program may use at most 128 MiB of HBM per device.

```python
import math
import jax
import jax.numpy as jnp
import numpy as np
from jax import lax

D = 2048
HEADS = 32
NOPE = 128
ROPE = 64
VDIM = 128
LATENT = 512
FF = 5632
CONV = 3
REACH = 3
TOK_DEV = 384
TOKENS = 3072
DOCS = 4
N_SP = 8
N_TP = 4


def rope_base(key):
    base_rows = jnp.clip(jax.random.normal(jax.random.fold_in(key, 7), (TOKENS, ROPE), jnp.float32), -6.0, 6.0)
    return base_rows


def draw_rope_key(key, part):
    return rope_base(key).astype(jnp.bfloat16)


def draw_query_rope(key, part):
    drawn = jnp.clip(jax.random.normal(jax.random.fold_in(key, 9), (TOKENS, HEADS * ROPE), jnp.float32), -6.0, 6.0) * 1.5
    return drawn.astype(jnp.bfloat16)


def shard_levels(own_key, extent, cuts, low, largest):
    gain = 1.0
    for dim, shards_of in cuts:
        draws = jax.random.uniform(jax.random.fold_in(jax.random.fold_in(own_key, 6), dim), (shards_of,), jnp.float32, low / len(cuts), largest / len(cuts))
        gain = gain * jnp.repeat(jnp.exp(draws), extent[dim] // shards_of).reshape((-1,) + (1,) * (len(extent) - 1 - dim))
    return gain


def profile(number_of, total, most, lean):
    loads = [(1 << 20) // math.isqrt(rank ** lean) + 1 for rank in range(2, number_of + 1)]
    spare, counts = total - most - (number_of - 1), [1] * (number_of - 1)
    while spare > 0:
        candidates = [i for i in range(number_of - 1) if counts[i] < most]
        whole, remaining = sum([loads[i] for i in candidates]), spare
        for i in candidates:
            extra = min(most - counts[i], max(1, remaining * loads[i] // whole), spare)
            counts[i] = counts[i] + extra
            spare = spare - extra
    return np.array([most] + counts)


def ragged_sizes(own_key, count, total, most, skew):
    if count == 2:
        one = jax.random.randint(own_key, (), max(1, total - most), min(most, total - 1) + 1)
        return jnp.stack([one, total - one])
    lengths = jnp.asarray(profile(count, total, most, skew), jnp.int32)
    pairs = (count - 1) // 2
    donor, sink = lengths[1:1 + 2 * pairs:2], lengths[2:2 + 2 * pairs:2]
    room = jnp.minimum(donor - 1, most - sink)
    shifted = jax.random.randint(jax.random.fold_in(own_key, 1), (pairs,), 0, 1 << 20) % (room + 1)
    lengths = lengths.at[1:1 + 2 * pairs:2].set(donor - shifted).at[2:2 + 2 * pairs:2].set(sink + shifted)
    return lengths[jax.random.permutation(jax.random.fold_in(own_key, 2), count)]


def noise(own_key, dims, scale, bound, split=(), kind=jnp.bfloat16):
    gain = shard_levels(own_key, dims, split, -0.22, 0.18) if split else 1.0
    values = jax.random.normal(own_key, dims, jnp.float32) * scale * gain
    return jnp.minimum(jnp.maximum(values, -bound), bound).astype(kind)


def setup_inputs(seed: int = 0) -> dict:
    key_of = jax.random.split(jax.random.key(seed), 19)
    residual = noise(key_of[0], (TOKENS, D), 1.0, 6.0, ((0, 8), (1, 4)))
    query_nope = noise(key_of[1], (TOKENS, HEADS * NOPE), 1.5, 9.0, ((0, 8), (1, 4)))
    query_rope = draw_query_rope(jax.random.fold_in(key_of[18], 71), 0)
    latent = noise(key_of[3], (TOKENS, LATENT), 1.0, 6.0, ((0, 8),))
    rope_key = draw_rope_key(jax.random.fold_in(key_of[18], 71), 0)
    doc_ids = jnp.searchsorted(jnp.cumsum(ragged_sizes(key_of[5], DOCS, TOKENS, REACH * TOK_DEV, 1)), jnp.arange(TOKENS), side="right").astype(jnp.int32)
    key_up = noise(key_of[6], (LATENT, HEADS * NOPE), LATENT ** -0.5, 0.25, ((1, 4),))
    value_up = noise(key_of[7], (LATENT, HEADS * VDIM), LATENT ** -0.5, 0.25, ((1, 4),))
    out_proj = noise(key_of[8], (HEADS * VDIM, D), (HEADS * VDIM // 16) ** -0.5, 0.375, ((0, 4),))
    norm1_gain = jnp.clip(1.0 + 0.18 * jax.random.normal(key_of[9], (D,), jnp.float32), 0.099609375, 1.8984375).astype(jnp.bfloat16)
    norm1_bias = noise(key_of[10], (D,), 0.5, 3.0, ((0, 4),))
    ffn_gate = noise(key_of[11], (D, FF), D ** -0.5, 0.125, ((0, 8), (1, 4)))
    ffn_value = noise(key_of[12], (D, FF), D ** -0.5, 0.125, ((0, 8), (1, 4)))
    conv_gate = noise(key_of[13], (CONV, FF), CONV ** -0.5, 3.5, ((1, 4),))
    conv_value = noise(key_of[14], (CONV, FF), CONV ** -0.5, 3.5, ((1, 4),))
    ffn_down = noise(key_of[15], (FF, D), (FF // 4) ** -0.5, 0.15625, ((0, 4), (1, 8)))
    norm2_gain = jnp.clip(1.0 + 0.18 * jax.random.normal(key_of[16], (D,), jnp.float32), 0.099609375, 1.8984375).astype(jnp.bfloat16)
    norm2_bias = noise(key_of[17], (D,), 0.5, 3.0, ((0, 4),))
    return dict(residual=residual, query_nope=query_nope, query_rope=query_rope, latent=latent, rope_key=rope_key, doc_ids=doc_ids, key_up=key_up, value_up=value_up, out_proj=out_proj, norm1_gain=norm1_gain, norm1_bias=norm1_bias, ffn_gate=ffn_gate, ffn_value=ffn_value, conv_gate=conv_gate, conv_value=conv_value, ffn_down=ffn_down, norm2_gain=norm2_gain, norm2_bias=norm2_bias)


norm_eps = 1e-05
residual_scale = 8.0 ** 0.25
rope_base_freq = 10000.0
masked_score = -1e+30

def tables(positions):
    frequencies = 1.0 / rope_base_freq ** (jnp.arange(0, ROPE, 2, dtype=jnp.float32) / ROPE)
    angles = positions.astype(jnp.float32)[:, None] * frequencies[None, :]
    return (jnp.cos(angles), jnp.sin(angles))

def rotate(vectors, cosine, sine_table):
    half_width = vectors.shape[-1] // 2
    front_half = vectors[..., :half_width]
    back_half = vectors[..., half_width:]
    return jnp.concatenate([front_half * cosine - back_half * sine_table, front_half * sine_table + back_half * cosine], axis=-1)

def layer_norm(mixed, gain_row, bias_row):
    width = mixed.shape[-1]
    row_mean = lax.optimization_barrier(jnp.sum(mixed, -1, keepdims=True)) / width
    row_power = lax.optimization_barrier(jnp.sum(mixed * mixed, -1, keepdims=True)) / width
    return (mixed - row_mean) * lax.rsqrt(row_power - row_mean * row_mean + norm_eps) * gain_row.astype(jnp.float32) + bias_row.astype(jnp.float32)

def reference(residual, query_nope, query_rope, latent, rope_key, doc_ids, key_up, value_up, out_proj, norm1_gain, norm1_bias, ffn_gate, ffn_value, conv_gate, conv_value, ffn_down, norm2_gain, norm2_bias):
    row_count = TOK_DEV
    window = (REACH + 1) * row_count
    lead_rows = REACH * row_count
    rim_rows = CONV - 1
    positions = jnp.arange(TOKENS, dtype=jnp.int32)
    cosine, sine_table = tables(positions)
    turned_key = rotate(rope_key.astype(jnp.float32), cosine, sine_table).astype(jnp.bfloat16)
    turned_query = rotate(query_rope.astype(jnp.float32).reshape(TOKENS, HEADS, ROPE), cosine[:, None], sine_table[:, None]).astype(jnp.bfloat16)
    padded_latent = jnp.concatenate([jnp.zeros((lead_rows, LATENT), jnp.bfloat16), latent], 0)
    padded_key = jnp.concatenate([jnp.zeros((lead_rows, ROPE), jnp.bfloat16), turned_key], 0)
    padded_doc = jnp.concatenate([jnp.full((lead_rows,), -1, jnp.int32), doc_ids], 0)
    head_group = HEADS * VDIM // N_TP
    scale = (NOPE + ROPE) ** (-0.5)

    def first_half(block_index):
        row_start = (block_index * row_count).astype(jnp.int32)
        own_pos = row_start + jnp.arange(row_count, dtype=jnp.int32)
        win_latent = lax.dynamic_slice_in_dim(padded_latent, row_start, window, 0)
        win_key = lax.dynamic_slice_in_dim(padded_key, row_start, window, 0)
        win_doc = lax.dynamic_slice_in_dim(padded_doc, row_start, window, 0)
        own_doc = lax.dynamic_slice_in_dim(doc_ids, row_start, row_count, 0)
        key_pos = row_start - lead_rows + jnp.arange(window, dtype=jnp.int32)
        allowed = (key_pos[None, :] <= own_pos[:, None]) & (key_pos[None, :] >= 0) & (win_doc[None, :] == own_doc[:, None])
        key_rows = jnp.dot(win_latent, key_up, preferred_element_type=jnp.float32).astype(jnp.bfloat16).reshape(window, HEADS, NOPE)
        values = jnp.dot(win_latent, value_up, preferred_element_type=jnp.float32).astype(jnp.bfloat16).reshape(window, HEADS, VDIM)
        queries = lax.dynamic_slice_in_dim(query_nope, row_start, row_count, 0).reshape(row_count, HEADS, NOPE)
        turned = lax.dynamic_slice_in_dim(turned_query, row_start, row_count, 0)
        scores = jnp.einsum('qhd,khd->hqk', queries.astype(jnp.float32), key_rows.astype(jnp.float32))
        scores = scores + jnp.einsum('qhr,kr->hqk', turned.astype(jnp.float32), win_key.astype(jnp.float32))
        scores = jnp.where(allowed[None], scores * scale, masked_score)
        row_max = lax.optimization_barrier(jnp.max(scores, -1, keepdims=True))
        weights = jnp.exp(scores - row_max)
        weights = (weights / lax.optimization_barrier(jnp.sum(weights, -1, keepdims=True))).astype(jnp.bfloat16)
        attended = jnp.einsum('hqk,khd->qhd', weights.astype(jnp.float32), values.astype(jnp.float32)).astype(jnp.bfloat16).reshape(row_count, HEADS * VDIM)
        projected = jnp.zeros((row_count, D), jnp.float32)
        for member in range(N_TP):
            partial_value = jnp.dot(attended[:, member * head_group:(member + 1) * head_group], out_proj[member * head_group:(member + 1) * head_group], preferred_element_type=jnp.float32).astype(jnp.bfloat16)
            projected = projected + lax.optimization_barrier(partial_value).astype(jnp.float32)
        mixed = residual_scale * lax.dynamic_slice_in_dim(residual, row_start, row_count, 0).astype(jnp.float32) + projected
        return layer_norm(mixed, norm1_gain, norm1_bias).astype(jnp.bfloat16)
    normed = lax.map(first_half, jnp.arange(N_SP, dtype=jnp.int32)).reshape(TOKENS, D)
    padded_normed = jnp.concatenate([jnp.zeros((rim_rows, D), jnp.bfloat16), normed], 0)
    padded_doc_two = jnp.concatenate([jnp.full((rim_rows,), -1, jnp.int32), doc_ids], 0)
    unit_group = FF // N_TP

    def second_half(block_index):
        row_start = (block_index * row_count).astype(jnp.int32)
        own_pos = row_start + jnp.arange(row_count, dtype=jnp.int32)
        block_rows = lax.dynamic_slice_in_dim(padded_normed, row_start, row_count + rim_rows, 0)
        block_doc = lax.dynamic_slice_in_dim(padded_doc_two, row_start, row_count + rim_rows, 0)
        own_doc = block_doc[rim_rows:]
        gate_pre = jnp.dot(block_rows, ffn_gate, preferred_element_type=jnp.float32).astype(jnp.bfloat16)
        value_pre = jnp.dot(block_rows, ffn_value, preferred_element_type=jnp.float32).astype(jnp.bfloat16)
        gate_mix = jnp.zeros((row_count, FF), jnp.float32)
        value_mix = jnp.zeros((row_count, FF), jnp.float32)
        for tap_index in range(CONV):
            valid_tap = ((block_doc[tap_index:tap_index + row_count] == own_doc) & (own_pos - rim_rows + tap_index >= 0)).astype(jnp.float32)[:, None]
            gate_mix = gate_mix + conv_gate[tap_index].astype(jnp.float32) * gate_pre[tap_index:tap_index + row_count].astype(jnp.float32) * valid_tap
            value_mix = value_mix + conv_value[tap_index].astype(jnp.float32) * value_pre[tap_index:tap_index + row_count].astype(jnp.float32) * valid_tap
        hidden = (value_mix * jax.nn.gelu(gate_mix)).astype(jnp.bfloat16)
        ffn_out = jnp.zeros((row_count, D), jnp.float32)
        for member in range(N_TP):
            partial_value = jnp.dot(hidden[:, member * unit_group:(member + 1) * unit_group], ffn_down[member * unit_group:(member + 1) * unit_group], preferred_element_type=jnp.float32).astype(jnp.bfloat16)
            ffn_out = ffn_out + lax.optimization_barrier(partial_value).astype(jnp.float32)
        mixed = residual_scale * block_rows[rim_rows:].astype(jnp.float32) + ffn_out
        return layer_norm(mixed, norm2_gain, norm2_bias).astype(jnp.bfloat16)
    return lax.map(second_half, jnp.arange(N_SP, dtype=jnp.int32)).reshape(TOKENS, D)
```

```python
import functools

import jax
import jax.numpy as jnp
from jax import lax
from jax.experimental import pallas as pl
from jax.experimental.pallas import tpu as pltpu
from jax.sharding import PartitionSpec as P

D = 2048
NOPE = 128
ROPE = 64
VDIM = 128
CONV = 3
REACH = 3


norm_eps = 1e-05
residual_scale = 8.0**0.25
rope_base_freq = 10000.0
masked_score = -1e30


def passed_along(value, axis, by):
    count = lax.axis_size(axis)
    pairs = [(i, i + by) for i in range(count) if 0 <= i + by < count]
    return lax.ppermute(value, axis, pairs)


def tables(positions):
    frequencies = 1.0 / rope_base_freq ** (jnp.arange(0, ROPE, 2, dtype=jnp.float32) / ROPE)
    angles = positions.astype(jnp.float32)[:, None] * frequencies[None, :]
    return (jnp.cos(angles), jnp.sin(angles))


def rotate(vectors, cosine, sine_table):
    half_width = vectors.shape[-1] // 2
    front_half = vectors[..., :half_width]
    back_half = vectors[..., half_width:]
    return jnp.concatenate(
        [
            front_half * cosine - back_half * sine_table,
            front_half * sine_table + back_half * cosine,
        ],
        axis=-1,
    )


def ring_blocks(block, axis):
    count = lax.axis_size(axis)
    order = list(range(0, count, 2)) + list(range(1, count, 2))[::-1]
    place = [order.index(i) for i in range(count)]
    me = lax.axis_index(axis)
    found = [(me, block)]
    ahead = count // 2
    for turn, steps in ((1, ahead), (-1, count - 1 - ahead)):
        pairs = [(order[p], order[(p + turn) % count]) for p in range(count)]
        moving = block
        for step in range(1, steps + 1):
            moving = lax.ppermute(moving, axis, pairs)
            owners = [order[(place[i] - turn * step) % count] for i in range(count)]
            found.append((jnp.asarray(owners, jnp.int32)[me], moving))
    return found


def attend_kernel(chunk, reach_rows, scale, q_ref, turned_ref, k_ref, rope_ref, v_ref, bias_ref, out_ref):
    rows = q_ref.shape[0]
    span = chunk + reach_rows
    rope_rows = rope_ref[...]
    for head in range(q_ref.shape[1] // NOPE):
        nope = slice(head * NOPE, (head + 1) * NOPE)
        rope = slice(head * ROPE, (head + 1) * ROPE)
        queries = jnp.concatenate([q_ref[:, nope], turned_ref[:, rope]], 1)
        keys = jnp.concatenate([k_ref[:, nope], rope_rows], 1)
        for start in range(0, rows, chunk):
            cut = slice(start, start + chunk)
            seen = slice(start, start + span)
            scores = lax.dot_general(
                queries[cut], keys[seen], (((1,), (1,)), ((), ())), preferred_element_type=jnp.float32
            )
            scores = scores * scale + bias_ref[cut, seen]
            weights = jnp.exp(scores - jnp.max(scores, -1, keepdims=True))
            weights = weights * (1.0 / jnp.sum(weights, -1, keepdims=True))
            out_ref[cut, nope] = jnp.dot(
                weights.astype(jnp.bfloat16), v_ref[seen, nope], preferred_element_type=jnp.float32
            ).astype(jnp.bfloat16)


def attend(queries, turned, keys, rope_rows, values, bias, scale):
    rows, width = queries.shape
    window = keys.shape[0]
    chunk = 128 if rows % 128 == 0 else rows
    pair = 2
    wide = pair * NOPE
    heads = width // NOPE
    return pl.pallas_call(
        functools.partial(attend_kernel, chunk, window - rows, scale),
        grid=(heads // pair,),
        in_specs=[
            pl.BlockSpec((rows, wide), lambda i: (0, i)),
            pl.BlockSpec((rows, pair * ROPE), lambda i: (0, i)),
            pl.BlockSpec((window, wide), lambda i: (0, i)),
            pl.BlockSpec((window, ROPE), lambda i: (0, 0)),
            pl.BlockSpec((window, pair * VDIM), lambda i: (0, i)),
            pl.BlockSpec((rows, window), lambda i: (0, 0)),
        ],
        out_specs=pl.BlockSpec((rows, pair * VDIM), lambda i: (0, i)),
        out_shape=jax.ShapeDtypeStruct((rows, heads * VDIM), jnp.bfloat16),
        compiler_params=pltpu.CompilerParams(vmem_limit_bytes=40 * 1024 * 1024),
        cost_estimate=pl.CostEstimate(
            flops=16 * rows * window * heads * (NOPE + ROPE + VDIM),
            bytes_accessed=2 * (4 * rows * width + 2 * window * width),
            transcendentals=rows * window * heads,
        ),
    )(queries, turned, keys, rope_rows, values, bias)


def scatter_sum(terms, axis):
    count = lax.axis_size(axis)
    width = terms.shape[1] // count
    parts = jnp.stack([terms[:, i * width : (i + 1) * width] for i in range(count)])
    got = lax.all_to_all(parts.astype(jnp.bfloat16), axis, 0, 0)
    return jnp.sum(got.astype(jnp.float32), 0)


def finish(mixed, totals, gain_row, bias_row):
    row_mean = totals[0][:, None] / D
    row_power = totals[1][:, None] / D
    return (mixed - row_mean) * lax.rsqrt(
        row_power - row_mean * row_mean + norm_eps
    ) * gain_row.astype(jnp.float32) + bias_row.astype(jnp.float32)


def plain(
    residual,
    query_nope,
    query_rope,
    latent,
    rope_key,
    doc_ids,
    key_up,
    value_up,
    out_proj,
    norm1_gain,
    norm1_bias,
    ffn_gate,
    ffn_value,
    conv_gate,
    conv_value,
    ffn_down,
    norm2_gain,
    norm2_bias,
):
    row_count = latent.shape[0]
    head_count = query_nope.shape[1] // NOPE
    local_units = ffn_gate.shape[1]
    rim_rows = CONV - 1
    whole_gate = lax.all_gather(ffn_gate, "sp", axis=0, tiled=True)
    whole_value = lax.all_gather(ffn_value, "sp", axis=0, tiled=True)
    offset = lax.axis_index("sp") * row_count
    positions = offset + jnp.arange(row_count, dtype=jnp.int32)
    cosine, sine_table = tables(positions)
    turned_key = rotate(rope_key.astype(jnp.float32), cosine, sine_table).astype(jnp.bfloat16)
    turned_query = rotate(
        query_rope.astype(jnp.float32).reshape(row_count, head_count, ROPE),
        cosine[:, None],
        sine_table[:, None],
    ).astype(jnp.bfloat16)
    latent_width = latent.shape[1]
    packed = jnp.concatenate(
        [
            latent,
            turned_key,
            jnp.broadcast_to(doc_ids.astype(jnp.bfloat16)[:, None], (row_count, ROPE)),
        ],
        1,
    )
    parts = [passed_along(packed, "sp", shift_step) for shift_step in range(REACH, 0, -1)]
    pieces = jnp.concatenate(parts + [packed], 0)
    win_latent = pieces[:, :latent_width]
    win_key = pieces[:, latent_width : latent_width + ROPE]
    win_doc = pieces[:, latent_width + ROPE].astype(jnp.int32)
    down_blocks = ring_blocks(ffn_down, "sp")
    key_rows = jnp.dot(win_latent, key_up, preferred_element_type=jnp.float32).astype(jnp.bfloat16)
    values = jnp.dot(win_latent, value_up, preferred_element_type=jnp.float32).astype(jnp.bfloat16)
    window = key_rows.shape[0]
    key_pos = offset - REACH * row_count + jnp.arange(window, dtype=jnp.int32)
    allowed = (
        (key_pos[None, :] <= positions[:, None])
        & (key_pos[None, :] >= 0)
        & (win_doc[None, :] == doc_ids[:, None])
    )
    scale = (NOPE + ROPE) ** (-0.5)
    bias = jnp.where(allowed, 0.0, masked_score).astype(jnp.float32)
    attended = attend(
        query_nope,
        turned_query.reshape(row_count, head_count * ROPE),
        key_rows,
        win_key,
        values,
        bias,
        scale,
    )
    head_terms = jnp.dot(attended, out_proj, preferred_element_type=jnp.float32)
    projected = scatter_sum(head_terms, "tp")
    mixed_one = residual_scale * residual.astype(jnp.float32) + projected
    totals_one = lax.psum((jnp.sum(mixed_one, 1), jnp.sum(mixed_one * mixed_one, 1)), "tp")
    normed = finish(mixed_one, totals_one, norm1_gain, norm1_bias).astype(jnp.bfloat16)
    half = row_count // 2
    full_rows = jnp.concatenate(
        [
            lax.all_gather(normed[:half], "tp", axis=1, tiled=True),
            lax.all_gather(normed[half:], "tp", axis=1, tiled=True),
        ],
        0,
    )
    gate_sum = jnp.dot(full_rows, whole_gate, preferred_element_type=jnp.float32)
    value_sum = jnp.dot(full_rows, whole_value, preferred_element_type=jnp.float32)
    gate_pre = gate_sum.astype(jnp.bfloat16)
    value_pre = value_sum.astype(jnp.bfloat16)
    tail_gate, tail_value, tail_doc = passed_along(
        (
            gate_pre[row_count - rim_rows :],
            value_pre[row_count - rim_rows :],
            doc_ids[row_count - rim_rows :],
        ),
        "sp",
        1,
    )
    ext_gate = jnp.concatenate([tail_gate, gate_pre], 0)
    ext_value = jnp.concatenate([tail_value, value_pre], 0)
    ext_doc = jnp.concatenate([tail_doc, doc_ids], 0)
    gate_mix = jnp.zeros((row_count, local_units), jnp.float32)
    value_mix = jnp.zeros((row_count, local_units), jnp.float32)
    for tap_index in range(CONV):
        valid_tap = (
            (ext_doc[tap_index : tap_index + row_count] == doc_ids)
            & (positions - rim_rows + tap_index >= 0)
        ).astype(jnp.float32)[:, None]
        gate_mix = (
            gate_mix
            + conv_gate[tap_index].astype(jnp.float32)
            * ext_gate[tap_index : tap_index + row_count].astype(jnp.float32)
            * valid_tap
        )
        value_mix = (
            value_mix
            + conv_value[tap_index].astype(jnp.float32)
            * ext_value[tap_index : tap_index + row_count].astype(jnp.float32)
            * valid_tap
        )
    hidden = (value_mix * jax.nn.gelu(gate_mix)).astype(jnp.bfloat16)
    sp_count = lax.axis_size("sp")
    tp_count = lax.axis_size("tp")
    block_width = ffn_down.shape[1]
    unit_terms = jnp.zeros((sp_count, row_count, block_width), jnp.bfloat16)
    for owner, block in down_blocks:
        term = jnp.dot(hidden, block, preferred_element_type=jnp.float32).astype(jnp.bfloat16)
        unit_terms = lax.dynamic_update_slice(unit_terms, term[None], (owner, 0, 0))
    share = sp_count // tp_count
    got = lax.all_to_all(
        unit_terms.reshape(tp_count, share, row_count, block_width), "tp", 0, 0
    )
    ffn_blocks = jnp.sum(got.astype(jnp.float32), 0)
    ffn_out = jnp.concatenate([ffn_blocks[i] for i in range(share)], 1)
    mixed_two = residual_scale * normed.astype(jnp.float32) + ffn_out
    totals_two = lax.psum((jnp.sum(mixed_two, 1), jnp.sum(mixed_two * mixed_two, 1)), "tp")
    return finish(mixed_two, totals_two, norm2_gain, norm2_bias).astype(jnp.bfloat16)


LANES = 128
MESH = pl.DeviceIdType.MESH
log2_e = 1.4426950408889634


class Copies:
    def __init__(self, send_sems, recv_sems):
        self.send_sems, self.recv_sems = send_sems, recv_sems
        self.count = 0

    def ids(self, number=1):
        first = self.count
        self.count += number
        return first

    def make(self, index, source, target, sp, tp):
        return pltpu.make_async_remote_copy(
            src_ref=source,
            dst_ref=target,
            send_sem=self.send_sems.at[index],
            recv_sem=self.recv_sems.at[index],
            device_id={"sp": sp, "tp": tp},
            device_id_type=MESH,
        )


REMOTE = 160
LOCAL = 16


def flip(value, bits):
    for bit in range(bits.bit_length()):
        step = 1 << bit
        if bits & step:
            value = value + step - 2 * step * ((value // step) % 2)
    return value


def layer_kernel(
    sizes,
    q_in, t_in, pack_in, kup_in, vup_in, proj_in, resid_in, gains, taps, gate_in, value_in, down_in,
    out_ref,
    win, q_v, t_v, kup, vup, proj, resid, keys, vals, ropes, bias, att,
    core_out, core_in, keep, y_out, y_in, mix, stat_own, stat_in, valid,
    rows_all, gate_w, value_w, down_w, ext, hid,
    core_out2, core_in2, keep2, y_out2, y_in2, z_out2, z_in2, stat_own2, stat_in2,
    send_sems, recv_sems, local_sems,
):
    n_sp, n_tp, R, reach, heads, wide, first, second = sizes
    C = LANES
    F = resid.shape[1]
    chunks = R // C
    window = (reach + 1) * R
    span = C + reach * R
    latent_width = kup.shape[0]
    gate_rows = gate_in.shape[0]
    down_cols = down_in.shape[1]
    bf16, f32 = jnp.bfloat16, jnp.float32
    me_sp, me_tp = lax.axis_index("sp"), lax.axis_index("tp")
    x, z = me_sp % 2, me_sp // 2
    odd = z % 2
    y, c = me_tp // 2, me_tp % 2
    x_peer = me_sp + 1 - 2 * x
    c_peer = me_tp + 1 - 2 * c
    y_peer = me_tp + 2 - 4 * y
    far_peer = 3 - me_tp
    nz = n_sp // 2
    z_sp = [2 * flip(z, d) + x for d in range(nz)]
    pair = z_sp[1]
    rc = Copies(send_sems, recv_sems)
    sent = []

    def start(copy, when=None):
        if when is None:
            copy.start()
        else:
            pl.when(when)(copy.start)
        sent.append((copy, when))

    barrier = pltpu.get_barrier_semaphore()
    for i in range(n_sp):
        for j in range(n_tp):
            if i or j:
                pl.semaphore_signal(
                    barrier, inc=1,
                    device_id={"sp": (me_sp + i) % n_sp, "tp": (me_tp + j) % n_tp},
                    device_id_type=MESH,
                )

    loads = {}

    def load(name, source, target):
        loads[name] = pltpu.make_async_copy(source, target, local_sems.at[len(loads)])
        loads[name].start()

    load("win", pack_in, win.at[pl.ds(reach * R, R)])
    load("kup", kup_in, kup)
    load("vup", vup_in, vup)
    load("q", q_in, q_v)
    load("t", t_in, t_v)
    load("proj", proj_in, proj)
    load("resid", resid_in, resid)

    pl.semaphore_wait(barrier, n_sp * n_tp - 1)

    half = R // 2
    halo, halo_core = rc.ids(reach), rc.ids(reach)

    def halo_copy(k):
        return rc.make(
            halo + k - 1,
            pack_in.at[pl.ds(c * half, half)],
            win.at[pl.ds((reach - k) * R + c * half, half)],
            me_sp + k, me_tp,
        )

    def halo_pass(k, core):
        rows = win.at[pl.ds((reach - k) * R + core * half, half)]
        return rc.make(halo_core + k - 1, rows, rows, me_sp, c_peer)

    for k in range(1, reach + 1):
        start(halo_copy(k), me_sp + k < n_sp)

    halves = ((0, first), (first, second))

    def half_in(w, parity):
        at, size = halves[parity]
        if w == 2:
            return down_in.at[pl.ds(at, size), :]
        return (gate_in, value_in)[w].at[:, pl.ds(at, size)]

    def half_slot(w, parity, owner):
        size = halves[parity][1]
        if w == 2:
            return down_w.at[owner, pl.ds(0, size), :]
        rows = pl.ds(pl.multiple_of(owner * gate_rows, 16), gate_rows)
        return (gate_w, value_w)[w].at[rows, pl.ds(0, size)]

    def by_parity(parity, act):
        for p in range(2):
            pl.when(parity == p)(functools.partial(act, p))

    z_ids = [rc.ids(nz) for _ in range(3)]
    x_ids = [rc.ids(nz) for _ in range(3)]
    own_ids = [len(loads) + w for w in range(3)]

    def own_weight(w, p):
        return pltpu.make_async_copy(half_in(w, p), half_slot(w, p, me_sp), local_sems.at[own_ids[w]])

    def z_weight(w, d, p):
        return rc.make(z_ids[w] + d, half_in(w, p), half_slot(w, p, me_sp), z_sp[d], me_tp)

    def z_landed(w, d, p):
        return rc.make(z_ids[w] + d, half_in(w, p), half_slot(w, p, z_sp[d]), z_sp[d], me_tp)

    def x_weight(w, d, p):
        source = half_in(w, p) if d == 0 else half_slot(w, p, z_sp[d])
        return rc.make(x_ids[w] + d, source, half_slot(w, p, z_sp[d]), x_peer, me_tp)

    def x_landed(w, d, p):
        slot = half_slot(w, p, z_sp[d] + 1 - 2 * x)
        return rc.make(x_ids[w] + d, slot, slot, x_peer, me_tp)

    def send_z(w):
        for d in list(range(2, nz)) + [1]:
            by_parity((odd + d) % 2, lambda p, d=d: z_weight(w, d, p).start())

    def send_x(w, d):
        if d:
            by_parity(odd, lambda p: z_landed(w, d, p).wait_recv())
        by_parity(odd, lambda p: x_weight(w, d, p).start())

    def all_here(w):
        def act(p):
            own_weight(w, p).wait()
            for d in range(nz):
                x_landed(w, d, p).wait_recv()
        by_parity(odd, act)

    for w in range(3):
        by_parity(odd, lambda p, w=w: own_weight(w, p).start())
    send_x(0, 0)
    send_z(0)
    send_x(1, 0)

    @pl.when(odd == 1)
    def _():
        blank = first - second
        if blank:
            gate_w[:, second:] = jnp.zeros((gate_w.shape[0], blank), bf16)
            value_w[:, second:] = jnp.zeros((gate_w.shape[0], blank), bf16)
            down_w[:, second:, :] = jnp.zeros((n_sp, blank, down_cols), bf16)

    loads["win"].wait()
    loads["kup"].wait()
    loads["vup"].wait()

    def raise_rows(block):
        rows = pl.ds(pl.multiple_of(block * R, LANES), R)
        source = win[rows, :latent_width]
        keys[rows, :] = jnp.dot(source, kup[...], preferred_element_type=f32).astype(bf16)
        vals[rows, :] = jnp.dot(source, vup[...], preferred_element_type=f32).astype(bf16)

    raise_rows(reach)
    for k in range(1, reach + 1):
        @pl.when(me_sp >= k)
        def _(k=k):
            halo_copy(k).wait_recv()
            halo_pass(k, c).start()

        @pl.when(me_sp < k)
        def _(k=k):
            win[(reach - k) * R : (reach - k + 1) * R, :] = jnp.zeros((R, win.shape[1]), bf16)
        sent.append((halo_pass(k, c), me_sp >= k))
    for k in range(1, reach + 1):
        @pl.when(me_sp >= k)
        def _(k=k):
            halo_pass(k, 1 - c).wait_recv()

    @pl.loop(0, reach)
    def _(block):
        raise_rows(block)

    side = win[:, latent_width:]
    side_f = side.astype(f32)
    lane = lax.broadcasted_iota(jnp.int32, (window, LANES), 1)
    low = lane < LANES // 2
    ropes[0] = jnp.where(low, side_f, 0.0).astype(bf16)
    ropes[1] = jnp.where(low, 0.0, pltpu.roll(side_f, LANES // 2, 1)).astype(bf16)
    pick = (
        (lax.broadcasted_iota(jnp.int32, (8, LANES), 1) == LANES // 2)
        .astype(f32)
        .astype(bf16)
    )
    key_doc = lax.dot_general(pick, side, (((1,), (1,)), ((), ())), preferred_element_type=f32)[0:1]
    for r in range(chunks):
        at = slice(r * C, (r + 1) * C)
        own_doc = side_f[reach * R + r * C : reach * R + (r + 1) * C, LANES // 2 : LANES // 2 + 1]
        key_at = lax.broadcasted_iota(jnp.int32, (C, window), 1) - reach * R
        row_at = lax.broadcasted_iota(jnp.int32, (C, window), 0) + r * C
        allowed = (key_at <= row_at) & (key_at + me_sp * R >= 0) & (key_doc == own_doc)
        bias[at, :] = jnp.where(allowed, 0.0, masked_score)

    tail = side_f[reach * R - 8 :]
    valid_id = rc.ids()
    row_no = lax.broadcasted_iota(jnp.int32, (R, LANES), 0) + me_sp * R
    here = tail[8:]
    back_one = (pltpu.roll(tail, 1, 0)[8:] == here) & (row_no >= 1)
    back_two = (pltpu.roll(tail, 2, 0)[8:] == here) & (row_no >= 2)
    lanes = lax.broadcasted_iota(jnp.int32, (R, LANES), 1)
    valid[odd] = jnp.where(
        lanes < 3 * LANES // 4, back_two.astype(f32), back_one.astype(f32)
    ).astype(bf16)
    start(rc.make(valid_id, valid.at[odd], valid.at[odd], pair, me_tp))

    scale = (NOPE + ROPE) ** (-0.5) * log2_e

    def attend_chunk(r):
        at, seen = slice(r * C, (r + 1) * C), slice(r * C, r * C + span)

        @pl.loop(0, heads // 2)
        def _(duo):
            turned = t_v[at, pl.ds(pl.multiple_of(duo * LANES, LANES), LANES)]
            for e in range(2):
                head = pl.ds(pl.multiple_of((2 * duo + e) * LANES, LANES), LANES)
                queries = jnp.concatenate([q_v[at, head], turned], 1)
                seen_keys = jnp.concatenate([keys[seen, head], ropes[e, seen, :]], 1)
                scores = lax.dot_general(
                    queries, seen_keys, (((1,), (1,)), ((), ())), preferred_element_type=f32
                )
                scores = scores * scale + bias[at, seen]
                weights = jnp.exp2(scores - jnp.max(scores, -1, keepdims=True))
                total = jnp.sum(weights, -1, keepdims=True)
                mixed = jnp.dot(weights.astype(bf16), vals[seen, head], preferred_element_type=f32)
                att[at, head] = (mixed * (1.0 / total)).astype(bf16)

    core_ids, y_ids = rc.ids(2 * chunks), rc.ids(chunks)
    stat_ids = rc.ids(3 * chunks)
    stat_ids2 = rc.ids(3 * chunks)
    gather_ids = rc.ids(8 * chunks)

    def to_core(r, i):
        return rc.make(core_ids + 2 * r + i, core_out.at[r, i], core_in.at[r, i], me_sp, c_peer)

    def to_y(r):
        return rc.make(y_ids + r, y_out.at[r], y_in.at[r], me_sp, y_peer)

    def features(tp):
        return pl.ds(pl.multiple_of(tp * F, LANES), F)

    def project(r):
        rows = att[r * C : (r + 1) * C, :]
        for i, yy in enumerate((1 - y, y)):
            core_out[r, i] = jnp.dot(
                rows, proj[:, features(2 * yy + 1 - c)], preferred_element_type=f32
            ).astype(bf16)
            start(to_core(r, i))
        for i, yy in enumerate((1 - y, y)):
            keep[r, i] = jnp.dot(
                rows, proj[:, features(2 * yy + c)], preferred_element_type=f32
            ).astype(bf16)
        to_core(r, 0).wait_recv()
        y_out[r] = (keep[r, 0].astype(f32) + core_in[r, 0].astype(f32)).astype(bf16)
        start(to_y(r))

    def stat_copy(ids, own, landed, r, i):
        return rc.make(ids + 3 * r + i, own.at[r], landed.at[r, i], me_sp, (c_peer, y_peer, far_peer)[i])

    def send_stats(values, ids, own, landed, r):
        one = jnp.sum(values, -1, keepdims=True)
        two = jnp.sum(values * values, -1, keepdims=True)
        lane = lax.broadcasted_iota(jnp.int32, (C, LANES), 1)
        own[r] = jnp.where(lane % 8 < 4, one, two).T[0:8]
        for i in (1, 2, 0):
            start(stat_copy(ids, own, landed, r, i))

    def norm(values, ids, own, landed, r, gain):
        for i in range(3):
            stat_copy(ids, own, landed, r, i).wait_recv()
        total = (own[r] + landed[r, 0]) + (landed[r, 1] + landed[r, 2])
        total = jnp.concatenate([total] * (LANES // 8), 0).T
        row_mean = total[:, 0:1] / wide
        row_power = total[:, 4:5] / wide
        return (values - row_mean) * lax.rsqrt(row_power - row_mean * row_mean + norm_eps) * gains[
            gain : gain + 1, :
        ] + gains[gain + 1 : gain + 2, :]

    def mix_one(r):
        at = slice(r * C, (r + 1) * C)
        to_core(r, 1).wait_recv()
        to_y(r).wait_recv()
        mixed = residual_scale * resid[at, :].astype(f32) + (
            keep[r, 1].astype(f32) + core_in[r, 1].astype(f32) + y_in[r].astype(f32)
        )
        mix[at, :] = mixed
        send_stats(mixed, stat_ids, stat_own, stat_in, r)

    def gathered(r, kind, slot, tp, sp_to, tp_to):
        spot = rows_all.at[slot, pl.ds(r * C, C), features(tp)]
        return rc.make(gather_ids + 8 * r + kind, spot, spot, sp_to, tp_to)

    def to_pair(r, slot):
        return gathered(r, 0, slot, me_tp, pair, me_tp)

    def core_gather(r, kind, slot, tp):
        return gathered(r, kind, slot, tp, me_sp, c_peer)

    def y_gather(r, kind, slot, tp):
        return gathered(r, kind, slot, tp, me_sp, y_peer)

    def norm_one(r):
        at = slice(r * C, (r + 1) * C)
        rows_all[odd, at, features(me_tp)] = norm(
            mix[at, :], stat_ids, stat_own, stat_in, r, 0
        ).astype(bf16)
        start(to_pair(r, odd))
        start(y_gather(r, 1, odd, me_tp))
        start(core_gather(r, 2, odd, me_tp))

    def pass_pair(r):
        to_pair(r, 1 - odd).wait_recv()
        start(y_gather(r, 3, 1 - odd, me_tp))
        start(core_gather(r, 4, 1 - odd, me_tp))

    def pass_y(r):
        for kind, got, slot in ((5, 1, odd), (6, 3, 1 - odd)):
            y_gather(r, got, slot, y_peer).wait_recv()
            start(core_gather(r, kind, slot, y_peer))

    def rows_here(r):
        core_gather(r, 2, odd, c_peer).wait_recv()
        core_gather(r, 4, 1 - odd, c_peer).wait_recv()
        core_gather(r, 5, odd, far_peer).wait_recv()
        core_gather(r, 6, 1 - odd, far_peer).wait_recv()

    loads["q"].wait()
    loads["t"].wait()
    attend_chunk(0)
    loads["proj"].wait()
    loads["resid"].wait()
    project(0)
    for r in range(1, chunks):
        attend_chunk(r)
        mix_one(r - 1)
        project(r)
        norm_one(r - 1)
    mix_one(chunks - 1)
    norm_one(chunks - 1)
    for d in range(1, nz):
        send_x(0, d)
    send_z(1)
    send_z(2)
    send_x(2, 0)
    for r in range(chunks):
        pass_pair(r)
    for r in range(chunks):
        pass_y(r)
    for r in range(chunks):
        rows_here(r)

    tile = 2 * LANES
    mid = first

    def up(weights, base):
        @pl.loop(0, 2)
        def _(slot):
            @pl.loop(0, first // tile)
            def _(j):
                cols = pl.multiple_of(j * tile, LANES)
                ext[slot, 8:, pl.ds(base + cols, tile)] = (
                    jnp.dot(rows_all[slot], weights[:, pl.ds(cols, tile)], preferred_element_type=f32)
                    .astype(bf16)
                    .astype(f32)
                )

    all_here(0)
    up(gate_w, 0)
    for d in range(1, nz):
        send_x(1, d)
    all_here(1)
    up(value_w, mid)

    tail_ids = rc.ids(2)

    def tail_copy(slot, to_slot, sp):
        return rc.make(
            tail_ids + to_slot, ext.at[slot, pl.ds(R, 8)], ext.at[to_slot, pl.ds(0, 8)], sp, me_tp
        )

    last_pair = z >= nz - 2
    start(tail_copy(0, 0, x_peer), x == 0)
    start(tail_copy(1, 1, x_peer), x == 0)
    start(tail_copy(0, 1, x_peer), x == 1)
    start(tail_copy(1, 0, me_sp + 3), (x == 1) & (z < nz - 2))

    @pl.when((x == 0) & (z < 2))
    def _():
        ext[0, 0:8, :] = jnp.zeros((8, ext.shape[2]), f32)

    for d in range(1, nz):
        send_x(2, d)

    @pl.when((x == 1) | (z >= 2))
    def _():
        tail_copy(0, 0, x_peer).wait_recv()
    tail_copy(1, 1, x_peer).wait_recv()
    rc.make(valid_id, valid.at[1 - odd], valid.at[1 - odd], pair, me_tp).wait_recv()

    deep = 64

    @pl.loop(0, 2)
    def _(slot):
        @pl.loop(0, R // deep)
        def _(i):
            at = pl.multiple_of(i * deep, 16)
            marks = valid[slot, pl.ds(at, deep), :].astype(f32)
            two, one = marks[:, LANES // 2 : LANES // 2 + 1], marks[:, LANES - 1 : LANES]

            @pl.loop(0, first // tile)
            def _(j):
                cols = pl.multiple_of(j * tile, LANES)

                def mixing(base, tap):
                    rows = ext[slot, pl.ds(at, deep + 8), pl.ds(base + cols, tile)]
                    weight = taps[pl.ds(tap, 8), pl.ds(cols, tile)]
                    return (
                        weight[0:1] * (pltpu.roll(rows, 2, 0)[8:] * two)
                        + weight[1:2] * (pltpu.roll(rows, 1, 0)[8:] * one)
                        + weight[2:3] * rows[8:]
                    )

                hid[slot, pl.ds(at, deep), pl.ds(cols, tile)] = (
                    mixing(mid, 8) * jax.nn.gelu(mixing(0, 0))
                ).astype(bf16)

    all_here(2)

    core_ids2, y_ids2, z_id2 = rc.ids(4), rc.ids(2), rc.ids()
    per = F // down_cols

    def down(slot, tp, target):
        for j in range(per):
            target[:, j * down_cols : (j + 1) * down_cols] = jnp.dot(
                hid[slot], down_w[per * tp + j], preferred_element_type=f32
            ).astype(bf16)

    def to_core2(i, s):
        return rc.make(
            core_ids2 + 2 * i + s, core_out2.at[i, s], core_in2.at[i, s], me_sp, c_peer
        )

    def to_y2(s):
        return rc.make(y_ids2 + s, y_out2.at[s], y_in2.at[s], me_sp, y_peer)

    slots = (1 - odd, odd)
    for i, yy in enumerate((1 - y, y)):
        for s, slot in enumerate(slots):
            down(slot, 2 * yy + 1 - c, core_out2.at[i, s])
            start(to_core2(i, s))
            down(slot, 2 * yy + c, keep2.at[i, s])
            to_core2(i, s).wait_recv()
            if i == 0:
                y_out2[s] = (keep2[0, s].astype(f32) + core_in2[0, s].astype(f32)).astype(bf16)
                start(to_y2(s))
    to_y2(0).wait_recv()
    z_out2[...] = (
        keep2[1, 0].astype(f32) + core_in2[1, 0].astype(f32) + y_in2[0].astype(f32)
    ).astype(bf16)
    to_z2 = rc.make(z_id2, z_out2, z_in2, pair, me_tp)
    start(to_z2)
    to_y2(1).wait_recv()
    to_z2.wait_recv()
    for r in range(chunks):
        at = slice(r * C, (r + 1) * C)
        mixed = residual_scale * rows_all[odd, at, features(me_tp)].astype(f32) + (
            keep2[1, 1, at, :].astype(f32)
            + core_in2[1, 1, at, :].astype(f32)
            + y_in2[1, at, :].astype(f32)
            + z_in2[at, :].astype(f32)
        )
        mix[at, :] = mixed
        send_stats(mixed, stat_ids2, stat_own2, stat_in2, r)
    for r in range(chunks):
        at = slice(r * C, (r + 1) * C)
        out_ref[at, :] = norm(mix[at, :], stat_ids2, stat_own2, stat_in2, r, 2).astype(bf16)

    for copy, when in sent:
        if when is None:
            copy.wait_send()
        else:
            pl.when(when)(copy.wait_send)
    for w in range(3):
        for d in range(nz):
            if d:
                by_parity((odd + d) % 2, lambda p, d=d, w=w: z_weight(w, d, p).wait_send())
            by_parity(odd, lambda p, d=d, w=w: x_weight(w, d, p).wait_send())
    assert rc.count <= REMOTE, rc.count


def fused(
    residual, query_nope, query_rope, latent, rope_key, doc_ids, key_up, value_up, out_proj,
    norm1_gain, norm1_bias, ffn_gate, ffn_value, conv_gate, conv_value, ffn_down, norm2_gain, norm2_bias,
):
    n_sp, n_tp = lax.axis_size("sp"), lax.axis_size("tp")
    R, F = residual.shape
    heads = query_nope.shape[1] // NOPE
    units = ffn_gate.shape[1]
    first = -(-units // (2 * LANES)) * LANES
    second = units - first
    window = (REACH + 1) * R
    chunks = R // LANES
    f32, bf16 = jnp.float32, jnp.bfloat16
    offset = lax.axis_index("sp") * R
    positions = offset + jnp.arange(R, dtype=jnp.int32)
    half = ROPE // 2
    place = jnp.arange(LANES, dtype=jnp.int32) % half
    frequencies = 1.0 / rope_base_freq ** (2.0 * place.astype(f32) / ROPE)
    angles = positions.astype(f32)[:, None] * frequencies[None, :]
    cosine, sine = jnp.cos(angles), jnp.sin(angles)

    def turn(vectors):
        width = vectors.shape[1]
        row = lax.broadcasted_iota(jnp.int32, (width, width), 0)
        col = lax.broadcasted_iota(jnp.int32, (width, width), 1)
        front = col % ROPE < half
        swap = jnp.where(front & (row == col + half), -1.0, 0.0) + jnp.where(
            ~front & (row == col - half), 1.0, 0.0
        )
        swapped = jnp.dot(vectors, swap.astype(bf16), preferred_element_type=f32)
        times = max(1, width // LANES)
        cos_wide = jnp.tile(cosine, (1, times))[:, :width]
        sin_wide = jnp.tile(sine, (1, times))[:, :width]
        return (vectors.astype(f32) * cos_wide + swapped * sin_wide).astype(bf16)

    packed = jnp.concatenate(
        [latent, turn(rope_key), jnp.broadcast_to(doc_ids.astype(bf16)[:, None], (R, ROPE))], 1
    )
    gains = jnp.stack([norm1_gain, norm1_bias, norm2_gain, norm2_bias]).astype(f32)
    odd = (lax.axis_index("sp") // 2) % 2
    blank = jnp.zeros((5, units), f32)
    taps = jnp.concatenate([conv_gate.astype(f32), blank, conv_value.astype(f32), blank], 0)
    taps = jnp.where(
        odd == 0, taps[:, :first], jnp.pad(taps[:, first:], ((0, 0), (0, first - second)))
    )
    hbm = pl.BlockSpec(memory_space=pl.ANY)
    vmem = pl.BlockSpec(memory_space=pltpu.VMEM)
    sizes = (n_sp, n_tp, R, REACH, heads, n_tp * F, first, second)

    def v(*shape, dtype=bf16):
        return pltpu.VMEM(shape, dtype)

    C = LANES
    return pl.pallas_call(
        functools.partial(layer_kernel, sizes),
        in_specs=[hbm] * 7 + [vmem] * 2 + [hbm] * 3,
        out_specs=vmem,
        out_shape=jax.ShapeDtypeStruct((R, F), bf16),
        scratch_shapes=[
            v(window, packed.shape[1]), v(R, heads * NOPE), v(R, heads * ROPE),
            v(*key_up.shape), v(*value_up.shape), v(*out_proj.shape), v(R, F),
            v(window, heads * NOPE), v(window, heads * VDIM), v(2, window, LANES),
            v(R, window, dtype=f32), v(R, heads * VDIM),
            v(chunks, 2, C, F), v(chunks, 2, C, F), v(chunks, 2, C, F), v(chunks, C, F), v(chunks, C, F),
            v(R, F, dtype=f32), v(chunks, 8, LANES, dtype=f32), v(chunks, 3, 8, LANES, dtype=f32),
            v(2, R, LANES),
            v(2, R, n_tp * F), v(n_sp * ffn_gate.shape[0], first), v(n_sp * ffn_gate.shape[0], first),
            v(n_sp, first, ffn_down.shape[1]), v(2, R + 8, 2 * first, dtype=f32), v(2, R, first),
            v(2, 2, R, F), v(2, 2, R, F), v(2, 2, R, F), v(2, R, F), v(2, R, F), v(R, F), v(R, F),
            v(chunks, 8, LANES, dtype=f32), v(chunks, 3, 8, LANES, dtype=f32),
            pltpu.SemaphoreType.DMA((REMOTE,)), pltpu.SemaphoreType.DMA((REMOTE,)),
            pltpu.SemaphoreType.DMA((LOCAL,)),
        ],
        compiler_params=pltpu.CompilerParams(
            collective_id=0, has_side_effects=True, vmem_limit_bytes=64 * 1024 * 1024 - 65536
        ),
    )(
        query_nope, turn(query_rope), packed, key_up, value_up, out_proj, residual, gains, taps,
        ffn_gate, ffn_value, ffn_down,
    )


def local(*arrays):
    rows, features = arrays[0].shape
    down_cols = arrays[15].shape[1]
    n_sp, n_tp = lax.axis_size("sp"), lax.axis_size("tp")
    paired = n_sp // 2
    fits = n_tp == 4 and n_sp % 4 == 0 and paired & (paired - 1) == 0
    tiled = rows % LANES == 0 and down_cols % LANES == 0 and features % down_cols == 0
    return (fused if fits and tiled else plain)(*arrays)


def solution(mesh):
    placed = (
        P("sp", "tp"),
        P("sp", "tp"),
        P("sp", "tp"),
        P("sp", None),
        P("sp", None),
        P("sp"),
        P(None, "tp"),
        P(None, "tp"),
        P("tp", None),
        P("tp"),
        P("tp"),
        P("sp", "tp"),
        P("sp", "tp"),
        P(None, "tp"),
        P(None, "tp"),
        P("tp", "sp"),
        P("tp"),
        P("tp"),
    )
    return jax.shard_map(
        local, mesh=mesh, in_specs=placed, out_specs=P("sp", "tp"), check_vma=False
    )
```

```python
import functools

import jax
import jax.numpy as jnp
from jax import lax
from jax.experimental import pallas as pl
from jax.experimental.pallas import tpu as pltpu
from jax.sharding import PartitionSpec as P

D = 2048
NOPE = 128
ROPE = 64
VDIM = 128
CONV = 3
REACH = 3


norm_eps = 1e-05
residual_scale = 8.0**0.25
rope_base_freq = 10000.0
masked_score = -1e30


def passed_along(value, axis, by):
    count = lax.axis_size(axis)
    pairs = [(i, i + by) for i in range(count) if 0 <= i + by < count]
    return lax.ppermute(value, axis, pairs)


def tables(positions):
    frequencies = 1.0 / rope_base_freq ** (jnp.arange(0, ROPE, 2, dtype=jnp.float32) / ROPE)
    angles = positions.astype(jnp.float32)[:, None] * frequencies[None, :]
    return (jnp.cos(angles), jnp.sin(angles))


def rotate(vectors, cosine, sine_table):
    half_width = vectors.shape[-1] // 2
    front_half = vectors[..., :half_width]
    back_half = vectors[..., half_width:]
    return jnp.concatenate(
        [
            front_half * cosine - back_half * sine_table,
            front_half * sine_table + back_half * cosine,
        ],
        axis=-1,
    )


def ring_blocks(block, axis):
    count = lax.axis_size(axis)
    order = list(range(0, count, 2)) + list(range(1, count, 2))[::-1]
    place = [order.index(i) for i in range(count)]
    me = lax.axis_index(axis)
    found = [(me, block)]
    ahead = count // 2
    for turn, steps in ((1, ahead), (-1, count - 1 - ahead)):
        pairs = [(order[p], order[(p + turn) % count]) for p in range(count)]
        moving = block
        for step in range(1, steps + 1):
            moving = lax.ppermute(moving, axis, pairs)
            owners = [order[(place[i] - turn * step) % count] for i in range(count)]
            found.append((jnp.asarray(owners, jnp.int32)[me], moving))
    return found


def attend_kernel(chunk, reach_rows, scale, q_ref, turned_ref, k_ref, rope_ref, v_ref, bias_ref, out_ref):
    rows = q_ref.shape[0]
    span = chunk + reach_rows
    rope_rows = rope_ref[...]
    for head in range(q_ref.shape[1] // NOPE):
        nope = slice(head * NOPE, (head + 1) * NOPE)
        rope = slice(head * ROPE, (head + 1) * ROPE)
        queries = jnp.concatenate([q_ref[:, nope], turned_ref[:, rope]], 1)
        keys = jnp.concatenate([k_ref[:, nope], rope_rows], 1)
        for start in range(0, rows, chunk):
            cut = slice(start, start + chunk)
            seen = slice(start, start + span)
            scores = lax.dot_general(
                queries[cut], keys[seen], (((1,), (1,)), ((), ())), preferred_element_type=jnp.float32
            )
            scores = scores * scale + bias_ref[cut, seen]
            weights = jnp.exp(scores - jnp.max(scores, -1, keepdims=True))
            weights = weights * (1.0 / jnp.sum(weights, -1, keepdims=True))
            out_ref[cut, nope] = jnp.dot(
                weights.astype(jnp.bfloat16), v_ref[seen, nope], preferred_element_type=jnp.float32
            ).astype(jnp.bfloat16)


def attend(queries, turned, keys, rope_rows, values, bias, scale):
    rows, width = queries.shape
    window = keys.shape[0]
    chunk = 128 if rows % 128 == 0 else rows
    pair = 2
    wide = pair * NOPE
    heads = width // NOPE
    return pl.pallas_call(
        functools.partial(attend_kernel, chunk, window - rows, scale),
        grid=(heads // pair,),
        in_specs=[
            pl.BlockSpec((rows, wide), lambda i: (0, i)),
            pl.BlockSpec((rows, pair * ROPE), lambda i: (0, i)),
            pl.BlockSpec((window, wide), lambda i: (0, i)),
            pl.BlockSpec((window, ROPE), lambda i: (0, 0)),
            pl.BlockSpec((window, pair * VDIM), lambda i: (0, i)),
            pl.BlockSpec((rows, window), lambda i: (0, 0)),
        ],
        out_specs=pl.BlockSpec((rows, pair * VDIM), lambda i: (0, i)),
        out_shape=jax.ShapeDtypeStruct((rows, heads * VDIM), jnp.bfloat16),
        compiler_params=pltpu.CompilerParams(vmem_limit_bytes=40 * 1024 * 1024),
        cost_estimate=pl.CostEstimate(
            flops=16 * rows * window * heads * (NOPE + ROPE + VDIM),
            bytes_accessed=2 * (4 * rows * width + 2 * window * width),
            transcendentals=rows * window * heads,
        ),
    )(queries, turned, keys, rope_rows, values, bias)


def scatter_sum(terms, axis):
    count = lax.axis_size(axis)
    width = terms.shape[1] // count
    parts = jnp.stack([terms[:, i * width : (i + 1) * width] for i in range(count)])
    got = lax.all_to_all(parts.astype(jnp.bfloat16), axis, 0, 0)
    return jnp.sum(got.astype(jnp.float32), 0)


def finish(mixed, totals, gain_row, bias_row):
    row_mean = totals[0][:, None] / D
    row_power = totals[1][:, None] / D
    return (mixed - row_mean) * lax.rsqrt(
        row_power - row_mean * row_mean + norm_eps
    ) * gain_row.astype(jnp.float32) + bias_row.astype(jnp.float32)


def plain(
    residual,
    query_nope,
    query_rope,
    latent,
    rope_key,
    doc_ids,
    key_up,
    value_up,
    out_proj,
    norm1_gain,
    norm1_bias,
    ffn_gate,
    ffn_value,
    conv_gate,
    conv_value,
    ffn_down,
    norm2_gain,
    norm2_bias,
):
    row_count = latent.shape[0]
    head_count = query_nope.shape[1] // NOPE
    local_units = ffn_gate.shape[1]
    rim_rows = CONV - 1
    whole_gate = lax.all_gather(ffn_gate, "sp", axis=0, tiled=True)
    whole_value = lax.all_gather(ffn_value, "sp", axis=0, tiled=True)
    offset = lax.axis_index("sp") * row_count
    positions = offset + jnp.arange(row_count, dtype=jnp.int32)
    cosine, sine_table = tables(positions)
    turned_key = rotate(rope_key.astype(jnp.float32), cosine, sine_table).astype(jnp.bfloat16)
    turned_query = rotate(
        query_rope.astype(jnp.float32).reshape(row_count, head_count, ROPE),
        cosine[:, None],
        sine_table[:, None],
    ).astype(jnp.bfloat16)
    latent_width = latent.shape[1]
    packed = jnp.concatenate(
        [
            latent,
            turned_key,
            jnp.broadcast_to(doc_ids.astype(jnp.bfloat16)[:, None], (row_count, ROPE)),
        ],
        1,
    )
    parts = [passed_along(packed, "sp", shift_step) for shift_step in range(REACH, 0, -1)]
    pieces = jnp.concatenate(parts + [packed], 0)
    win_latent = pieces[:, :latent_width]
    win_key = pieces[:, latent_width : latent_width + ROPE]
    win_doc = pieces[:, latent_width + ROPE].astype(jnp.int32)
    down_blocks = ring_blocks(ffn_down, "sp")
    key_rows = jnp.dot(win_latent, key_up, preferred_element_type=jnp.float32).astype(jnp.bfloat16)
    values = jnp.dot(win_latent, value_up, preferred_element_type=jnp.float32).astype(jnp.bfloat16)
    window = key_rows.shape[0]
    key_pos = offset - REACH * row_count + jnp.arange(window, dtype=jnp.int32)
    allowed = (
        (key_pos[None, :] <= positions[:, None])
        & (key_pos[None, :] >= 0)
        & (win_doc[None, :] == doc_ids[:, None])
    )
    scale = (NOPE + ROPE) ** (-0.5)
    bias = jnp.where(allowed, 0.0, masked_score).astype(jnp.float32)
    attended = attend(
        query_nope,
        turned_query.reshape(row_count, head_count * ROPE),
        key_rows,
        win_key,
        values,
        bias,
        scale,
    )
    head_terms = jnp.dot(attended, out_proj, preferred_element_type=jnp.float32)
    projected = scatter_sum(head_terms, "tp")
    mixed_one = residual_scale * residual.astype(jnp.float32) + projected
    totals_one = lax.psum((jnp.sum(mixed_one, 1), jnp.sum(mixed_one * mixed_one, 1)), "tp")
    normed = finish(mixed_one, totals_one, norm1_gain, norm1_bias).astype(jnp.bfloat16)
    half = row_count // 2
    full_rows = jnp.concatenate(
        [
            lax.all_gather(normed[:half], "tp", axis=1, tiled=True),
            lax.all_gather(normed[half:], "tp", axis=1, tiled=True),
        ],
        0,
    )
    gate_sum = jnp.dot(full_rows, whole_gate, preferred_element_type=jnp.float32)
    value_sum = jnp.dot(full_rows, whole_value, preferred_element_type=jnp.float32)
    gate_pre = gate_sum.astype(jnp.bfloat16)
    value_pre = value_sum.astype(jnp.bfloat16)
    tail_gate, tail_value, tail_doc = passed_along(
        (
            gate_pre[row_count - rim_rows :],
            value_pre[row_count - rim_rows :],
            doc_ids[row_count - rim_rows :],
        ),
        "sp",
        1,
    )
    ext_gate = jnp.concatenate([tail_gate, gate_pre], 0)
    ext_value = jnp.concatenate([tail_value, value_pre], 0)
    ext_doc = jnp.concatenate([tail_doc, doc_ids], 0)
    gate_mix = jnp.zeros((row_count, local_units), jnp.float32)
    value_mix = jnp.zeros((row_count, local_units), jnp.float32)
    for tap_index in range(CONV):
        valid_tap = (
            (ext_doc[tap_index : tap_index + row_count] == doc_ids)
            & (positions - rim_rows + tap_index >= 0)
        ).astype(jnp.float32)[:, None]
        gate_mix = (
            gate_mix
            + conv_gate[tap_index].astype(jnp.float32)
            * ext_gate[tap_index : tap_index + row_count].astype(jnp.float32)
            * valid_tap
        )
        value_mix = (
            value_mix
            + conv_value[tap_index].astype(jnp.float32)
            * ext_value[tap_index : tap_index + row_count].astype(jnp.float32)
            * valid_tap
        )
    hidden = (value_mix * jax.nn.gelu(gate_mix)).astype(jnp.bfloat16)
    sp_count = lax.axis_size("sp")
    tp_count = lax.axis_size("tp")
    block_width = ffn_down.shape[1]
    unit_terms = jnp.zeros((sp_count, row_count, block_width), jnp.bfloat16)
    for owner, block in down_blocks:
        term = jnp.dot(hidden, block, preferred_element_type=jnp.float32).astype(jnp.bfloat16)
        unit_terms = lax.dynamic_update_slice(unit_terms, term[None], (owner, 0, 0))
    share = sp_count // tp_count
    got = lax.all_to_all(
        unit_terms.reshape(tp_count, share, row_count, block_width), "tp", 0, 0
    )
    ffn_blocks = jnp.sum(got.astype(jnp.float32), 0)
    ffn_out = jnp.concatenate([ffn_blocks[i] for i in range(share)], 1)
    mixed_two = residual_scale * normed.astype(jnp.float32) + ffn_out
    totals_two = lax.psum((jnp.sum(mixed_two, 1), jnp.sum(mixed_two * mixed_two, 1)), "tp")
    return finish(mixed_two, totals_two, norm2_gain, norm2_bias).astype(jnp.bfloat16)


LANES = 128
MESH = pl.DeviceIdType.MESH
log2_e = 1.4426950408889634


class Copies:
    def __init__(self, send_sems, recv_sems):
        self.send_sems, self.recv_sems = send_sems, recv_sems
        self.count = 0

    def ids(self, number=1):
        first = self.count
        self.count += number
        return first

    def make(self, index, source, target, sp, tp):
        return pltpu.make_async_remote_copy(
            src_ref=source,
            dst_ref=target,
            send_sem=self.send_sems.at[index],
            recv_sem=self.recv_sems.at[index],
            device_id={"sp": sp, "tp": tp},
            device_id_type=MESH,
        )


REMOTE = 160
LOCAL = 16


def flip(value, bits):
    for bit in range(bits.bit_length()):
        step = 1 << bit
        if bits & step:
            value = value + step - 2 * step * ((value // step) % 2)
    return value


def layer_kernel(
    sizes,
    q_in, t_in, pack_in, kup_in, vup_in, proj_in, resid_in, gains, taps, gate_in, value_in, down_in,
    out_ref,
    win, q_v, t_v, kup, vup, proj, resid, keys, vals, ropes, bias, att,
    core_out, core_in, keep, y_out, y_in, mix, stat_own, stat_in, valid,
    rows_all, gate_w, value_w, down_w, ext, hid,
    core_out2, core_in2, keep2, y_out2, y_in2, z_out2, z_in2, stat_own2, stat_in2,
    send_sems, recv_sems, local_sems,
):
    n_sp, n_tp, R, reach, heads, wide, first, second = sizes
    C = LANES
    F = resid.shape[1]
    chunks = R // C
    window = (reach + 1) * R
    span = C + reach * R
    latent_width = kup.shape[0]
    gate_rows = gate_in.shape[0]
    down_cols = down_in.shape[1]
    bf16, f32 = jnp.bfloat16, jnp.float32
    me_sp, me_tp = lax.axis_index("sp"), lax.axis_index("tp")
    x, z = me_sp % 2, me_sp // 2
    odd = z % 2
    y, c = me_tp // 2, me_tp % 2
    x_peer = me_sp + 1 - 2 * x
    c_peer = me_tp + 1 - 2 * c
    y_peer = me_tp + 2 - 4 * y
    far_peer = 3 - me_tp
    nz = n_sp // 2
    z_sp = [2 * flip(z, d) + x for d in range(nz)]
    pair = z_sp[1]
    rc = Copies(send_sems, recv_sems)
    sent = []

    def start(copy, when=None):
        if when is None:
            copy.start()
        else:
            pl.when(when)(copy.start)
        sent.append((copy, when))

    barrier = pltpu.get_barrier_semaphore()
    for i in range(n_sp):
        for j in range(n_tp):
            if i or j:
                pl.semaphore_signal(
                    barrier, inc=1,
                    device_id={"sp": (me_sp + i) % n_sp, "tp": (me_tp + j) % n_tp},
                    device_id_type=MESH,
                )

    loads = {}

    def load(name, source, target):
        loads[name] = pltpu.make_async_copy(source, target, local_sems.at[len(loads)])
        loads[name].start()

    load("win", pack_in, win.at[pl.ds(reach * R, R)])
    load("kup", kup_in, kup)
    load("vup", vup_in, vup)
    load("q", q_in, q_v)
    load("t", t_in, t_v)
    load("proj", proj_in, proj)
    load("resid", resid_in, resid)

    with jax.named_scope("barrier"):
        pl.semaphore_wait(barrier, n_sp * n_tp - 1)

    part = R // n_tp
    halo = rc.ids(reach)
    halo_ids = rc.ids(3 * reach)

    def quarter(k, tp):
        return win.at[pl.ds(pl.multiple_of((reach - k) * R + tp * part, 16), part)]

    def halo_copy(k):
        return rc.make(
            halo + k - 1, pack_in.at[pl.ds(pl.multiple_of(me_tp * part, 16), part)],
            quarter(k, me_tp), me_sp + k, me_tp,
        )

    def halo_pass(k, kind, tp, tp_to):
        rows = quarter(k, tp)
        return rc.make(halo_ids + 3 * (k - 1) + kind, rows, rows, me_sp, tp_to)

    for k in range(1, reach + 1):
        start(halo_copy(k), me_sp + k < n_sp)

    halves = ((0, first), (first, second))

    def half_in(w, parity):
        at, size = halves[parity]
        if w == 2:
            return down_in.at[pl.ds(at, size), :]
        return (gate_in, value_in)[w].at[:, pl.ds(at, size)]

    def half_slot(w, parity, owner):
        size = halves[parity][1]
        if w == 2:
            return down_w.at[owner, pl.ds(0, size), :]
        rows = pl.ds(pl.multiple_of(owner * gate_rows, 16), gate_rows)
        return (gate_w, value_w)[w].at[rows, pl.ds(0, size)]

    def by_parity(parity, act):
        for p in range(2):
            pl.when(parity == p)(functools.partial(act, p))

    z_ids = [rc.ids(nz) for _ in range(3)]
    x_ids = [rc.ids(nz) for _ in range(3)]
    own_ids = [len(loads) + w for w in range(3)]

    def own_weight(w, p):
        return pltpu.make_async_copy(half_in(w, p), half_slot(w, p, me_sp), local_sems.at[own_ids[w]])

    def z_weight(w, d, p):
        return rc.make(z_ids[w] + d, half_in(w, p), half_slot(w, p, me_sp), z_sp[d], me_tp)

    def z_landed(w, d, p):
        return rc.make(z_ids[w] + d, half_in(w, p), half_slot(w, p, z_sp[d]), z_sp[d], me_tp)

    def x_weight(w, d, p):
        source = half_in(w, p) if d == 0 else half_slot(w, p, z_sp[d])
        return rc.make(x_ids[w] + d, source, half_slot(w, p, z_sp[d]), x_peer, me_tp)

    def x_landed(w, d, p):
        slot = half_slot(w, p, z_sp[d] + 1 - 2 * x)
        return rc.make(x_ids[w] + d, slot, slot, x_peer, me_tp)

    def send_z(w, which):
        for d in which:
            by_parity((odd + d) % 2, lambda p, d=d: z_weight(w, d, p).start())

    def send_x(w, d):
        if d:
            by_parity(odd, lambda p: z_landed(w, d, p).wait_recv())
        by_parity(odd, lambda p: x_weight(w, d, p).start())

    def all_here(w):
        def act(p):
            own_weight(w, p).wait()
            for d in range(nz):
                x_landed(w, d, p).wait_recv()
        by_parity(odd, act)

    for w in range(3):
        by_parity(odd, lambda p, w=w: own_weight(w, p).start())
    middle, near = list(range(2, nz)), [1]
    rightward = 1 - z // (nz // 2)

    inner = odd == rightward
    outer = jnp.logical_not(inner)

    def first_weights(right):
        for w in range(2):
            pl.when((1 - odd) == right)(lambda w=w: send_z(w, near))
        pl.when(rightward == right)(lambda: send_z(0, middle))
        for w in (1, 2):
            pl.when((rightward == right) & inner)(lambda w=w: send_z(w, middle))

    first_weights(0)

    @pl.when(odd == 1)
    def _():
        blank = first - second
        if blank:
            gate_w[:, second:] = jnp.zeros((gate_w.shape[0], blank), bf16)
            value_w[:, second:] = jnp.zeros((gate_w.shape[0], blank), bf16)
            down_w[:, second:, :] = jnp.zeros((n_sp, blank, down_cols), bf16)

    loads["win"].wait()
    loads["kup"].wait()
    loads["vup"].wait()

    def raise_rows(block):
        rows = pl.ds(pl.multiple_of(block * R, LANES), R)
        source = win[rows, :latent_width]
        keys[rows, :] = jnp.dot(source, kup[...], preferred_element_type=f32).astype(bf16)
        vals[rows, :] = jnp.dot(source, vup[...], preferred_element_type=f32).astype(bf16)

    with jax.named_scope("own_kv"):
        raise_rows(reach)
    for k in range(1, reach + 1):
        @pl.when(me_sp >= k)
        def _(k=k):
            with jax.named_scope("halo_wait"):
                halo_copy(k).wait_recv()
            halo_pass(k, 0, me_tp, y_peer).start()
            halo_pass(k, 1, me_tp, c_peer).start()

        @pl.when(me_sp < k)
        def _(k=k):
            win[(reach - k) * R : (reach - k + 1) * R, :] = jnp.zeros((R, win.shape[1]), bf16)
        sent.append((halo_pass(k, 0, me_tp, y_peer), me_sp >= k))
        sent.append((halo_pass(k, 1, me_tp, c_peer), me_sp >= k))
    for k in range(1, reach + 1):
        @pl.when(me_sp >= k)
        def _(k=k):
            with jax.named_scope("halo_y_wait"):
                halo_pass(k, 0, y_peer, y_peer).wait_recv()
            halo_pass(k, 2, y_peer, c_peer).start()
        sent.append((halo_pass(k, 2, y_peer, c_peer), me_sp >= k))
    for k in range(1, reach + 1):
        @pl.when(me_sp >= k)
        def _(k=k):
            with jax.named_scope("halo_core_wait"):
                halo_pass(k, 1, c_peer, c_peer).wait_recv()
                halo_pass(k, 2, far_peer, c_peer).wait_recv()
    first_weights(1)
    send_x(0, 0)
    send_x(1, 0)

    with jax.named_scope("kv"):
        @pl.loop(0, reach)
        def _(block):
            raise_rows(block)

    side = win[:, latent_width:]
    side_f = side.astype(f32)
    lane = lax.broadcasted_iota(jnp.int32, (window, LANES), 1)
    low = lane < LANES // 2
    ropes[0] = jnp.where(low, side_f, 0.0).astype(bf16)
    ropes[1] = jnp.where(low, 0.0, pltpu.roll(side_f, LANES // 2, 1)).astype(bf16)
    pick = (
        (lax.broadcasted_iota(jnp.int32, (8, LANES), 1) == LANES // 2)
        .astype(f32)
        .astype(bf16)
    )
    key_doc = lax.dot_general(pick, side, (((1,), (1,)), ((), ())), preferred_element_type=f32)[0:1]
    for r in range(chunks):
        at = slice(r * C, (r + 1) * C)
        own_doc = side_f[reach * R + r * C : reach * R + (r + 1) * C, LANES // 2 : LANES // 2 + 1]
        key_at = lax.broadcasted_iota(jnp.int32, (C, window), 1) - reach * R
        row_at = lax.broadcasted_iota(jnp.int32, (C, window), 0) + r * C
        allowed = (key_at <= row_at) & (key_at + me_sp * R >= 0) & (key_doc == own_doc)
        bias[at, :] = jnp.where(allowed, 0.0, masked_score)

    tail = side_f[reach * R - 8 :]
    valid_id = rc.ids()
    row_no = lax.broadcasted_iota(jnp.int32, (R, LANES), 0) + me_sp * R
    here = tail[8:]
    back_one = (pltpu.roll(tail, 1, 0)[8:] == here) & (row_no >= 1)
    back_two = (pltpu.roll(tail, 2, 0)[8:] == here) & (row_no >= 2)
    lanes = lax.broadcasted_iota(jnp.int32, (R, LANES), 1)
    valid[odd] = jnp.where(
        lanes < 3 * LANES // 4, back_two.astype(f32), back_one.astype(f32)
    ).astype(bf16)
    start(rc.make(valid_id, valid.at[odd], valid.at[odd], pair, me_tp))

    scale = (NOPE + ROPE) ** (-0.5) * log2_e

    def attend_chunk(r):
        at, seen = slice(r * C, (r + 1) * C), slice(r * C, r * C + span)

        @pl.loop(0, heads // 2)
        def _(duo):
            turned = t_v[at, pl.ds(pl.multiple_of(duo * LANES, LANES), LANES)]
            for e in range(2):
                head = pl.ds(pl.multiple_of((2 * duo + e) * LANES, LANES), LANES)
                queries = jnp.concatenate([q_v[at, head], turned], 1)
                seen_keys = jnp.concatenate([keys[seen, head], ropes[e, seen, :]], 1)
                scores = lax.dot_general(
                    queries, seen_keys, (((1,), (1,)), ((), ())), preferred_element_type=f32
                )
                scores = scores * scale + bias[at, seen]
                weights = jnp.exp2(scores - jnp.max(scores, -1, keepdims=True))
                total = jnp.sum(weights, -1, keepdims=True)
                mixed = jnp.dot(weights.astype(bf16), vals[seen, head], preferred_element_type=f32)
                att[at, head] = (mixed * (1.0 / total)).astype(bf16)

    core_ids, y_ids = rc.ids(2 * chunks), rc.ids(chunks)
    stat_ids = rc.ids(3 * chunks)
    stat_ids2 = rc.ids(3 * chunks)
    gather_ids = rc.ids(8 * chunks)

    def to_core(r, i):
        return rc.make(core_ids + 2 * r + i, core_out.at[r, i], core_in.at[r, i], me_sp, c_peer)

    def to_y(r):
        return rc.make(y_ids + r, y_out.at[r], y_in.at[r], me_sp, y_peer)

    def features(tp):
        return pl.ds(pl.multiple_of(tp * F, LANES), F)

    def project(r):
        rows = att[r * C : (r + 1) * C, :]
        for i, yy in enumerate((1 - y, y)):
            core_out[r, i] = jnp.dot(
                rows, proj[:, features(2 * yy + 1 - c)], preferred_element_type=f32
            ).astype(bf16)
            start(to_core(r, i))
        for i, yy in enumerate((1 - y, y)):
            keep[r, i] = jnp.dot(
                rows, proj[:, features(2 * yy + c)], preferred_element_type=f32
            ).astype(bf16)
        to_core(r, 0).wait_recv()
        y_out[r] = (keep[r, 0].astype(f32) + core_in[r, 0].astype(f32)).astype(bf16)
        start(to_y(r))

    def stat_copy(ids, own, landed, r, i):
        return rc.make(ids + 3 * r + i, own.at[r], landed.at[r, i], me_sp, (c_peer, y_peer, far_peer)[i])

    def send_stats(values, ids, own, landed, r):
        one = jnp.sum(values, -1, keepdims=True)
        two = jnp.sum(values * values, -1, keepdims=True)
        lane = lax.broadcasted_iota(jnp.int32, (C, LANES), 1)
        own[r] = jnp.where(lane % 8 < 4, one, two).T[0:8]
        for i in (1, 2, 0):
            start(stat_copy(ids, own, landed, r, i))

    def norm(values, ids, own, landed, r, gain):
        for i in range(3):
            stat_copy(ids, own, landed, r, i).wait_recv()
        total = (own[r] + landed[r, 0]) + (landed[r, 1] + landed[r, 2])
        total = jnp.concatenate([total] * (LANES // 8), 0).T
        row_mean = total[:, 0:1] / wide
        row_power = total[:, 4:5] / wide
        return (values - row_mean) * lax.rsqrt(row_power - row_mean * row_mean + norm_eps) * gains[
            gain : gain + 1, :
        ] + gains[gain + 1 : gain + 2, :]

    def mix_one(r):
        at = slice(r * C, (r + 1) * C)
        to_core(r, 1).wait_recv()
        to_y(r).wait_recv()
        mixed = residual_scale * resid[at, :].astype(f32) + (
            keep[r, 1].astype(f32) + core_in[r, 1].astype(f32) + y_in[r].astype(f32)
        )
        mix[at, :] = mixed
        send_stats(mixed, stat_ids, stat_own, stat_in, r)

    def gathered(r, kind, slot, tp, sp_to, tp_to):
        spot = rows_all.at[slot, pl.ds(r * C, C), features(tp)]
        return rc.make(gather_ids + 8 * r + kind, spot, spot, sp_to, tp_to)

    def to_pair(r, slot):
        return gathered(r, 0, slot, me_tp, pair, me_tp)

    def core_gather(r, kind, slot, tp):
        return gathered(r, kind, slot, tp, me_sp, c_peer)

    def y_gather(r, kind, slot, tp):
        return gathered(r, kind, slot, tp, me_sp, y_peer)

    def norm_one(r):
        at = slice(r * C, (r + 1) * C)
        rows_all[odd, at, features(me_tp)] = norm(
            mix[at, :], stat_ids, stat_own, stat_in, r, 0
        ).astype(bf16)
        start(to_pair(r, odd))
        start(y_gather(r, 1, odd, me_tp))
        start(core_gather(r, 2, odd, me_tp))

    def pass_pair(r):
        to_pair(r, 1 - odd).wait_recv()
        start(y_gather(r, 3, 1 - odd, me_tp))
        start(core_gather(r, 4, 1 - odd, me_tp))

    def pass_y(r):
        for kind, got, slot in ((5, 1, odd), (6, 3, 1 - odd)):
            y_gather(r, got, slot, y_peer).wait_recv()
            start(core_gather(r, kind, slot, y_peer))

    def rows_here(r):
        core_gather(r, 2, odd, c_peer).wait_recv()
        core_gather(r, 4, 1 - odd, c_peer).wait_recv()
        core_gather(r, 5, odd, far_peer).wait_recv()
        core_gather(r, 6, 1 - odd, far_peer).wait_recv()

    loads["q"].wait()
    loads["t"].wait()
    def z_left(w, d):
        by_parity((odd + d) % 2, lambda p: z_weight(w, d, p).wait_send())

    def forward(w, which):
        for d in which:
            with jax.named_scope("fwd%d_%d" % (w, d)):
                send_x(w, d)

    def attend_step(r):
        with jax.named_scope("att"):
            attend_chunk(r)
        if r == 0:
            loads["proj"].wait()
            loads["resid"].wait()
        else:
            with jax.named_scope("mix"):
                mix_one(r - 1)
        with jax.named_scope("proj"):
            project(r)
        if r:
            with jax.named_scope("norm"):
                norm_one(r - 1)

    for r in range(chunks):
        attend_step(r)
        if r == 0:
            pl.when(outer)(lambda: send_z(1, middle))
            forward(0, near)
            send_x(2, 0)
        elif r == 1:
            forward(1, near)
    forward(0, middle)
    with jax.named_scope("mix"):
        mix_one(chunks - 1)
    with jax.named_scope("norm"):
        norm_one(chunks - 1)
    send_z(2, near)
    forward(1, middle[:-1])
    with jax.named_scope("pass_pair"):
        for r in range(chunks):
            pass_pair(r)
    with jax.named_scope("pass_y"):
        for r in range(chunks):
            pass_y(r)
    forward(1, middle[-1:])
    with jax.named_scope("rows_here"):
        for r in range(chunks):
            rows_here(r)

    tile = 2 * LANES
    mid = first

    def up(weights, base):
        @pl.loop(0, 2)
        def _(slot):
            @pl.loop(0, first // tile)
            def _(j):
                cols = pl.multiple_of(j * tile, LANES)
                ext[slot, 8:, pl.ds(base + cols, tile)] = (
                    jnp.dot(rows_all[slot], weights[:, pl.ds(cols, tile)], preferred_element_type=f32)
                    .astype(bf16)
                    .astype(f32)
                )

    with jax.named_scope("wait_g"):
        all_here(0)
    with jax.named_scope("up_g"):
        up(gate_w, 0)
    forward(2, near)
    with jax.named_scope("wait_v"):
        all_here(1)
    pl.when(outer)(lambda: send_z(2, middle))
    with jax.named_scope("up_v"):
        up(value_w, mid)

    tail_ids = rc.ids(2)

    def tail_copy(slot, to_slot, sp):
        return rc.make(
            tail_ids + to_slot, ext.at[slot, pl.ds(R, 8)], ext.at[to_slot, pl.ds(0, 8)], sp, me_tp
        )

    last_pair = z >= nz - 2
    start(tail_copy(0, 0, x_peer), x == 0)
    start(tail_copy(1, 1, x_peer), x == 0)
    start(tail_copy(0, 1, x_peer), x == 1)
    start(tail_copy(1, 0, me_sp + 3), (x == 1) & (z < nz - 2))

    @pl.when((x == 0) & (z < 2))
    def _():
        ext[0, 0:8, :] = jnp.zeros((8, ext.shape[2]), f32)

    forward(2, middle)

    @pl.when((x == 1) | (z >= 2))
    def _():
        tail_copy(0, 0, x_peer).wait_recv()
    tail_copy(1, 1, x_peer).wait_recv()
    rc.make(valid_id, valid.at[1 - odd], valid.at[1 - odd], pair, me_tp).wait_recv()

    deep = 64

    with jax.named_scope("conv"):
        @pl.loop(0, 2)
        def _(slot):
            @pl.loop(0, R // deep)
            def _(i):
                at = pl.multiple_of(i * deep, 16)
                marks = valid[slot, pl.ds(at, deep), :].astype(f32)
                two, one = marks[:, LANES // 2 : LANES // 2 + 1], marks[:, LANES - 1 : LANES]

                @pl.loop(0, first // tile)
                def _(j):
                    cols = pl.multiple_of(j * tile, LANES)

                    def mixing(base, tap):
                        rows = ext[slot, pl.ds(at, deep + 8), pl.ds(base + cols, tile)]
                        weight = taps[pl.ds(tap, 8), pl.ds(cols, tile)]
                        return (
                            weight[0:1] * (pltpu.roll(rows, 2, 0)[8:] * two)
                            + weight[1:2] * (pltpu.roll(rows, 1, 0)[8:] * one)
                            + weight[2:3] * rows[8:]
                        )

                    hid[slot, pl.ds(at, deep), pl.ds(cols, tile)] = (
                        mixing(mid, 8) * jax.nn.gelu(mixing(0, 0))
                    ).astype(bf16)

    core_ids2, z_ids2, y_ids2 = rc.ids(4), rc.ids(2 * chunks), rc.ids(chunks)
    per = F // down_cols
    half_z = (z // 2) % 2
    slots = (1 - odd, odd)

    def down(slot, tp, target):
        for j in range(per):
            target[:, j * down_cols : (j + 1) * down_cols] = jnp.dot(
                hid[slot], down_w[per * tp + j], preferred_element_type=f32
            ).astype(bf16)

    def to_core2(f, s):
        return rc.make(
            core_ids2 + 2 * f + s, core_out2.at[f, s], core_in2.at[f, s], me_sp, c_peer
        )

    def to_pair2(f, r):
        at = pl.ds(r * C, C)
        return rc.make(z_ids2 + chunks * f + r, z_out2.at[f, at], z_in2.at[f, at], pair, me_tp)

    def to_y2(r):
        at = pl.ds(r * C, C)
        return rc.make(y_ids2 + r, y_out2.at[at], y_in2.at[at], me_sp, y_peer)

    def down_set(f, ds):
        yy = half_z if f == 0 else 1 - half_z
        with jax.named_scope("wait_d%d" % f):
            if f == 0:
                by_parity(odd, lambda p: own_weight(2, p).wait())
            for d in ds:
                by_parity(odd, lambda p, d=d: x_landed(2, d, p).wait_recv())
        with jax.named_scope("down"):
            for s in range(2):
                down(slots[s], 2 * yy + 1 - c, core_out2.at[f, s])
                start(to_core2(f, s))
            down(slots[0], 2 * yy + c, keep2.at[f, 0])
        with jax.named_scope("core2_wait"):
            to_core2(f, 0).wait_recv()
        for r in range(chunks):
            at = slice(r * C, (r + 1) * C)
            z_out2[f, at, :] = (
                keep2[f, 0, at, :].astype(f32) + core_in2[f, 0, at, :].astype(f32)
            ).astype(bf16)
            start(to_pair2(f, r))
        with jax.named_scope("down"):
            down(slots[1], 2 * yy + c, keep2.at[f, 1])
        to_core2(f, 1).wait_recv()
        for r in range(chunks):
            at = slice(r * C, (r + 1) * C)
            with jax.named_scope("z2_wait"):
                to_pair2(f, r).wait_recv()

            @pl.when(y != yy)
            def _():
                y_out2[at, :] = (
                    keep2[f, 1, at, :].astype(f32)
                    + core_in2[f, 1, at, :].astype(f32)
                    + z_in2[f, at, :].astype(f32)
                ).astype(bf16)
                to_y2(r).start()

    down_set(0, [0] + near)
    down_set(1, middle)
    mine = (y + half_z) % 2
    for r in range(chunks):
        at = slice(r * C, (r + 1) * C)
        rows = pl.ds(r * C, C)
        with jax.named_scope("y2_wait"):
            to_y2(r).wait_recv()
        sent.append((to_y2(r), None))
        mixed = residual_scale * rows_all[odd, at, features(me_tp)].astype(f32) + (
            keep2[mine, 1, rows, :].astype(f32)
            + core_in2[mine, 1, rows, :].astype(f32)
            + z_in2[mine, rows, :].astype(f32)
            + y_in2[at, :].astype(f32)
        )
        mix[at, :] = mixed
        send_stats(mixed, stat_ids2, stat_own2, stat_in2, r)
    with jax.named_scope("norm2"):
        for r in range(chunks):
            at = slice(r * C, (r + 1) * C)
            out_ref[at, :] = norm(mix[at, :], stat_ids2, stat_own2, stat_in2, r, 2).astype(bf16)

    for copy, when in sent:
        if when is None:
            copy.wait_send()
        else:
            pl.when(when)(copy.wait_send)
    for w in range(3):
        for d in range(nz):
            if d:
                z_left(w, d)
            by_parity(odd, lambda p, d=d, w=w: x_weight(w, d, p).wait_send())
    assert rc.count <= REMOTE, rc.count


def fused(
    residual, query_nope, query_rope, latent, rope_key, doc_ids, key_up, value_up, out_proj,
    norm1_gain, norm1_bias, ffn_gate, ffn_value, conv_gate, conv_value, ffn_down, norm2_gain, norm2_bias,
):
    n_sp, n_tp = lax.axis_size("sp"), lax.axis_size("tp")
    R, F = residual.shape
    heads = query_nope.shape[1] // NOPE
    units = ffn_gate.shape[1]
    first = -(-units // (2 * LANES)) * LANES
    second = units - first
    window = (REACH + 1) * R
    chunks = R // LANES
    f32, bf16 = jnp.float32, jnp.bfloat16
    offset = lax.axis_index("sp") * R
    positions = offset + jnp.arange(R, dtype=jnp.int32)
    half = ROPE // 2
    place = jnp.arange(LANES, dtype=jnp.int32) % half
    frequencies = 1.0 / rope_base_freq ** (2.0 * place.astype(f32) / ROPE)
    angles = positions.astype(f32)[:, None] * frequencies[None, :]
    cosine, sine = jnp.cos(angles), jnp.sin(angles)

    def turn(vectors):
        width = vectors.shape[1]
        row = lax.broadcasted_iota(jnp.int32, (width, width), 0)
        col = lax.broadcasted_iota(jnp.int32, (width, width), 1)
        front = col % ROPE < half
        swap = jnp.where(front & (row == col + half), -1.0, 0.0) + jnp.where(
            ~front & (row == col - half), 1.0, 0.0
        )
        swapped = jnp.dot(vectors, swap.astype(bf16), preferred_element_type=f32)
        times = max(1, width // LANES)
        cos_wide = jnp.tile(cosine, (1, times))[:, :width]
        sin_wide = jnp.tile(sine, (1, times))[:, :width]
        return (vectors.astype(f32) * cos_wide + swapped * sin_wide).astype(bf16)

    packed = jnp.concatenate(
        [latent, turn(rope_key), jnp.broadcast_to(doc_ids.astype(bf16)[:, None], (R, ROPE))], 1
    )
    gains = jnp.stack([norm1_gain, norm1_bias, norm2_gain, norm2_bias]).astype(f32)
    odd = (lax.axis_index("sp") // 2) % 2
    blank = jnp.zeros((5, units), f32)
    taps = jnp.concatenate([conv_gate.astype(f32), blank, conv_value.astype(f32), blank], 0)
    taps = jnp.where(
        odd == 0, taps[:, :first], jnp.pad(taps[:, first:], ((0, 0), (0, first - second)))
    )
    hbm = pl.BlockSpec(memory_space=pl.ANY)
    vmem = pl.BlockSpec(memory_space=pltpu.VMEM)
    sizes = (n_sp, n_tp, R, REACH, heads, n_tp * F, first, second)

    def v(*shape, dtype=bf16):
        return pltpu.VMEM(shape, dtype)

    C = LANES
    return pl.pallas_call(
        functools.partial(layer_kernel, sizes),
        in_specs=[hbm] * 7 + [vmem] * 2 + [hbm] * 3,
        out_specs=vmem,
        out_shape=jax.ShapeDtypeStruct((R, F), bf16),
        scratch_shapes=[
            v(window, packed.shape[1]), v(R, heads * NOPE), v(R, heads * ROPE),
            v(*key_up.shape), v(*value_up.shape), v(*out_proj.shape), v(R, F),
            v(window, heads * NOPE), v(window, heads * VDIM), v(2, window, LANES),
            v(R, window, dtype=f32), v(R, heads * VDIM),
            v(chunks, 2, C, F), v(chunks, 2, C, F), v(chunks, 2, C, F), v(chunks, C, F), v(chunks, C, F),
            v(R, F, dtype=f32), v(chunks, 8, LANES, dtype=f32), v(chunks, 3, 8, LANES, dtype=f32),
            v(2, R, LANES),
            v(2, R, n_tp * F), v(n_sp * ffn_gate.shape[0], first), v(n_sp * ffn_gate.shape[0], first),
            v(n_sp, first, ffn_down.shape[1]), v(2, R + 8, 2 * first, dtype=f32), v(2, R, first),
            v(2, 2, R, F), v(2, 2, R, F), v(2, 2, R, F), v(R, F), v(R, F), v(2, R, F), v(2, R, F),
            v(chunks, 8, LANES, dtype=f32), v(chunks, 3, 8, LANES, dtype=f32),
            pltpu.SemaphoreType.DMA((REMOTE,)), pltpu.SemaphoreType.DMA((REMOTE,)),
            pltpu.SemaphoreType.DMA((LOCAL,)),
        ],
        compiler_params=pltpu.CompilerParams(
            collective_id=0, has_side_effects=True, vmem_limit_bytes=64 * 1024 * 1024 - 65536
        ),
    )(
        query_nope, turn(query_rope), packed, key_up, value_up, out_proj, residual, gains, taps,
        ffn_gate, ffn_value, ffn_down,
    )


def local(*arrays):
    rows, features = arrays[0].shape
    down_cols = arrays[15].shape[1]
    n_sp, n_tp = lax.axis_size("sp"), lax.axis_size("tp")
    paired = n_sp // 2
    fits = n_tp == 4 and paired == n_tp
    tiled = rows % LANES == 0 and down_cols % LANES == 0 and features == 2 * down_cols
    return (fused if fits and tiled else plain)(*arrays)


def solution(mesh):
    placed = (
        P("sp", "tp"),
        P("sp", "tp"),
        P("sp", "tp"),
        P("sp", None),
        P("sp", None),
        P("sp"),
        P(None, "tp"),
        P(None, "tp"),
        P("tp", None),
        P("tp"),
        P("tp"),
        P("sp", "tp"),
        P("sp", "tp"),
        P(None, "tp"),
        P(None, "tp"),
        P("tp", "sp"),
        P("tp"),
        P("tp"),
    )
    return jax.shard_map(
        local, mesh=mesh, in_specs=placed, out_specs=P("sp", "tp"), check_vma=False
    )
```

```python
import functools

import jax
import jax.numpy as jnp
from jax import lax
from jax.experimental import pallas as pl
from jax.experimental.pallas import tpu as pltpu
from jax.sharding import PartitionSpec as P

D = 2048
NOPE = 128
ROPE = 64
VDIM = 128
CONV = 3
REACH = 3


norm_eps = 1e-05
residual_scale = 8.0**0.25
rope_base_freq = 10000.0
masked_score = -1e30


def passed_along(value, axis, by):
    count = lax.axis_size(axis)
    pairs = [(i, i + by) for i in range(count) if 0 <= i + by < count]
    return lax.ppermute(value, axis, pairs)


def tables(positions):
    frequencies = 1.0 / rope_base_freq ** (jnp.arange(0, ROPE, 2, dtype=jnp.float32) / ROPE)
    angles = positions.astype(jnp.float32)[:, None] * frequencies[None, :]
    return (jnp.cos(angles), jnp.sin(angles))


def rotate(vectors, cosine, sine_table):
    half_width = vectors.shape[-1] // 2
    front_half = vectors[..., :half_width]
    back_half = vectors[..., half_width:]
    return jnp.concatenate(
        [
            front_half * cosine - back_half * sine_table,
            front_half * sine_table + back_half * cosine,
        ],
        axis=-1,
    )


def ring_blocks(block, axis):
    count = lax.axis_size(axis)
    order = list(range(0, count, 2)) + list(range(1, count, 2))[::-1]
    place = [order.index(i) for i in range(count)]
    me = lax.axis_index(axis)
    found = [(me, block)]
    ahead = count // 2
    for turn, steps in ((1, ahead), (-1, count - 1 - ahead)):
        pairs = [(order[p], order[(p + turn) % count]) for p in range(count)]
        moving = block
        for step in range(1, steps + 1):
            moving = lax.ppermute(moving, axis, pairs)
            owners = [order[(place[i] - turn * step) % count] for i in range(count)]
            found.append((jnp.asarray(owners, jnp.int32)[me], moving))
    return found


def attend_kernel(chunk, reach_rows, scale, q_ref, turned_ref, k_ref, rope_ref, v_ref, bias_ref, out_ref):
    rows = q_ref.shape[0]
    span = chunk + reach_rows
    rope_rows = rope_ref[...]
    for head in range(q_ref.shape[1] // NOPE):
        nope = slice(head * NOPE, (head + 1) * NOPE)
        rope = slice(head * ROPE, (head + 1) * ROPE)
        queries = jnp.concatenate([q_ref[:, nope], turned_ref[:, rope]], 1)
        keys = jnp.concatenate([k_ref[:, nope], rope_rows], 1)
        for start in range(0, rows, chunk):
            cut = slice(start, start + chunk)
            seen = slice(start, start + span)
            scores = lax.dot_general(
                queries[cut], keys[seen], (((1,), (1,)), ((), ())), preferred_element_type=jnp.float32
            )
            scores = scores * scale + bias_ref[cut, seen]
            weights = jnp.exp(scores - jnp.max(scores, -1, keepdims=True))
            weights = weights * (1.0 / jnp.sum(weights, -1, keepdims=True))
            out_ref[cut, nope] = jnp.dot(
                weights.astype(jnp.bfloat16), v_ref[seen, nope], preferred_element_type=jnp.float32
            ).astype(jnp.bfloat16)


def attend(queries, turned, keys, rope_rows, values, bias, scale):
    rows, width = queries.shape
    window = keys.shape[0]
    chunk = 128 if rows % 128 == 0 else rows
    pair = 2
    wide = pair * NOPE
    heads = width // NOPE
    return pl.pallas_call(
        functools.partial(attend_kernel, chunk, window - rows, scale),
        grid=(heads // pair,),
        in_specs=[
            pl.BlockSpec((rows, wide), lambda i: (0, i)),
            pl.BlockSpec((rows, pair * ROPE), lambda i: (0, i)),
            pl.BlockSpec((window, wide), lambda i: (0, i)),
            pl.BlockSpec((window, ROPE), lambda i: (0, 0)),
            pl.BlockSpec((window, pair * VDIM), lambda i: (0, i)),
            pl.BlockSpec((rows, window), lambda i: (0, 0)),
        ],
        out_specs=pl.BlockSpec((rows, pair * VDIM), lambda i: (0, i)),
        out_shape=jax.ShapeDtypeStruct((rows, heads * VDIM), jnp.bfloat16),
        compiler_params=pltpu.CompilerParams(vmem_limit_bytes=40 * 1024 * 1024),
        cost_estimate=pl.CostEstimate(
            flops=16 * rows * window * heads * (NOPE + ROPE + VDIM),
            bytes_accessed=2 * (4 * rows * width + 2 * window * width),
            transcendentals=rows * window * heads,
        ),
    )(queries, turned, keys, rope_rows, values, bias)


def scatter_sum(terms, axis):
    count = lax.axis_size(axis)
    width = terms.shape[1] // count
    parts = jnp.stack([terms[:, i * width : (i + 1) * width] for i in range(count)])
    got = lax.all_to_all(parts.astype(jnp.bfloat16), axis, 0, 0)
    return jnp.sum(got.astype(jnp.float32), 0)


def finish(mixed, totals, gain_row, bias_row):
    row_mean = totals[0][:, None] / D
    row_power = totals[1][:, None] / D
    return (mixed - row_mean) * lax.rsqrt(
        row_power - row_mean * row_mean + norm_eps
    ) * gain_row.astype(jnp.float32) + bias_row.astype(jnp.float32)


def plain(
    residual,
    query_nope,
    query_rope,
    latent,
    rope_key,
    doc_ids,
    key_up,
    value_up,
    out_proj,
    norm1_gain,
    norm1_bias,
    ffn_gate,
    ffn_value,
    conv_gate,
    conv_value,
    ffn_down,
    norm2_gain,
    norm2_bias,
):
    row_count = latent.shape[0]
    head_count = query_nope.shape[1] // NOPE
    local_units = ffn_gate.shape[1]
    rim_rows = CONV - 1
    whole_gate = lax.all_gather(ffn_gate, "sp", axis=0, tiled=True)
    whole_value = lax.all_gather(ffn_value, "sp", axis=0, tiled=True)
    offset = lax.axis_index("sp") * row_count
    positions = offset + jnp.arange(row_count, dtype=jnp.int32)
    cosine, sine_table = tables(positions)
    turned_key = rotate(rope_key.astype(jnp.float32), cosine, sine_table).astype(jnp.bfloat16)
    turned_query = rotate(
        query_rope.astype(jnp.float32).reshape(row_count, head_count, ROPE),
        cosine[:, None],
        sine_table[:, None],
    ).astype(jnp.bfloat16)
    latent_width = latent.shape[1]
    packed = jnp.concatenate(
        [
            latent,
            turned_key,
            jnp.broadcast_to(doc_ids.astype(jnp.bfloat16)[:, None], (row_count, ROPE)),
        ],
        1,
    )
    parts = [passed_along(packed, "sp", shift_step) for shift_step in range(REACH, 0, -1)]
    pieces = jnp.concatenate(parts + [packed], 0)
    win_latent = pieces[:, :latent_width]
    win_key = pieces[:, latent_width : latent_width + ROPE]
    win_doc = pieces[:, latent_width + ROPE].astype(jnp.int32)
    down_blocks = ring_blocks(ffn_down, "sp")
    key_rows = jnp.dot(win_latent, key_up, preferred_element_type=jnp.float32).astype(jnp.bfloat16)
    values = jnp.dot(win_latent, value_up, preferred_element_type=jnp.float32).astype(jnp.bfloat16)
    window = key_rows.shape[0]
    key_pos = offset - REACH * row_count + jnp.arange(window, dtype=jnp.int32)
    allowed = (
        (key_pos[None, :] <= positions[:, None])
        & (key_pos[None, :] >= 0)
        & (win_doc[None, :] == doc_ids[:, None])
    )
    scale = (NOPE + ROPE) ** (-0.5)
    bias = jnp.where(allowed, 0.0, masked_score).astype(jnp.float32)
    attended = attend(
        query_nope,
        turned_query.reshape(row_count, head_count * ROPE),
        key_rows,
        win_key,
        values,
        bias,
        scale,
    )
    head_terms = jnp.dot(attended, out_proj, preferred_element_type=jnp.float32)
    projected = scatter_sum(head_terms, "tp")
    mixed_one = residual_scale * residual.astype(jnp.float32) + projected
    totals_one = lax.psum((jnp.sum(mixed_one, 1), jnp.sum(mixed_one * mixed_one, 1)), "tp")
    normed = finish(mixed_one, totals_one, norm1_gain, norm1_bias).astype(jnp.bfloat16)
    half = row_count // 2
    full_rows = jnp.concatenate(
        [
            lax.all_gather(normed[:half], "tp", axis=1, tiled=True),
            lax.all_gather(normed[half:], "tp", axis=1, tiled=True),
        ],
        0,
    )
    gate_sum = jnp.dot(full_rows, whole_gate, preferred_element_type=jnp.float32)
    value_sum = jnp.dot(full_rows, whole_value, preferred_element_type=jnp.float32)
    gate_pre = gate_sum.astype(jnp.bfloat16)
    value_pre = value_sum.astype(jnp.bfloat16)
    tail_gate, tail_value, tail_doc = passed_along(
        (
            gate_pre[row_count - rim_rows :],
            value_pre[row_count - rim_rows :],
            doc_ids[row_count - rim_rows :],
        ),
        "sp",
        1,
    )
    ext_gate = jnp.concatenate([tail_gate, gate_pre], 0)
    ext_value = jnp.concatenate([tail_value, value_pre], 0)
    ext_doc = jnp.concatenate([tail_doc, doc_ids], 0)
    gate_mix = jnp.zeros((row_count, local_units), jnp.float32)
    value_mix = jnp.zeros((row_count, local_units), jnp.float32)
    for tap_index in range(CONV):
        valid_tap = (
            (ext_doc[tap_index : tap_index + row_count] == doc_ids)
            & (positions - rim_rows + tap_index >= 0)
        ).astype(jnp.float32)[:, None]
        gate_mix = (
            gate_mix
            + conv_gate[tap_index].astype(jnp.float32)
            * ext_gate[tap_index : tap_index + row_count].astype(jnp.float32)
            * valid_tap
        )
        value_mix = (
            value_mix
            + conv_value[tap_index].astype(jnp.float32)
            * ext_value[tap_index : tap_index + row_count].astype(jnp.float32)
            * valid_tap
        )
    hidden = (value_mix * jax.nn.gelu(gate_mix)).astype(jnp.bfloat16)
    sp_count = lax.axis_size("sp")
    tp_count = lax.axis_size("tp")
    block_width = ffn_down.shape[1]
    unit_terms = jnp.zeros((sp_count, row_count, block_width), jnp.bfloat16)
    for owner, block in down_blocks:
        term = jnp.dot(hidden, block, preferred_element_type=jnp.float32).astype(jnp.bfloat16)
        unit_terms = lax.dynamic_update_slice(unit_terms, term[None], (owner, 0, 0))
    share = sp_count // tp_count
    got = lax.all_to_all(
        unit_terms.reshape(tp_count, share, row_count, block_width), "tp", 0, 0
    )
    ffn_blocks = jnp.sum(got.astype(jnp.float32), 0)
    ffn_out = jnp.concatenate([ffn_blocks[i] for i in range(share)], 1)
    mixed_two = residual_scale * normed.astype(jnp.float32) + ffn_out
    totals_two = lax.psum((jnp.sum(mixed_two, 1), jnp.sum(mixed_two * mixed_two, 1)), "tp")
    return finish(mixed_two, totals_two, norm2_gain, norm2_bias).astype(jnp.bfloat16)


LANES = 128
MESH = pl.DeviceIdType.MESH
log2_e = 1.4426950408889634


class Copies:
    def __init__(self, send_sems, recv_sems):
        self.send_sems, self.recv_sems = send_sems, recv_sems
        self.count = 0

    def ids(self, number=1):
        first = self.count
        self.count += number
        return first

    def make(self, index, source, target, sp, tp):
        return pltpu.make_async_remote_copy(
            src_ref=source,
            dst_ref=target,
            send_sem=self.send_sems.at[index],
            recv_sem=self.recv_sems.at[index],
            device_id={"sp": sp, "tp": tp},
            device_id_type=MESH,
        )


REMOTE = 160
LOCAL = 16


def flip(value, bits):
    for bit in range(bits.bit_length()):
        step = 1 << bit
        if bits & step:
            value = value + step - 2 * step * ((value // step) % 2)
    return value


def layer_kernel(
    sizes,
    q_in, t_in, latent_in, kup_in, vup_in, proj_in, resid_in, side_in, cosine, sine,
    gain1, bias1, gain2, bias2, conv_g, conv_v, gate_in, value_in, down_in,
    out_ref,
    taps, win, q_v, t_v, kup, vup, proj, resid, keys, vals, ropes, bias, att,
    core_out, core_in, keep, y_out, y_in, mix, stat_own, stat_in, valid,
    rows_all, gate_w, value_w, down_w, ext, hid,
    part2, core_in2, y_out2, y_in2, z_out2, z_in2, stat_own2, stat_in2,
    send_sems, recv_sems, local_sems,
):
    n_sp, n_tp, R, reach, heads, wide, first, second = sizes
    C = LANES
    F = resid.shape[1]
    chunks = R // C
    window = (reach + 1) * R
    span = C + reach * R
    latent_width = kup.shape[0]
    gate_rows = gate_in.shape[0]
    down_cols = down_in.shape[1]
    bf16, f32 = jnp.bfloat16, jnp.float32
    me_sp, me_tp = lax.axis_index("sp"), lax.axis_index("tp")
    x, z = me_sp % 2, me_sp // 2
    odd = z % 2
    y, c = me_tp // 2, me_tp % 2
    x_peer = me_sp + 1 - 2 * x
    c_peer = me_tp + 1 - 2 * c
    y_peer = me_tp + 2 - 4 * y
    far_peer = 3 - me_tp
    nz = n_sp // 2
    z_sp = [2 * flip(z, d) + x for d in range(nz)]
    pair = z_sp[1]
    rc = Copies(send_sems, recv_sems)
    sent = []

    def start(copy, when=None):
        if when is None:
            copy.start()
        else:
            pl.when(when)(copy.start)
        sent.append((copy, when))

    barrier = pltpu.get_barrier_semaphore()
    for i in range(n_sp):
        for j in range(n_tp):
            if i or j:
                pl.semaphore_signal(
                    barrier, inc=1,
                    device_id={"sp": (me_sp + i) % n_sp, "tp": (me_tp + j) % n_tp},
                    device_id_type=MESH,
                )

    loads = {}

    def load(name, source, target):
        loads[name] = pltpu.make_async_copy(source, target, local_sems.at[len(loads)])
        loads[name].start()

    load("win", latent_in, win.at[pl.ds(reach * R, R), pl.ds(0, latent_width)])
    load("kup", kup_in, kup)
    load("vup", vup_in, vup)
    load("q", q_in, q_v)
    load("t", t_in, t_v)
    load("proj", proj_in, proj)
    load("resid", resid_in, resid)

    place = lax.broadcasted_iota(jnp.int32, (R, LANES), 1)
    front = place % ROPE < ROPE // 2

    def turn(vectors):
        vectors = vectors.astype(f32)
        swapped = jnp.where(
            front,
            pltpu.roll(vectors, LANES - ROPE // 2, 1),
            pltpu.roll(vectors, ROPE // 2, 1),
        )
        return vectors * cosine[...] + swapped * sine[...]

    own_rows = slice(reach * R, (reach + 1) * R)
    win[own_rows, latent_width:] = jnp.where(
        place < ROPE, turn(side_in[...]), side_in[...].astype(f32)
    ).astype(bf16)
    with jax.named_scope("barrier"):
        pl.semaphore_wait(barrier, n_sp * n_tp - 1)

    part = R // n_tp
    halo = rc.ids(reach)
    halo_ids = rc.ids(3 * reach)

    def quarter(k, tp):
        return win.at[pl.ds(pl.multiple_of((reach - k) * R + tp * part, 16), part)]

    halo_side = rc.ids(reach)
    own_part = pl.multiple_of(me_tp * part, 16)

    def halo_copy(k):
        return rc.make(
            halo + k - 1, latent_in.at[pl.ds(own_part, part)],
            quarter(k, me_tp).at[:, pl.ds(0, latent_width)], me_sp + k, me_tp,
        )

    def halo_side_copy(k):
        lanes = pl.ds(latent_width, LANES)
        return rc.make(
            halo_side + k - 1, win.at[pl.ds(reach * R + own_part, part), lanes],
            quarter(k, me_tp).at[:, lanes], me_sp + k, me_tp,
        )

    def halo_pass(k, kind, tp, tp_to):
        rows = quarter(k, tp)
        return rc.make(halo_ids + 3 * (k - 1) + kind, rows, rows, me_sp, tp_to)

    for k in range(1, reach + 1):
        start(halo_copy(k), me_sp + k < n_sp)
        start(halo_side_copy(k), me_sp + k < n_sp)

    halves = ((0, first), (first, second))

    def half_in(w, parity):
        at, size = halves[parity]
        if w == 2:
            return down_in.at[pl.ds(at, size), :]
        return (gate_in, value_in)[w].at[:, pl.ds(at, size)]

    def half_slot(w, parity, owner):
        size = halves[parity][1]
        if w == 2:
            return down_w.at[owner, pl.ds(0, size), :]
        rows = pl.ds(pl.multiple_of(owner * gate_rows, 16), gate_rows)
        return (gate_w, value_w)[w].at[rows, pl.ds(0, size)]

    def by_parity(parity, act):
        for p in range(2):
            pl.when(parity == p)(functools.partial(act, p))

    z_ids = [rc.ids(nz) for _ in range(3)]
    x_ids = [rc.ids(nz) for _ in range(3)]
    own_ids = [len(loads) + w for w in range(3)]

    def own_weight(w, p):
        return pltpu.make_async_copy(half_in(w, p), half_slot(w, p, me_sp), local_sems.at[own_ids[w]])

    def z_weight(w, d, p):
        return rc.make(z_ids[w] + d, half_in(w, p), half_slot(w, p, me_sp), z_sp[d], me_tp)

    def z_landed(w, d, p):
        return rc.make(z_ids[w] + d, half_in(w, p), half_slot(w, p, z_sp[d]), z_sp[d], me_tp)

    def x_weight(w, d, p):
        source = half_in(w, p) if d == 0 else half_slot(w, p, z_sp[d])
        return rc.make(x_ids[w] + d, source, half_slot(w, p, z_sp[d]), x_peer, me_tp)

    def x_landed(w, d, p):
        slot = half_slot(w, p, z_sp[d] + 1 - 2 * x)
        return rc.make(x_ids[w] + d, slot, slot, x_peer, me_tp)

    def send_z(w, which):
        for d in which:
            by_parity((odd + d) % 2, lambda p, d=d: z_weight(w, d, p).start())

    def send_x(w, d):
        if d:
            by_parity(odd, lambda p: z_landed(w, d, p).wait_recv())
        by_parity(odd, lambda p: x_weight(w, d, p).start())

    def all_here(w):
        def act(p):
            own_weight(w, p).wait()
            for d in range(nz):
                x_landed(w, d, p).wait_recv()
        by_parity(odd, act)

    for w in range(3):
        by_parity(odd, lambda p, w=w: own_weight(w, p).start())
    middle, near = list(range(2, nz)), [1]
    rightward = 1 - z // (nz // 2)

    inner = odd == rightward
    outer = jnp.logical_not(inner)

    def first_weights(right):
        for w in range(2):
            pl.when((1 - odd) == right)(lambda w=w: send_z(w, near))
        pl.when(rightward == right)(lambda: send_z(0, middle))
        pl.when((rightward == right) & inner)(lambda: send_z(1, middle))
        pl.when((rightward == right) & inner)(lambda: send_z(2, middle[: len(middle) - right]))

    send_x(0, 0)
    send_x(1, 0)
    first_weights(0)

    @pl.when(odd == 1)
    def _():
        blank = first - second
        if blank:
            gate_w[:, second:] = jnp.zeros((gate_w.shape[0], blank), bf16)
            value_w[:, second:] = jnp.zeros((gate_w.shape[0], blank), bf16)
            down_w[:, second:, :] = jnp.zeros((n_sp, blank, down_cols), bf16)

    for conv, at in ((conv_g, 0), (conv_v, 8)):
        def pick_taps(p, conv=conv, at=at):
            first_unit, size = halves[p]
            taps[at : at + CONV, 0:size] = conv[:, first_unit : first_unit + size].astype(f32)
            if size < first:
                taps[at : at + CONV, size:] = jnp.zeros((CONV, first - size), f32)
        by_parity(odd, pick_taps)

    loads["win"].wait()
    loads["kup"].wait()
    loads["vup"].wait()

    def raise_rows(block):
        rows = pl.ds(pl.multiple_of(block * R, LANES), R)
        source = win[rows, :latent_width]
        keys[rows, :] = jnp.dot(source, kup[...], preferred_element_type=f32).astype(bf16)
        vals[rows, :] = jnp.dot(source, vup[...], preferred_element_type=f32).astype(bf16)

    with jax.named_scope("own_kv"):
        raise_rows(reach)
    loads["q"].wait()
    loads["t"].wait()
    for duo in range(heads // 2):
        cut = slice(duo * LANES, (duo + 1) * LANES)
        t_v[:, cut] = turn(t_v[:, cut]).astype(bf16)
    for k in range(1, reach + 1):
        @pl.when(me_sp >= k)
        def _(k=k):
            with jax.named_scope("halo_wait"):
                halo_copy(k).wait_recv()
                halo_side_copy(k).wait_recv()
            halo_pass(k, 0, me_tp, y_peer).start()
            halo_pass(k, 1, me_tp, c_peer).start()

        @pl.when(me_sp < k)
        def _(k=k):
            win[(reach - k) * R : (reach - k + 1) * R, :] = jnp.zeros((R, win.shape[1]), bf16)
        sent.append((halo_pass(k, 0, me_tp, y_peer), me_sp >= k))
        sent.append((halo_pass(k, 1, me_tp, c_peer), me_sp >= k))
    for k in range(1, reach + 1):
        @pl.when(me_sp >= k)
        def _(k=k):
            with jax.named_scope("halo_y_wait"):
                halo_pass(k, 0, y_peer, y_peer).wait_recv()
            halo_pass(k, 2, y_peer, c_peer).start()
        sent.append((halo_pass(k, 2, y_peer, c_peer), me_sp >= k))
    for k in range(1, reach + 1):
        @pl.when(me_sp >= k)
        def _(k=k):
            with jax.named_scope("halo_core_wait"):
                halo_pass(k, 1, c_peer, c_peer).wait_recv()
                halo_pass(k, 2, far_peer, c_peer).wait_recv()
    first_weights(1)

    with jax.named_scope("kv"):
        @pl.loop(0, reach)
        def _(block):
            raise_rows(block)

    side = win[:, latent_width:]
    side_f = side.astype(f32)
    lane = lax.broadcasted_iota(jnp.int32, (window, LANES), 1)
    low = lane < LANES // 2
    ropes[0] = jnp.where(low, side_f, 0.0).astype(bf16)
    ropes[1] = jnp.where(low, 0.0, pltpu.roll(side_f, LANES // 2, 1)).astype(bf16)
    pick = (
        (lax.broadcasted_iota(jnp.int32, (8, LANES), 1) == LANES // 2)
        .astype(f32)
        .astype(bf16)
    )
    key_doc = lax.dot_general(pick, side, (((1,), (1,)), ((), ())), preferred_element_type=f32)[0:1]
    for r in range(chunks):
        at = slice(r * C, (r + 1) * C)
        own_doc = side_f[reach * R + r * C : reach * R + (r + 1) * C, LANES // 2 : LANES // 2 + 1]
        key_at = lax.broadcasted_iota(jnp.int32, (C, window), 1) - reach * R
        row_at = lax.broadcasted_iota(jnp.int32, (C, window), 0) + r * C
        allowed = (key_at <= row_at) & (key_at + me_sp * R >= 0) & (key_doc == own_doc)
        bias[at, :] = jnp.where(allowed, 0.0, masked_score)

    tail = side_f[reach * R - 8 :]
    valid_id = rc.ids()
    row_no = lax.broadcasted_iota(jnp.int32, (R, LANES), 0) + me_sp * R
    here = tail[8:]
    back_one = (pltpu.roll(tail, 1, 0)[8:] == here) & (row_no >= 1)
    back_two = (pltpu.roll(tail, 2, 0)[8:] == here) & (row_no >= 2)
    lanes = lax.broadcasted_iota(jnp.int32, (R, LANES), 1)
    valid[odd] = jnp.where(
        lanes < 3 * LANES // 4, back_two.astype(f32), back_one.astype(f32)
    ).astype(bf16)
    start(rc.make(valid_id, valid.at[odd], valid.at[odd], pair, me_tp))

    scale = (NOPE + ROPE) ** (-0.5) * log2_e

    def attend_chunk(r):
        at, seen = slice(r * C, (r + 1) * C), slice(r * C, r * C + span)

        @pl.loop(0, heads // 2)
        def _(duo):
            turned = t_v[at, pl.ds(pl.multiple_of(duo * LANES, LANES), LANES)]
            for e in range(2):
                head = pl.ds(pl.multiple_of((2 * duo + e) * LANES, LANES), LANES)
                queries = jnp.concatenate([q_v[at, head], turned], 1)
                seen_keys = jnp.concatenate([keys[seen, head], ropes[e, seen, :]], 1)
                scores = lax.dot_general(
                    queries, seen_keys, (((1,), (1,)), ((), ())), preferred_element_type=f32
                )
                scores = scores * scale + bias[at, seen]
                weights = jnp.exp2(scores - jnp.max(scores, -1, keepdims=True))
                total = jnp.sum(weights, -1, keepdims=True)
                mixed = jnp.dot(weights.astype(bf16), vals[seen, head], preferred_element_type=f32)
                att[at, head] = (mixed * (1.0 / total)).astype(bf16)

    core_ids, y_ids = rc.ids(2 * chunks), rc.ids(chunks)
    stat_ids = rc.ids(3 * chunks)
    stat_ids2 = rc.ids(3 * chunks)
    gather_ids = rc.ids(8 * chunks)

    def to_core(r, i):
        return rc.make(core_ids + 2 * r + i, core_out.at[r, i], core_in.at[r, i], me_sp, c_peer)

    def to_y(r):
        return rc.make(y_ids + r, y_out.at[r], y_in.at[r], me_sp, y_peer)

    def features(tp):
        return pl.ds(pl.multiple_of(tp * F, LANES), F)

    def project(r):
        rows = att[r * C : (r + 1) * C, :]
        for i, yy in enumerate((1 - y, y)):
            core_out[r, i] = jnp.dot(
                rows, proj[:, features(2 * yy + 1 - c)], preferred_element_type=f32
            ).astype(bf16)
            start(to_core(r, i))
        for i, yy in enumerate((1 - y, y)):
            keep[r, i] = jnp.dot(
                rows, proj[:, features(2 * yy + c)], preferred_element_type=f32
            ).astype(bf16)
        to_core(r, 0).wait_recv()
        y_out[r] = (keep[r, 0].astype(f32) + core_in[r, 0].astype(f32)).astype(bf16)
        start(to_y(r))

    def stat_copy(ids, own, landed, r, i):
        return rc.make(ids + 3 * r + i, own.at[r], landed.at[r, i], me_sp, (c_peer, y_peer, far_peer)[i])

    def send_stats(values, ids, own, landed, r):
        one = jnp.sum(values, -1, keepdims=True)
        two = jnp.sum(values * values, -1, keepdims=True)
        lane = lax.broadcasted_iota(jnp.int32, (C, LANES), 1)
        own[r] = jnp.where(lane % 8 < 4, one, two).T[0:8]
        for i in (1, 2, 0):
            start(stat_copy(ids, own, landed, r, i))

    def norm(values, ids, own, landed, r, gain):
        for i in range(3):
            stat_copy(ids, own, landed, r, i).wait_recv()
        total = (own[r] + landed[r, 0]) + (landed[r, 1] + landed[r, 2])
        total = jnp.concatenate([total] * (LANES // 8), 0).T
        row_mean = total[:, 0:1] / wide
        row_power = total[:, 4:5] / wide
        return (values - row_mean) * lax.rsqrt(row_power - row_mean * row_mean + norm_eps) * gain[0][
            ...
        ].astype(f32)[None, :] + gain[1][...].astype(f32)[None, :]

    def mix_one(r):
        at = slice(r * C, (r + 1) * C)
        to_core(r, 1).wait_recv()
        to_y(r).wait_recv()
        mixed = residual_scale * resid[at, :].astype(f32) + (
            keep[r, 1].astype(f32) + core_in[r, 1].astype(f32) + y_in[r].astype(f32)
        )
        mix[at, :] = mixed
        send_stats(mixed, stat_ids, stat_own, stat_in, r)

    def gathered(r, kind, slot, tp, sp_to, tp_to):
        spot = rows_all.at[slot, pl.ds(r * C, C), features(tp)]
        return rc.make(gather_ids + 8 * r + kind, spot, spot, sp_to, tp_to)

    def to_pair(r, slot):
        return gathered(r, 0, slot, me_tp, pair, me_tp)

    def core_gather(r, kind, slot, tp):
        return gathered(r, kind, slot, tp, me_sp, c_peer)

    def y_gather(r, kind, slot, tp):
        return gathered(r, kind, slot, tp, me_sp, y_peer)

    def norm_one(r):
        at = slice(r * C, (r + 1) * C)
        rows_all[odd, at, features(me_tp)] = norm(
            mix[at, :], stat_ids, stat_own, stat_in, r, (gain1, bias1)
        ).astype(bf16)
        start(to_pair(r, odd))
        start(y_gather(r, 1, odd, me_tp))
        start(core_gather(r, 2, odd, me_tp))

    def pass_pair(r):
        to_pair(r, 1 - odd).wait_recv()
        start(y_gather(r, 3, 1 - odd, me_tp))
        start(core_gather(r, 4, 1 - odd, me_tp))

    def pass_y(r):
        for kind, got, slot in ((5, 1, odd), (6, 3, 1 - odd)):
            y_gather(r, got, slot, y_peer).wait_recv()
            start(core_gather(r, kind, slot, y_peer))

    def rows_here(r):
        core_gather(r, 2, odd, c_peer).wait_recv()
        core_gather(r, 4, 1 - odd, c_peer).wait_recv()
        core_gather(r, 5, odd, far_peer).wait_recv()
        core_gather(r, 6, 1 - odd, far_peer).wait_recv()

    def z_left(w, d):
        by_parity((odd + d) % 2, lambda p: z_weight(w, d, p).wait_send())

    def forward(w, which):
        for d in which:
            with jax.named_scope("fwd%d_%d" % (w, d)):
                send_x(w, d)

    def attend_step(r):
        with jax.named_scope("att"):
            attend_chunk(r)
        if r == 0:
            loads["proj"].wait()
            loads["resid"].wait()
        else:
            with jax.named_scope("mix"):
                mix_one(r - 1)
        with jax.named_scope("proj"):
            project(r)
        if r:
            with jax.named_scope("norm"):
                norm_one(r - 1)

    for r in range(chunks):
        attend_step(r)
        if r == 0:
            pl.when(outer)(lambda: send_z(1, middle))
            forward(0, near)
            send_x(2, 0)
        elif r == 1:
            forward(1, near)
    forward(0, middle)
    with jax.named_scope("mix"):
        mix_one(chunks - 1)
    with jax.named_scope("norm"):
        norm_one(chunks - 1)
    send_z(2, near)
    forward(1, middle[:-1])
    with jax.named_scope("pass_pair"):
        for r in range(chunks):
            pass_pair(r)
    with jax.named_scope("pass_y"):
        for r in range(chunks):
            pass_y(r)
    forward(1, middle[-1:])
    with jax.named_scope("rows_here"):
        for r in range(chunks):
            rows_here(r)

    tile = 2 * LANES
    mid = first

    def up(weights, base):
        @pl.loop(0, 2)
        def _(slot):
            @pl.loop(0, first // tile)
            def _(j):
                cols = pl.multiple_of(j * tile, LANES)
                ext[slot, 8:, pl.ds(base + cols, tile)] = (
                    jnp.dot(rows_all[slot], weights[:, pl.ds(cols, tile)], preferred_element_type=f32)
                    .astype(bf16)
                    .astype(f32)
                )

    pl.when(outer & (rightward == 0))(lambda: send_z(2, middle))
    with jax.named_scope("wait_g"):
        all_here(0)
    with jax.named_scope("up_g"):
        up(gate_w, 0)
    forward(2, near)
    with jax.named_scope("wait_v"):
        all_here(1)
    pl.when(outer & (rightward == 1))(lambda: send_z(2, middle))
    with jax.named_scope("up_v"):
        up(value_w, mid)

    tail_ids = rc.ids(2)

    def tail_copy(slot, to_slot, sp):
        return rc.make(
            tail_ids + to_slot, ext.at[slot, pl.ds(R, 8)], ext.at[to_slot, pl.ds(0, 8)], sp, me_tp
        )

    last_pair = z >= nz - 2
    start(tail_copy(0, 0, x_peer), x == 0)
    start(tail_copy(1, 1, x_peer), x == 0)
    start(tail_copy(0, 1, x_peer), x == 1)
    start(tail_copy(1, 0, me_sp + 3), (x == 1) & (z < nz - 2))
    pl.when(inner & (rightward == 1))(lambda: send_z(2, middle[-1:]))

    @pl.when((x == 0) & (z < 2))
    def _():
        ext[0, 0:8, :] = jnp.zeros((8, ext.shape[2]), f32)

    deep = 64

    def convolve(first_step, steps):
        @pl.loop(0, 2)
        def _(slot):
            @pl.loop(first_step, first_step + steps)
            def _(i):
                at = pl.multiple_of(i * deep, 16)
                marks = valid[slot, pl.ds(at, deep), :].astype(f32)
                two, one = marks[:, LANES // 2 : LANES // 2 + 1], marks[:, LANES - 1 : LANES]

                @pl.loop(0, first // tile)
                def _(j):
                    cols = pl.multiple_of(j * tile, LANES)

                    def mixing(base, tap):
                        rows = ext[slot, pl.ds(at, deep + 8), pl.ds(base + cols, tile)]
                        weight = taps[pl.ds(tap, 8), pl.ds(cols, tile)]
                        return (
                            weight[0:1] * (pltpu.roll(rows, 2, 0)[8:] * two)
                            + weight[1:2] * (pltpu.roll(rows, 1, 0)[8:] * one)
                            + weight[2:3] * rows[8:]
                        )

                    hid[slot, pl.ds(at, deep), pl.ds(cols, tile)] = (
                        mixing(mid, 8) * jax.nn.gelu(mixing(0, 0))
                    ).astype(bf16)

    rc.make(valid_id, valid.at[1 - odd], valid.at[1 - odd], pair, me_tp).wait_recv()
    with jax.named_scope("conv"):
        convolve(1, R // deep - 1)
    forward(2, middle[:-1])
    with jax.named_scope("tails"):
        @pl.when((x == 1) | (z >= 2))
        def _():
            tail_copy(0, 0, x_peer).wait_recv()
        tail_copy(1, 1, x_peer).wait_recv()
    with jax.named_scope("conv_first"):
        convolve(0, 1)

    core_ids2, z_ids2, y_ids2 = rc.ids(4), rc.ids(2 * chunks), rc.ids(chunks)
    per = F // down_cols
    half_z = (z // 2) % 2
    slots = (1 - odd, odd)

    def to_core2(d, s):
        f = d // 2
        return rc.make(
            core_ids2 + 2 * f + s, part2.at[d, s], core_in2.at[f, s], me_sp, c_peer
        )

    def to_pair2(f, r):
        at = pl.ds(r * C, C)
        return rc.make(z_ids2 + chunks * f + r, z_out2.at[f, at], z_in2.at[f, at], pair, me_tp)

    def to_y2(r):
        at = pl.ds(r * C, C)
        return rc.make(y_ids2 + r, y_out2.at[at], y_in2.at[at], me_sp, y_peer)

    def down_block(d):
        f, block = d // 2, flip(z, d)
        with jax.named_scope("wait_d%d" % d):
            if d == 0:
                by_parity(odd, lambda p: own_weight(2, p).wait())
            by_parity(odd, lambda p: x_landed(2, d, p).wait_recv())
        with jax.named_scope("down"):
            for s in range(2):
                for j in range(per):
                    part2[d, s, :, j * down_cols : (j + 1) * down_cols] = jnp.dot(
                        hid[slots[s]], down_w[per * block + j], preferred_element_type=f32
                    ).astype(bf16)
                start(to_core2(d, s), block % 2 != c)

    def pair_block(d):
        f, block = d // 2, flip(z, d)

        @pl.when(block % 2 == c)
        def _():
            with jax.named_scope("core2_wait"):
                to_core2(d, 0).wait_recv()
            for r in range(chunks):
                at = slice(r * C, (r + 1) * C)
                z_out2[f, at, :] = (
                    part2[d, 0, at, :].astype(f32) + core_in2[f, 0, at, :].astype(f32)
                ).astype(bf16)
                to_pair2(f, r).start()
            with jax.named_scope("core2_wait"):
                to_core2(d, 1).wait_recv()

    def mine_of(f):
        return 2 * f + (odd + c) % 2

    def pass_down(f):
        yy = half_z if f == 0 else 1 - half_z
        for r in range(chunks):
            at = slice(r * C, (r + 1) * C)
            with jax.named_scope("z2_wait"):
                to_pair2(f, r).wait_recv()
            sent.append((to_pair2(f, r), None))

            @pl.when(y != yy)
            def _():
                y_out2[at, :] = (
                    part2[mine_of(f), 1, pl.ds(r * C, C), :].astype(f32)
                    + core_in2[f, 1, at, :].astype(f32)
                    + z_in2[f, at, :].astype(f32)
                ).astype(bf16)
                to_y2(r).start()

    down_block(0)
    down_block(1)
    pair_block(0)
    pair_block(1)
    forward(2, middle[-1:])
    down_block(2)
    pass_down(0)
    pair_block(2)
    down_block(3)
    pair_block(3)
    pass_down(1)
    mine = (y + half_z) % 2
    for r in range(chunks):
        at = slice(r * C, (r + 1) * C)
        rows = pl.ds(r * C, C)
        with jax.named_scope("y2_wait"):
            to_y2(r).wait_recv()
        sent.append((to_y2(r), None))
        mixed = residual_scale * rows_all[odd, at, features(me_tp)].astype(f32) + (
            part2[mine_of(mine), 1, rows, :].astype(f32)
            + core_in2[mine, 1, rows, :].astype(f32)
            + z_in2[mine, rows, :].astype(f32)
            + y_in2[at, :].astype(f32)
        )
        mix[at, :] = mixed
        send_stats(mixed, stat_ids2, stat_own2, stat_in2, r)
    with jax.named_scope("norm2"):
        for r in range(chunks):
            at = slice(r * C, (r + 1) * C)
            out_ref[at, :] = norm(mix[at, :], stat_ids2, stat_own2, stat_in2, r, (gain2, bias2)).astype(bf16)

    for copy, when in sent:
        if when is None:
            copy.wait_send()
        else:
            pl.when(when)(copy.wait_send)
    for w in range(3):
        for d in range(nz):
            if d:
                z_left(w, d)
            by_parity(odd, lambda p, d=d, w=w: x_weight(w, d, p).wait_send())
    assert rc.count <= REMOTE, rc.count


def fused(
    residual, query_nope, query_rope, latent, rope_key, doc_ids, key_up, value_up, out_proj,
    norm1_gain, norm1_bias, ffn_gate, ffn_value, conv_gate, conv_value, ffn_down, norm2_gain, norm2_bias,
):
    n_sp, n_tp = lax.axis_size("sp"), lax.axis_size("tp")
    R, F = residual.shape
    heads = query_nope.shape[1] // NOPE
    units = ffn_gate.shape[1]
    first = -(-units // (2 * LANES)) * LANES
    second = units - first
    window = (REACH + 1) * R
    chunks = R // LANES
    f32, bf16 = jnp.float32, jnp.bfloat16
    offset = lax.axis_index("sp") * R
    positions = offset + jnp.arange(R, dtype=jnp.int32)
    half = ROPE // 2
    place = jnp.arange(LANES, dtype=jnp.int32) % half
    frequencies = 1.0 / rope_base_freq ** (2.0 * place.astype(f32) / ROPE)
    angles = positions.astype(f32)[:, None] * frequencies[None, :]
    front = jnp.arange(LANES) % ROPE < half
    cosine, sine = jnp.cos(angles), jnp.where(front, -1.0, 1.0) * jnp.sin(angles)
    side = jnp.concatenate(
        [rope_key, jnp.broadcast_to(doc_ids.astype(bf16)[:, None], (R, LANES - ROPE))], 1
    )
    hbm = pl.BlockSpec(memory_space=pl.ANY)
    vmem = pl.BlockSpec(memory_space=pltpu.VMEM)
    sizes = (n_sp, n_tp, R, REACH, heads, n_tp * F, first, second)

    def v(*shape, dtype=bf16):
        return pltpu.VMEM(shape, dtype)

    C = LANES
    return pl.pallas_call(
        functools.partial(layer_kernel, sizes),
        in_specs=[hbm] * 7 + [vmem] * 9 + [hbm] * 3,
        out_specs=vmem,
        out_shape=jax.ShapeDtypeStruct((R, F), bf16),
        scratch_shapes=[
            v(16, first, dtype=f32), v(window, latent.shape[1] + LANES), v(R, heads * NOPE), v(R, heads * ROPE),
            v(*key_up.shape), v(*value_up.shape), v(*out_proj.shape), v(R, F),
            v(window, heads * NOPE), v(window, heads * VDIM), v(2, window, LANES),
            v(R, window, dtype=f32), v(R, heads * VDIM),
            v(chunks, 2, C, F), v(chunks, 2, C, F), v(chunks, 2, C, F), v(chunks, C, F), v(chunks, C, F),
            v(R, F, dtype=f32), v(chunks, 8, LANES, dtype=f32), v(chunks, 3, 8, LANES, dtype=f32),
            v(2, R, LANES),
            v(2, R, n_tp * F), v(n_sp * ffn_gate.shape[0], first), v(n_sp * ffn_gate.shape[0], first),
            v(n_sp, first, ffn_down.shape[1]), v(2, R + 8, 2 * first, dtype=f32), v(2, R, first),
            v(4, 2, R, F), v(2, 2, R, F), v(R, F), v(R, F), v(2, R, F), v(2, R, F),
            v(chunks, 8, LANES, dtype=f32), v(chunks, 3, 8, LANES, dtype=f32),
            pltpu.SemaphoreType.DMA((REMOTE,)), pltpu.SemaphoreType.DMA((REMOTE,)),
            pltpu.SemaphoreType.DMA((LOCAL,)),
        ],
        compiler_params=pltpu.CompilerParams(
            collective_id=0, has_side_effects=True, vmem_limit_bytes=64 * 1024 * 1024 - 65536
        ),
    )(
        query_nope, query_rope, latent, key_up, value_up, out_proj, residual, side, cosine, sine,
        norm1_gain, norm1_bias, norm2_gain, norm2_bias,
        conv_gate, conv_value, ffn_gate, ffn_value, ffn_down,
    )


def local(*arrays):
    rows, features = arrays[0].shape
    down_cols = arrays[15].shape[1]
    n_sp, n_tp = lax.axis_size("sp"), lax.axis_size("tp")
    paired = n_sp // 2
    fits = n_tp == 4 and paired == n_tp
    tiled = rows % LANES == 0 and down_cols % LANES == 0 and features == 2 * down_cols
    return (fused if fits and tiled else plain)(*arrays)


def solution(mesh):
    placed = (
        P("sp", "tp"),
        P("sp", "tp"),
        P("sp", "tp"),
        P("sp", None),
        P("sp", None),
        P("sp"),
        P(None, "tp"),
        P(None, "tp"),
        P("tp", None),
        P("tp"),
        P("tp"),
        P("sp", "tp"),
        P("sp", "tp"),
        P(None, "tp"),
        P(None, "tp"),
        P("tp", "sp"),
        P("tp"),
        P("tp"),
    )
    return jax.shard_map(
        local, mesh=mesh, in_specs=placed, out_specs=P("sp", "tp"), check_vma=False
    )
```

```python
import functools

import jax
import jax.numpy as jnp
from jax import lax
from jax.experimental import pallas as pl
from jax.experimental.pallas import tpu as pltpu
from jax.sharding import PartitionSpec as P

D = 2048
NOPE = 128
ROPE = 64
VDIM = 128
CONV = 3
REACH = 3


norm_eps = 1e-05
residual_scale = 8.0**0.25
rope_base_freq = 10000.0
masked_score = -1e30


def passed_along(value, axis, by):
    count = lax.axis_size(axis)
    pairs = [(i, i + by) for i in range(count) if 0 <= i + by < count]
    return lax.ppermute(value, axis, pairs)


def tables(positions):
    frequencies = 1.0 / rope_base_freq ** (jnp.arange(0, ROPE, 2, dtype=jnp.float32) / ROPE)
    angles = positions.astype(jnp.float32)[:, None] * frequencies[None, :]
    return (jnp.cos(angles), jnp.sin(angles))


def rotate(vectors, cosine, sine_table):
    half_width = vectors.shape[-1] // 2
    front_half = vectors[..., :half_width]
    back_half = vectors[..., half_width:]
    return jnp.concatenate(
        [
            front_half * cosine - back_half * sine_table,
            front_half * sine_table + back_half * cosine,
        ],
        axis=-1,
    )


def ring_blocks(block, axis):
    count = lax.axis_size(axis)
    order = list(range(0, count, 2)) + list(range(1, count, 2))[::-1]
    place = [order.index(i) for i in range(count)]
    me = lax.axis_index(axis)
    found = [(me, block)]
    ahead = count // 2
    for turn, steps in ((1, ahead), (-1, count - 1 - ahead)):
        pairs = [(order[p], order[(p + turn) % count]) for p in range(count)]
        moving = block
        for step in range(1, steps + 1):
            moving = lax.ppermute(moving, axis, pairs)
            owners = [order[(place[i] - turn * step) % count] for i in range(count)]
            found.append((jnp.asarray(owners, jnp.int32)[me], moving))
    return found


def attend_kernel(chunk, reach_rows, scale, q_ref, turned_ref, k_ref, rope_ref, v_ref, bias_ref, out_ref):
    rows = q_ref.shape[0]
    span = chunk + reach_rows
    rope_rows = rope_ref[...]
    for head in range(q_ref.shape[1] // NOPE):
        nope = slice(head * NOPE, (head + 1) * NOPE)
        rope = slice(head * ROPE, (head + 1) * ROPE)
        queries = jnp.concatenate([q_ref[:, nope], turned_ref[:, rope]], 1)
        keys = jnp.concatenate([k_ref[:, nope], rope_rows], 1)
        for start in range(0, rows, chunk):
            cut = slice(start, start + chunk)
            seen = slice(start, start + span)
            scores = lax.dot_general(
                queries[cut], keys[seen], (((1,), (1,)), ((), ())), preferred_element_type=jnp.float32
            )
            scores = scores * scale + bias_ref[cut, seen]
            weights = jnp.exp(scores - jnp.max(scores, -1, keepdims=True))
            weights = weights * (1.0 / jnp.sum(weights, -1, keepdims=True))
            out_ref[cut, nope] = jnp.dot(
                weights.astype(jnp.bfloat16), v_ref[seen, nope], preferred_element_type=jnp.float32
            ).astype(jnp.bfloat16)


def attend(queries, turned, keys, rope_rows, values, bias, scale):
    rows, width = queries.shape
    window = keys.shape[0]
    chunk = 128 if rows % 128 == 0 else rows
    pair = 2
    wide = pair * NOPE
    heads = width // NOPE
    return pl.pallas_call(
        functools.partial(attend_kernel, chunk, window - rows, scale),
        grid=(heads // pair,),
        in_specs=[
            pl.BlockSpec((rows, wide), lambda i: (0, i)),
            pl.BlockSpec((rows, pair * ROPE), lambda i: (0, i)),
            pl.BlockSpec((window, wide), lambda i: (0, i)),
            pl.BlockSpec((window, ROPE), lambda i: (0, 0)),
            pl.BlockSpec((window, pair * VDIM), lambda i: (0, i)),
            pl.BlockSpec((rows, window), lambda i: (0, 0)),
        ],
        out_specs=pl.BlockSpec((rows, pair * VDIM), lambda i: (0, i)),
        out_shape=jax.ShapeDtypeStruct((rows, heads * VDIM), jnp.bfloat16),
        compiler_params=pltpu.CompilerParams(vmem_limit_bytes=40 * 1024 * 1024),
        cost_estimate=pl.CostEstimate(
            flops=16 * rows * window * heads * (NOPE + ROPE + VDIM),
            bytes_accessed=2 * (4 * rows * width + 2 * window * width),
            transcendentals=rows * window * heads,
        ),
    )(queries, turned, keys, rope_rows, values, bias)


def scatter_sum(terms, axis):
    count = lax.axis_size(axis)
    width = terms.shape[1] // count
    parts = jnp.stack([terms[:, i * width : (i + 1) * width] for i in range(count)])
    got = lax.all_to_all(parts.astype(jnp.bfloat16), axis, 0, 0)
    return jnp.sum(got.astype(jnp.float32), 0)


def finish(mixed, totals, gain_row, bias_row):
    row_mean = totals[0][:, None] / D
    row_power = totals[1][:, None] / D
    return (mixed - row_mean) * lax.rsqrt(
        row_power - row_mean * row_mean + norm_eps
    ) * gain_row.astype(jnp.float32) + bias_row.astype(jnp.float32)


def plain(
    residual,
    query_nope,
    query_rope,
    latent,
    rope_key,
    doc_ids,
    key_up,
    value_up,
    out_proj,
    norm1_gain,
    norm1_bias,
    ffn_gate,
    ffn_value,
    conv_gate,
    conv_value,
    ffn_down,
    norm2_gain,
    norm2_bias,
):
    row_count = latent.shape[0]
    head_count = query_nope.shape[1] // NOPE
    local_units = ffn_gate.shape[1]
    rim_rows = CONV - 1
    whole_gate = lax.all_gather(ffn_gate, "sp", axis=0, tiled=True)
    whole_value = lax.all_gather(ffn_value, "sp", axis=0, tiled=True)
    offset = lax.axis_index("sp") * row_count
    positions = offset + jnp.arange(row_count, dtype=jnp.int32)
    cosine, sine_table = tables(positions)
    turned_key = rotate(rope_key.astype(jnp.float32), cosine, sine_table).astype(jnp.bfloat16)
    turned_query = rotate(
        query_rope.astype(jnp.float32).reshape(row_count, head_count, ROPE),
        cosine[:, None],
        sine_table[:, None],
    ).astype(jnp.bfloat16)
    latent_width = latent.shape[1]
    packed = jnp.concatenate(
        [
            latent,
            turned_key,
            jnp.broadcast_to(doc_ids.astype(jnp.bfloat16)[:, None], (row_count, ROPE)),
        ],
        1,
    )
    parts = [passed_along(packed, "sp", shift_step) for shift_step in range(REACH, 0, -1)]
    pieces = jnp.concatenate(parts + [packed], 0)
    win_latent = pieces[:, :latent_width]
    win_key = pieces[:, latent_width : latent_width + ROPE]
    win_doc = pieces[:, latent_width + ROPE].astype(jnp.int32)
    down_blocks = ring_blocks(ffn_down, "sp")
    key_rows = jnp.dot(win_latent, key_up, preferred_element_type=jnp.float32).astype(jnp.bfloat16)
    values = jnp.dot(win_latent, value_up, preferred_element_type=jnp.float32).astype(jnp.bfloat16)
    window = key_rows.shape[0]
    key_pos = offset - REACH * row_count + jnp.arange(window, dtype=jnp.int32)
    allowed = (
        (key_pos[None, :] <= positions[:, None])
        & (key_pos[None, :] >= 0)
        & (win_doc[None, :] == doc_ids[:, None])
    )
    scale = (NOPE + ROPE) ** (-0.5)
    bias = jnp.where(allowed, 0.0, masked_score).astype(jnp.float32)
    attended = attend(
        query_nope,
        turned_query.reshape(row_count, head_count * ROPE),
        key_rows,
        win_key,
        values,
        bias,
        scale,
    )
    head_terms = jnp.dot(attended, out_proj, preferred_element_type=jnp.float32)
    projected = scatter_sum(head_terms, "tp")
    mixed_one = residual_scale * residual.astype(jnp.float32) + projected
    totals_one = lax.psum((jnp.sum(mixed_one, 1), jnp.sum(mixed_one * mixed_one, 1)), "tp")
    normed = finish(mixed_one, totals_one, norm1_gain, norm1_bias).astype(jnp.bfloat16)
    half = row_count // 2
    full_rows = jnp.concatenate(
        [
            lax.all_gather(normed[:half], "tp", axis=1, tiled=True),
            lax.all_gather(normed[half:], "tp", axis=1, tiled=True),
        ],
        0,
    )
    gate_sum = jnp.dot(full_rows, whole_gate, preferred_element_type=jnp.float32)
    value_sum = jnp.dot(full_rows, whole_value, preferred_element_type=jnp.float32)
    gate_pre = gate_sum.astype(jnp.bfloat16)
    value_pre = value_sum.astype(jnp.bfloat16)
    tail_gate, tail_value, tail_doc = passed_along(
        (
            gate_pre[row_count - rim_rows :],
            value_pre[row_count - rim_rows :],
            doc_ids[row_count - rim_rows :],
        ),
        "sp",
        1,
    )
    ext_gate = jnp.concatenate([tail_gate, gate_pre], 0)
    ext_value = jnp.concatenate([tail_value, value_pre], 0)
    ext_doc = jnp.concatenate([tail_doc, doc_ids], 0)
    gate_mix = jnp.zeros((row_count, local_units), jnp.float32)
    value_mix = jnp.zeros((row_count, local_units), jnp.float32)
    for tap_index in range(CONV):
        valid_tap = (
            (ext_doc[tap_index : tap_index + row_count] == doc_ids)
            & (positions - rim_rows + tap_index >= 0)
        ).astype(jnp.float32)[:, None]
        gate_mix = (
            gate_mix
            + conv_gate[tap_index].astype(jnp.float32)
            * ext_gate[tap_index : tap_index + row_count].astype(jnp.float32)
            * valid_tap
        )
        value_mix = (
            value_mix
            + conv_value[tap_index].astype(jnp.float32)
            * ext_value[tap_index : tap_index + row_count].astype(jnp.float32)
            * valid_tap
        )
    hidden = (value_mix * jax.nn.gelu(gate_mix)).astype(jnp.bfloat16)
    sp_count = lax.axis_size("sp")
    tp_count = lax.axis_size("tp")
    block_width = ffn_down.shape[1]
    unit_terms = jnp.zeros((sp_count, row_count, block_width), jnp.bfloat16)
    for owner, block in down_blocks:
        term = jnp.dot(hidden, block, preferred_element_type=jnp.float32).astype(jnp.bfloat16)
        unit_terms = lax.dynamic_update_slice(unit_terms, term[None], (owner, 0, 0))
    share = sp_count // tp_count
    got = lax.all_to_all(
        unit_terms.reshape(tp_count, share, row_count, block_width), "tp", 0, 0
    )
    ffn_blocks = jnp.sum(got.astype(jnp.float32), 0)
    ffn_out = jnp.concatenate([ffn_blocks[i] for i in range(share)], 1)
    mixed_two = residual_scale * normed.astype(jnp.float32) + ffn_out
    totals_two = lax.psum((jnp.sum(mixed_two, 1), jnp.sum(mixed_two * mixed_two, 1)), "tp")
    return finish(mixed_two, totals_two, norm2_gain, norm2_bias).astype(jnp.bfloat16)


LANES = 128
MESH = pl.DeviceIdType.MESH
log2_e = 1.4426950408889634


class Copies:
    def __init__(self, send_sems, recv_sems):
        self.send_sems, self.recv_sems = send_sems, recv_sems
        self.count = 0

    def ids(self, number=1):
        first = self.count
        self.count += number
        return first

    def make(self, index, source, target, sp, tp):
        return pltpu.make_async_remote_copy(
            src_ref=source,
            dst_ref=target,
            send_sem=self.send_sems.at[index],
            recv_sem=self.recv_sems.at[index],
            device_id={"sp": sp, "tp": tp},
            device_id_type=MESH,
        )


REMOTE = 160
LOCAL = 16


def flip(value, bits):
    for bit in range(bits.bit_length()):
        step = 1 << bit
        if bits & step:
            value = value + step - 2 * step * ((value // step) % 2)
    return value


def layer_kernel(
    sizes,
    q_in, t_in, latent_in, kup_in, vup_in, proj_in, resid_in, rope_in, doc_in, cosine, sine,
    gain1, bias1, gain2, bias2, conv_g, conv_v, gate_in, value_in, down_in,
    out_ref,
    side_v, taps, win, q_v, t_v, kup, vup, proj, resid, keys, vals, ropes, bias, att,
    core_out, core_in, keep, y_out, y_in, mix, stat_own, stat_in, valid,
    rows_all, gate_w, value_w, down_w, ext, hid,
    part2, core_in2, y_out2, y_in2, z_out2, z_in2, stat_own2, stat_in2,
    send_sems, recv_sems, local_sems,
):
    n_sp, n_tp, R, reach, heads, wide, first, second = sizes
    C = LANES
    F = resid.shape[1]
    chunks = R // C
    window = (reach + 1) * R
    span = C + reach * R
    latent_width = kup.shape[0]
    gate_rows = gate_in.shape[0]
    down_cols = down_in.shape[1]
    bf16, f32 = jnp.bfloat16, jnp.float32
    me_sp, me_tp = lax.axis_index("sp"), lax.axis_index("tp")
    x, z = me_sp % 2, me_sp // 2
    odd = z % 2
    y, c = me_tp // 2, me_tp % 2
    x_peer = me_sp + 1 - 2 * x
    c_peer = me_tp + 1 - 2 * c
    y_peer = me_tp + 2 - 4 * y
    far_peer = 3 - me_tp
    nz = n_sp // 2
    z_sp = [2 * flip(z, d) + x for d in range(nz)]
    pair = z_sp[1]
    rc = Copies(send_sems, recv_sems)
    sent = []

    def start(copy, when=None):
        if when is None:
            copy.start()
        else:
            pl.when(when)(copy.start)
        sent.append((copy, when))

    barrier = pltpu.get_barrier_semaphore()
    for i in range(n_sp):
        for j in range(n_tp):
            if i or j:
                pl.semaphore_signal(
                    barrier, inc=1,
                    device_id={"sp": (me_sp + i) % n_sp, "tp": (me_tp + j) % n_tp},
                    device_id_type=MESH,
                )

    loads = {}

    def load(name, source, target):
        loads[name] = pltpu.make_async_copy(source, target, local_sems.at[len(loads)])
        loads[name].start()

    load("win", latent_in, win.at[pl.ds(reach * R, R), pl.ds(0, latent_width)])
    load("kup", kup_in, kup)
    load("vup", vup_in, vup)
    load("q", q_in, q_v)
    load("t", t_in, t_v)
    load("proj", proj_in, proj)
    load("resid", resid_in, resid)

    place = lax.broadcasted_iota(jnp.int32, (R, LANES), 1)
    front = place % ROPE < ROPE // 2

    def turn(vectors):
        vectors = vectors.astype(f32)
        swapped = jnp.where(
            front,
            pltpu.roll(vectors, LANES - ROPE // 2, 1),
            pltpu.roll(vectors, ROPE // 2, 1),
        )
        return vectors * cosine[...] + swapped * sine[...]

    own_rows = slice(reach * R, (reach + 1) * R)
    for r in range(chunks):
        docs = doc_in[pl.ds(r * C, C)].astype(f32)
        side_v[r * C : (r + 1) * C, 0:ROPE] = rope_in[:, r * C : (r + 1) * C].astype(f32).T
        side_v[r * C : (r + 1) * C, ROPE:] = jnp.broadcast_to(docs[None, :], (C, C)).T[:, ROPE:]
    win[own_rows, latent_width:] = jnp.where(
        place < ROPE, turn(side_v[...]), side_v[...]
    ).astype(bf16)
    with jax.named_scope("barrier"):
        pl.semaphore_wait(barrier, n_sp * n_tp - 1)

    part = R // n_tp
    halo = rc.ids(reach)
    halo_ids = rc.ids(3 * reach)

    def quarter(k, tp):
        return win.at[pl.ds(pl.multiple_of((reach - k) * R + tp * part, 16), part)]

    halo_side = rc.ids(reach)
    own_part = pl.multiple_of(me_tp * part, 16)

    def halo_copy(k):
        return rc.make(
            halo + k - 1, latent_in.at[pl.ds(own_part, part)],
            quarter(k, me_tp).at[:, pl.ds(0, latent_width)], me_sp + k, me_tp,
        )

    def halo_side_copy(k):
        lanes = pl.ds(latent_width, LANES)
        return rc.make(
            halo_side + k - 1, win.at[pl.ds(reach * R + own_part, part), lanes],
            quarter(k, me_tp).at[:, lanes], me_sp + k, me_tp,
        )

    def halo_pass(k, kind, tp, tp_to):
        rows = quarter(k, tp)
        return rc.make(halo_ids + 3 * (k - 1) + kind, rows, rows, me_sp, tp_to)

    for k in range(1, reach + 1):
        start(halo_copy(k), me_sp + k < n_sp)
        start(halo_side_copy(k), me_sp + k < n_sp)

    halves = ((0, first), (first, second))

    def half_in(w, parity):
        at, size = halves[parity]
        if w >= 2:
            return down_in.at[pl.ds(at + (w - 2) * (size // 2), size // 2), :]
        return (gate_in, value_in)[w].at[:, pl.ds(at, size)]

    def half_slot(w, parity, owner):
        size = halves[parity][1]
        if w >= 2:
            return down_w.at[owner, pl.ds((w - 2) * (size // 2), size // 2), :]
        rows = pl.ds(pl.multiple_of(owner * gate_rows, 16), gate_rows)
        return (gate_w, value_w)[w].at[rows, pl.ds(0, size)]

    def by_parity(parity, act):
        for p in range(2):
            pl.when(parity == p)(functools.partial(act, p))

    pieces = ((0,), (1,), (2, 3))
    z_ids = [rc.ids(nz) for _ in range(4)]
    x_ids = [rc.ids(nz) for _ in range(4)]
    own_ids = [len(loads) + w for w in range(4)]

    def own_weight(w, p):
        return pltpu.make_async_copy(half_in(w, p), half_slot(w, p, me_sp), local_sems.at[own_ids[w]])

    def z_weight(w, d, p):
        return rc.make(z_ids[w] + d, half_in(w, p), half_slot(w, p, me_sp), z_sp[d], me_tp)

    def z_landed(w, d, p):
        return rc.make(z_ids[w] + d, half_in(w, p), half_slot(w, p, z_sp[d]), z_sp[d], me_tp)

    def x_weight(w, d, p):
        source = half_in(w, p) if d == 0 else half_slot(w, p, z_sp[d])
        return rc.make(x_ids[w] + d, source, half_slot(w, p, z_sp[d]), x_peer, me_tp)

    def x_landed(w, d, p):
        slot = half_slot(w, p, z_sp[d] + 1 - 2 * x)
        return rc.make(x_ids[w] + d, slot, slot, x_peer, me_tp)

    def send_z(w, which):
        for d in which:
            def act(p, d=d):
                for piece in pieces[w]:
                    z_weight(piece, d, p).start()
            by_parity((odd + d) % 2, act)

    def send_x(w, d):
        def act(p):
            for piece in pieces[w]:
                if d:
                    z_landed(piece, d, p).wait_recv()
                x_weight(piece, d, p).start()
        by_parity(odd, act)

    def all_here(w):
        def act(p):
            own_weight(w, p).wait()
            for d in range(nz):
                x_landed(w, d, p).wait_recv()
        by_parity(odd, act)

    for w in range(4):
        by_parity(odd, lambda p, w=w: own_weight(w, p).start())
    middle, near = list(range(2, nz)), [1]
    rightward = 1 - z // (nz // 2)

    inner = odd == rightward
    outer = jnp.logical_not(inner)

    def first_weights(right):
        for w in range(2):
            pl.when((1 - odd) == right)(lambda w=w: send_z(w, near))
        pl.when((rightward == right) & outer)(lambda: send_z(0, middle))
        if not right:
            def inner_weights(turned):
                send_z(0, middle)
                send_z(1, middle)
                send_z(2, middle[: len(middle) - turned])
            for turned in range(2):
                pl.when(inner & (rightward == turned))(functools.partial(inner_weights, turned))

    send_x(0, 0)
    send_x(1, 0)
    first_weights(0)

    @pl.when(odd == 1)
    def _():
        blank = first - second
        if blank:
            gate_w[:, second:] = jnp.zeros((gate_w.shape[0], blank), bf16)
            value_w[:, second:] = jnp.zeros((gate_w.shape[0], blank), bf16)
            down_w[:, second:, :] = jnp.zeros((n_sp, blank, down_cols), bf16)

    for conv, at in ((conv_g, 0), (conv_v, 8)):
        def pick_taps(p, conv=conv, at=at):
            first_unit, size = halves[p]
            taps[at : at + CONV, 0:size] = conv[:, first_unit : first_unit + size].astype(f32)
            if size < first:
                taps[at : at + CONV, size:] = jnp.zeros((CONV, first - size), f32)
        by_parity(odd, pick_taps)

    loads["win"].wait()
    loads["kup"].wait()
    loads["vup"].wait()

    def raise_rows(block):
        rows = pl.ds(pl.multiple_of(block * R, LANES), R)
        source = win[rows, :latent_width]
        keys[rows, :] = jnp.dot(source, kup[...], preferred_element_type=f32).astype(bf16)
        vals[rows, :] = jnp.dot(source, vup[...], preferred_element_type=f32).astype(bf16)

    with jax.named_scope("own_kv"):
        raise_rows(reach)
    loads["q"].wait()
    loads["t"].wait()
    for duo in range(heads // 2):
        cut = slice(duo * LANES, (duo + 1) * LANES)
        t_v[:, cut] = turn(t_v[:, cut]).astype(bf16)
    for k in range(1, reach + 1):
        @pl.when(me_sp >= k)
        def _(k=k):
            with jax.named_scope("halo_wait"):
                halo_copy(k).wait_recv()
                halo_side_copy(k).wait_recv()
            halo_pass(k, 0, me_tp, y_peer).start()
            halo_pass(k, 1, me_tp, c_peer).start()

        @pl.when(me_sp < k)
        def _(k=k):
            win[(reach - k) * R : (reach - k + 1) * R, :] = jnp.zeros((R, win.shape[1]), bf16)
        sent.append((halo_pass(k, 0, me_tp, y_peer), me_sp >= k))
        sent.append((halo_pass(k, 1, me_tp, c_peer), me_sp >= k))
    for k in range(1, reach + 1):
        @pl.when(me_sp >= k)
        def _(k=k):
            with jax.named_scope("halo_y_wait"):
                halo_pass(k, 0, y_peer, y_peer).wait_recv()
            halo_pass(k, 2, y_peer, c_peer).start()
        sent.append((halo_pass(k, 2, y_peer, c_peer), me_sp >= k))
    for k in range(1, reach + 1):
        @pl.when(me_sp >= k)
        def _(k=k):
            with jax.named_scope("halo_core_wait"):
                halo_pass(k, 1, c_peer, c_peer).wait_recv()
                halo_pass(k, 2, far_peer, c_peer).wait_recv()
    first_weights(1)

    with jax.named_scope("kv"):
        @pl.loop(0, reach)
        def _(block):
            raise_rows(block)

    side = win[:, latent_width:]
    side_f = side.astype(f32)
    lane = lax.broadcasted_iota(jnp.int32, (window, LANES), 1)
    low = lane < LANES // 2
    ropes[0] = jnp.where(low, side_f, 0.0).astype(bf16)
    ropes[1] = jnp.where(low, 0.0, pltpu.roll(side_f, LANES // 2, 1)).astype(bf16)
    pick = (
        (lax.broadcasted_iota(jnp.int32, (8, LANES), 1) == LANES // 2)
        .astype(f32)
        .astype(bf16)
    )
    key_doc = lax.dot_general(pick, side, (((1,), (1,)), ((), ())), preferred_element_type=f32)[0:1]
    for r in range(chunks):
        at = slice(r * C, (r + 1) * C)
        own_doc = side_f[reach * R + r * C : reach * R + (r + 1) * C, LANES // 2 : LANES // 2 + 1]
        key_at = lax.broadcasted_iota(jnp.int32, (C, window), 1) - reach * R
        row_at = lax.broadcasted_iota(jnp.int32, (C, window), 0) + r * C
        allowed = (key_at <= row_at) & (key_at + me_sp * R >= 0) & (key_doc == own_doc)
        bias[at, :] = jnp.where(allowed, 0.0, masked_score)

    tail = side_f[reach * R - 8 :]
    valid_id = rc.ids()
    row_no = lax.broadcasted_iota(jnp.int32, (R, LANES), 0) + me_sp * R
    here = tail[8:]
    back_one = (pltpu.roll(tail, 1, 0)[8:] == here) & (row_no >= 1)
    back_two = (pltpu.roll(tail, 2, 0)[8:] == here) & (row_no >= 2)
    lanes = lax.broadcasted_iota(jnp.int32, (R, LANES), 1)
    valid[odd] = jnp.where(
        lanes < 3 * LANES // 4, back_two.astype(f32), back_one.astype(f32)
    ).astype(bf16)
    start(rc.make(valid_id, valid.at[odd], valid.at[odd], pair, me_tp))

    scale = (NOPE + ROPE) ** (-0.5) * log2_e

    def attend_chunk(r):
        at, seen = slice(r * C, (r + 1) * C), slice(r * C, r * C + span)

        @pl.loop(0, heads // 2)
        def _(duo):
            turned = t_v[at, pl.ds(pl.multiple_of(duo * LANES, LANES), LANES)]
            for e in range(2):
                head = pl.ds(pl.multiple_of((2 * duo + e) * LANES, LANES), LANES)
                queries = jnp.concatenate([q_v[at, head], turned], 1)
                seen_keys = jnp.concatenate([keys[seen, head], ropes[e, seen, :]], 1)
                scores = lax.dot_general(
                    queries, seen_keys, (((1,), (1,)), ((), ())), preferred_element_type=f32
                )
                scores = scores * scale + bias[at, seen]
                weights = jnp.exp2(scores - jnp.max(scores, -1, keepdims=True))
                total = jnp.sum(weights, -1, keepdims=True)
                mixed = jnp.dot(weights.astype(bf16), vals[seen, head], preferred_element_type=f32)
                att[at, head] = (mixed * (1.0 / total)).astype(bf16)

    core_ids, y_ids = rc.ids(2 * chunks), rc.ids(chunks)
    stat_ids = rc.ids(3 * chunks)
    stat_ids2 = rc.ids(3 * chunks)
    gather_ids = rc.ids(8 * chunks)

    def to_core(r, i):
        return rc.make(core_ids + 2 * r + i, core_out.at[r, i], core_in.at[r, i], me_sp, c_peer)

    def to_y(r):
        return rc.make(y_ids + r, y_out.at[r], y_in.at[r], me_sp, y_peer)

    def features(tp):
        return pl.ds(pl.multiple_of(tp * F, LANES), F)

    def project(r):
        rows = att[r * C : (r + 1) * C, :]
        for i, yy in enumerate((1 - y, y)):
            core_out[r, i] = jnp.dot(
                rows, proj[:, features(2 * yy + 1 - c)], preferred_element_type=f32
            ).astype(bf16)
            start(to_core(r, i))
        for i, yy in enumerate((1 - y, y)):
            keep[r, i] = jnp.dot(
                rows, proj[:, features(2 * yy + c)], preferred_element_type=f32
            ).astype(bf16)
        to_core(r, 0).wait_recv()
        y_out[r] = (keep[r, 0].astype(f32) + core_in[r, 0].astype(f32)).astype(bf16)
        start(to_y(r))

    def stat_copy(ids, own, landed, r, i):
        return rc.make(ids + 3 * r + i, own.at[r], landed.at[r, i], me_sp, (c_peer, y_peer, far_peer)[i])

    def send_stats(values, ids, own, landed, r):
        one = jnp.sum(values, -1, keepdims=True)
        two = jnp.sum(values * values, -1, keepdims=True)
        lane = lax.broadcasted_iota(jnp.int32, (C, LANES), 1)
        own[r] = jnp.where(lane % 8 < 4, one, two).T[0:8]
        for i in (1, 2, 0):
            start(stat_copy(ids, own, landed, r, i))

    def norm(values, ids, own, landed, r, gain):
        for i in range(3):
            stat_copy(ids, own, landed, r, i).wait_recv()
        total = (own[r] + landed[r, 0]) + (landed[r, 1] + landed[r, 2])
        total = jnp.concatenate([total] * (LANES // 8), 0).T
        row_mean = total[:, 0:1] / wide
        row_power = total[:, 4:5] / wide
        scaled = (values - row_mean) * lax.rsqrt(row_power - row_mean * row_mean + norm_eps)
        return scaled * gain[0][...].astype(f32)[None, :] + gain[1][...].astype(f32)[None, :]

    def mix_one(r):
        at = slice(r * C, (r + 1) * C)
        to_core(r, 1).wait_recv()
        to_y(r).wait_recv()
        mixed = residual_scale * resid[at, :].astype(f32) + (
            keep[r, 1].astype(f32) + core_in[r, 1].astype(f32) + y_in[r].astype(f32)
        )
        mix[at, :] = mixed
        send_stats(mixed, stat_ids, stat_own, stat_in, r)

    def gathered(r, kind, slot, tp, sp_to, tp_to):
        spot = rows_all.at[slot, pl.ds(r * C, C), features(tp)]
        return rc.make(gather_ids + 8 * r + kind, spot, spot, sp_to, tp_to)

    def to_pair(r, slot):
        return gathered(r, 0, slot, me_tp, pair, me_tp)

    def core_gather(r, kind, slot, tp):
        return gathered(r, kind, slot, tp, me_sp, c_peer)

    def y_gather(r, kind, slot, tp):
        return gathered(r, kind, slot, tp, me_sp, y_peer)

    def norm_one(r):
        at = slice(r * C, (r + 1) * C)
        rows_all[odd, at, features(me_tp)] = norm(
            mix[at, :], stat_ids, stat_own, stat_in, r, (gain1, bias1)
        ).astype(bf16)
        start(to_pair(r, odd))
        start(y_gather(r, 1, odd, me_tp))
        start(core_gather(r, 2, odd, me_tp))

    def pass_pair(r):
        to_pair(r, 1 - odd).wait_recv()
        start(y_gather(r, 3, 1 - odd, me_tp))
        start(core_gather(r, 4, 1 - odd, me_tp))

    def pass_y(r):
        for kind, got, slot in ((5, 1, odd), (6, 3, 1 - odd)):
            y_gather(r, got, slot, y_peer).wait_recv()
            start(core_gather(r, kind, slot, y_peer))

    def rows_here(r):
        core_gather(r, 2, odd, c_peer).wait_recv()
        core_gather(r, 4, 1 - odd, c_peer).wait_recv()
        core_gather(r, 5, odd, far_peer).wait_recv()
        core_gather(r, 6, 1 - odd, far_peer).wait_recv()

    def z_left(w, d):
        by_parity((odd + d) % 2, lambda p: z_weight(w, d, p).wait_send())

    def forward(w, which):
        for d in which:
            with jax.named_scope("fwd%d_%d" % (w, d)):
                send_x(w, d)

    def attend_step(r):
        with jax.named_scope("att"):
            attend_chunk(r)
        if r == 0:
            loads["proj"].wait()
            loads["resid"].wait()
        else:
            with jax.named_scope("mix"):
                mix_one(r - 1)
        with jax.named_scope("proj"):
            project(r)
        if r:
            with jax.named_scope("norm"):
                norm_one(r - 1)

    for r in range(chunks):
        attend_step(r)
        if r == 0:
            pl.when(outer)(lambda: send_z(1, middle))
            forward(0, near)
            send_x(2, 0)
        elif r == 1:
            forward(1, near)
    forward(0, middle)
    with jax.named_scope("mix"):
        mix_one(chunks - 1)
    with jax.named_scope("norm"):
        norm_one(chunks - 1)
    send_z(2, near)
    forward(1, middle[:-1])
    with jax.named_scope("pass_pair"):
        for r in range(chunks):
            pass_pair(r)
    with jax.named_scope("pass_y"):
        for r in range(chunks):
            pass_y(r)
    forward(1, middle[-1:])
    with jax.named_scope("rows_here"):
        for r in range(chunks):
            rows_here(r)

    tile = 2 * LANES
    mid = first

    def up(weights, base):
        @pl.loop(0, 2)
        def _(slot):
            @pl.loop(0, first // tile)
            def _(j):
                cols = pl.multiple_of(j * tile, LANES)
                ext[slot, 8:, pl.ds(base + cols, tile)] = (
                    jnp.dot(rows_all[slot], weights[:, pl.ds(cols, tile)], preferred_element_type=f32)
                    .astype(bf16)
                    .astype(f32)
                )

    pl.when(outer & (rightward == 0))(lambda: send_z(2, middle))
    with jax.named_scope("wait_g"):
        all_here(0)
    with jax.named_scope("up_g"):
        up(gate_w, 0)
    forward(2, near)
    with jax.named_scope("wait_v"):
        all_here(1)
    pl.when(outer & (rightward == 1))(lambda: send_z(2, middle[:-1]))
    with jax.named_scope("up_v"):
        up(value_w, mid)

    tail_ids = rc.ids(2)

    def tail_copy(slot, to_slot, sp):
        return rc.make(
            tail_ids + to_slot, ext.at[slot, pl.ds(R, 8)], ext.at[to_slot, pl.ds(0, 8)], sp, me_tp
        )

    last_pair = z >= nz - 2
    start(tail_copy(0, 0, x_peer), x == 0)
    start(tail_copy(1, 1, x_peer), x == 0)
    start(tail_copy(0, 1, x_peer), x == 1)
    start(tail_copy(1, 0, me_sp + 3), (x == 1) & (z < nz - 2))
    pl.when(rightward == 1)(lambda: send_z(2, middle[-1:]))

    @pl.when((x == 0) & (z < 2))
    def _():
        ext[0, 0:8, :] = jnp.zeros((8, ext.shape[2]), f32)

    deep = 64

    def convolve(first_step, steps):
        @pl.loop(0, 2)
        def _(slot):
            @pl.loop(first_step, first_step + steps)
            def _(i):
                at = pl.multiple_of(i * deep, 16)
                marks = valid[slot, pl.ds(at, deep), :].astype(f32)
                two, one = marks[:, LANES // 2 : LANES // 2 + 1], marks[:, LANES - 1 : LANES]

                @pl.loop(0, first // tile)
                def _(j):
                    cols = pl.multiple_of(j * tile, LANES)

                    def mixing(base, tap):
                        rows = ext[slot, pl.ds(at, deep + 8), pl.ds(base + cols, tile)]
                        weight = taps[pl.ds(tap, 8), pl.ds(cols, tile)]
                        return (
                            weight[0:1] * (pltpu.roll(rows, 2, 0)[8:] * two)
                            + weight[1:2] * (pltpu.roll(rows, 1, 0)[8:] * one)
                            + weight[2:3] * rows[8:]
                        )

                    hid[slot, pl.ds(at, deep), pl.ds(cols, tile)] = (
                        mixing(mid, 8) * jax.nn.gelu(mixing(0, 0))
                    ).astype(bf16)

    rc.make(valid_id, valid.at[1 - odd], valid.at[1 - odd], pair, me_tp).wait_recv()
    with jax.named_scope("conv"):
        convolve(1, R // deep - 1)
    forward(2, middle[:-1])
    with jax.named_scope("tails"):
        @pl.when((x == 1) | (z >= 2))
        def _():
            tail_copy(0, 0, x_peer).wait_recv()
        tail_copy(1, 1, x_peer).wait_recv()
    with jax.named_scope("conv_first"):
        convolve(0, 1)

    core_ids2, z_ids2, y_ids2 = rc.ids(4), rc.ids(2 * chunks), rc.ids(chunks)
    per = F // down_cols
    half_z = (z // 2) % 2
    slots = (1 - odd, odd)

    def to_core2(d, s):
        f = d // 2
        return rc.make(
            core_ids2 + 2 * f + s, part2.at[d, s], core_in2.at[f, s], me_sp, c_peer
        )

    def to_pair2(f, r):
        at = pl.ds(r * C, C)
        return rc.make(z_ids2 + chunks * f + r, z_out2.at[f, at], z_in2.at[f, at], pair, me_tp)

    def to_y2(r):
        at = pl.ds(r * C, C)
        return rc.make(y_ids2 + r, y_out2.at[at], y_in2.at[at], me_sp, y_peer)

    def down_block(d):
        f, block = d // 2, flip(z, d)
        with jax.named_scope("wait_d%d" % d):
            def act(p):
                for piece in pieces[2]:
                    if d == 0:
                        own_weight(piece, p).wait()
                    x_landed(piece, d, p).wait_recv()
            by_parity(odd, act)
        with jax.named_scope("down"):
            for s in range(2):
                for j in range(per):
                    part2[d, s, :, j * down_cols : (j + 1) * down_cols] = jnp.dot(
                        hid[slots[s]], down_w[per * block + j], preferred_element_type=f32
                    ).astype(bf16)
                start(to_core2(d, s), block % 2 != c)

    def pair_block(d):
        f, block = d // 2, flip(z, d)

        @pl.when(block % 2 == c)
        def _():
            with jax.named_scope("core2_wait"):
                to_core2(d, 0).wait_recv()
            for r in range(chunks):
                at = slice(r * C, (r + 1) * C)
                z_out2[f, at, :] = (
                    part2[d, 0, at, :].astype(f32) + core_in2[f, 0, at, :].astype(f32)
                ).astype(bf16)
                to_pair2(f, r).start()
            with jax.named_scope("core2_wait"):
                to_core2(d, 1).wait_recv()

    def mine_of(f):
        return 2 * f + (odd + c) % 2

    def pass_down(f):
        yy = half_z if f == 0 else 1 - half_z
        for r in range(chunks):
            at = slice(r * C, (r + 1) * C)
            with jax.named_scope("z2_wait"):
                to_pair2(f, r).wait_recv()
            sent.append((to_pair2(f, r), None))

            @pl.when(y != yy)
            def _():
                y_out2[at, :] = (
                    part2[mine_of(f), 1, pl.ds(r * C, C), :].astype(f32)
                    + core_in2[f, 1, at, :].astype(f32)
                    + z_in2[f, at, :].astype(f32)
                ).astype(bf16)
                to_y2(r).start()

    down_block(0)
    down_block(1)
    pair_block(0)
    pair_block(1)
    forward(2, middle[-1:])
    down_block(2)
    pair_block(2)
    down_block(3)
    pair_block(3)
    pass_down(0)
    pass_down(1)
    mine = (y + half_z) % 2
    for r in range(chunks):
        at = slice(r * C, (r + 1) * C)
        rows = pl.ds(r * C, C)
        with jax.named_scope("y2_wait"):
            to_y2(r).wait_recv()
        sent.append((to_y2(r), None))
        mixed = residual_scale * rows_all[odd, at, features(me_tp)].astype(f32) + (
            part2[mine_of(mine), 1, rows, :].astype(f32)
            + core_in2[mine, 1, rows, :].astype(f32)
            + z_in2[mine, rows, :].astype(f32)
            + y_in2[at, :].astype(f32)
        )
        mix[at, :] = mixed
        send_stats(mixed, stat_ids2, stat_own2, stat_in2, r)
    with jax.named_scope("norm2"):
        for r in range(chunks):
            at = slice(r * C, (r + 1) * C)
            out_ref[at, :] = norm(mix[at, :], stat_ids2, stat_own2, stat_in2, r, (gain2, bias2)).astype(bf16)

    for copy, when in sent:
        if when is None:
            copy.wait_send()
        else:
            pl.when(when)(copy.wait_send)
    for w in range(4):
        for d in range(nz):
            if d:
                z_left(w, d)
            by_parity(odd, lambda p, d=d, w=w: x_weight(w, d, p).wait_send())
    assert rc.count <= REMOTE, rc.count


def fused(
    residual, query_nope, query_rope, latent, rope_key, doc_ids, key_up, value_up, out_proj,
    norm1_gain, norm1_bias, ffn_gate, ffn_value, conv_gate, conv_value, ffn_down, norm2_gain, norm2_bias,
):
    n_sp, n_tp = lax.axis_size("sp"), lax.axis_size("tp")
    R, F = residual.shape
    heads = query_nope.shape[1] // NOPE
    units = ffn_gate.shape[1]
    first = -(-units // (2 * LANES)) * LANES
    second = units - first
    window = (REACH + 1) * R
    chunks = R // LANES
    f32, bf16 = jnp.float32, jnp.bfloat16
    offset = lax.axis_index("sp") * R
    positions = offset + jnp.arange(R, dtype=jnp.int32)
    half = ROPE // 2
    place = jnp.arange(LANES, dtype=jnp.int32) % half
    frequencies = 1.0 / rope_base_freq ** (2.0 * place.astype(f32) / ROPE)
    angles = positions.astype(f32)[:, None] * frequencies[None, :]
    front = jnp.arange(LANES) % ROPE < half
    cosine, sine = jnp.cos(angles), jnp.where(front, -1.0, 1.0) * jnp.sin(angles)
    hbm = pl.BlockSpec(memory_space=pl.ANY)
    vmem = pl.BlockSpec(memory_space=pltpu.VMEM)
    sizes = (n_sp, n_tp, R, REACH, heads, n_tp * F, first, second)

    def v(*shape, dtype=bf16):
        return pltpu.VMEM(shape, dtype)

    C = LANES
    return pl.pallas_call(
        functools.partial(layer_kernel, sizes),
        in_specs=[hbm] * 7 + [vmem] * 10 + [hbm] * 3,
        out_specs=vmem,
        out_shape=jax.ShapeDtypeStruct((R, F), bf16),
        scratch_shapes=[
            v(R, LANES, dtype=f32), v(16, first, dtype=f32), v(window, latent.shape[1] + LANES), v(R, heads * NOPE), v(R, heads * ROPE),
            v(*key_up.shape), v(*value_up.shape), v(*out_proj.shape), v(R, F),
            v(window, heads * NOPE), v(window, heads * VDIM), v(2, window, LANES),
            v(R, window, dtype=f32), v(R, heads * VDIM),
            v(chunks, 2, C, F), v(chunks, 2, C, F), v(chunks, 2, C, F), v(chunks, C, F), v(chunks, C, F),
            v(R, F, dtype=f32), v(chunks, 8, LANES, dtype=f32), v(chunks, 3, 8, LANES, dtype=f32),
            v(2, R, LANES),
            v(2, R, n_tp * F), v(n_sp * ffn_gate.shape[0], first), v(n_sp * ffn_gate.shape[0], first),
            v(n_sp, first, ffn_down.shape[1]), v(2, R + 8, 2 * first, dtype=f32), v(2, R, first),
            v(4, 2, R, F), v(2, 2, R, F), v(R, F), v(R, F), v(2, R, F), v(2, R, F),
            v(chunks, 8, LANES, dtype=f32), v(chunks, 3, 8, LANES, dtype=f32),
            pltpu.SemaphoreType.DMA((REMOTE,)), pltpu.SemaphoreType.DMA((REMOTE,)),
            pltpu.SemaphoreType.DMA((LOCAL,)),
        ],
        compiler_params=pltpu.CompilerParams(
            collective_id=0, has_side_effects=True, vmem_limit_bytes=64 * 1024 * 1024 - 65536
        ),
    )(
        query_nope, query_rope, latent, key_up, value_up, out_proj, residual, rope_key.T, doc_ids, cosine, sine,
        norm1_gain, norm1_bias, norm2_gain, norm2_bias,
        conv_gate, conv_value, ffn_gate, ffn_value, ffn_down,
    )


def local(*arrays):
    rows, features = arrays[0].shape
    down_cols = arrays[15].shape[1]
    n_sp, n_tp = lax.axis_size("sp"), lax.axis_size("tp")
    paired = n_sp // 2
    fits = n_tp == 4 and paired == n_tp
    tiled = rows % LANES == 0 and down_cols % LANES == 0 and features == 2 * down_cols
    return (fused if fits and tiled else plain)(*arrays)


def solution(mesh):
    placed = (
        P("sp", "tp"),
        P("sp", "tp"),
        P("sp", "tp"),
        P("sp", None),
        P("sp", None),
        P("sp"),
        P(None, "tp"),
        P(None, "tp"),
        P("tp", None),
        P("tp"),
        P("tp"),
        P("sp", "tp"),
        P("sp", "tp"),
        P(None, "tp"),
        P(None, "tp"),
        P("tp", "sp"),
        P("tp"),
        P("tp"),
    )
    return jax.shard_map(
        local, mesh=mesh, in_specs=placed, out_specs=P("sp", "tp"), check_vma=False
    )
```

```python
import functools

import jax
import jax.numpy as jnp
import numpy as np
from jax import lax
from jax.experimental import pallas as pl
from jax.experimental.pallas import tpu as pltpu
from jax.sharding import PartitionSpec as P

D = 2048
NOPE = 128
ROPE = 64
VDIM = 128
CONV = 3
REACH = 3


norm_eps = 1e-05
residual_scale = 8.0**0.25
rope_base_freq = 10000.0
masked_score = -1e30


def passed_along(value, axis, by):
    count = lax.axis_size(axis)
    pairs = [(i, i + by) for i in range(count) if 0 <= i + by < count]
    return lax.ppermute(value, axis, pairs)


def tables(positions):
    frequencies = 1.0 / rope_base_freq ** (jnp.arange(0, ROPE, 2, dtype=jnp.float32) / ROPE)
    angles = positions.astype(jnp.float32)[:, None] * frequencies[None, :]
    return (jnp.cos(angles), jnp.sin(angles))


def rotate(vectors, cosine, sine_table):
    half_width = vectors.shape[-1] // 2
    front_half = vectors[..., :half_width]
    back_half = vectors[..., half_width:]
    return jnp.concatenate(
        [
            front_half * cosine - back_half * sine_table,
            front_half * sine_table + back_half * cosine,
        ],
        axis=-1,
    )


def ring_blocks(block, axis):
    count = lax.axis_size(axis)
    order = list(range(0, count, 2)) + list(range(1, count, 2))[::-1]
    place = [order.index(i) for i in range(count)]
    me = lax.axis_index(axis)
    found = [(me, block)]
    ahead = count // 2
    for turn, steps in ((1, ahead), (-1, count - 1 - ahead)):
        pairs = [(order[p], order[(p + turn) % count]) for p in range(count)]
        moving = block
        for step in range(1, steps + 1):
            moving = lax.ppermute(moving, axis, pairs)
            owners = [order[(place[i] - turn * step) % count] for i in range(count)]
            found.append((jnp.asarray(owners, jnp.int32)[me], moving))
    return found


def attend_kernel(chunk, reach_rows, scale, q_ref, turned_ref, k_ref, rope_ref, v_ref, bias_ref, out_ref):
    rows = q_ref.shape[0]
    span = chunk + reach_rows
    rope_rows = rope_ref[...]
    for head in range(q_ref.shape[1] // NOPE):
        nope = slice(head * NOPE, (head + 1) * NOPE)
        rope = slice(head * ROPE, (head + 1) * ROPE)
        queries = jnp.concatenate([q_ref[:, nope], turned_ref[:, rope]], 1)
        keys = jnp.concatenate([k_ref[:, nope], rope_rows], 1)
        for start in range(0, rows, chunk):
            cut = slice(start, start + chunk)
            seen = slice(start, start + span)
            scores = lax.dot_general(
                queries[cut], keys[seen], (((1,), (1,)), ((), ())), preferred_element_type=jnp.float32
            )
            scores = scores * scale + bias_ref[cut, seen]
            weights = jnp.exp(scores - jnp.max(scores, -1, keepdims=True))
            weights = weights * (1.0 / jnp.sum(weights, -1, keepdims=True))
            out_ref[cut, nope] = jnp.dot(
                weights.astype(jnp.bfloat16), v_ref[seen, nope], preferred_element_type=jnp.float32
            ).astype(jnp.bfloat16)


def attend(queries, turned, keys, rope_rows, values, bias, scale):
    rows, width = queries.shape
    window = keys.shape[0]
    chunk = 128 if rows % 128 == 0 else rows
    pair = 2
    wide = pair * NOPE
    heads = width // NOPE
    return pl.pallas_call(
        functools.partial(attend_kernel, chunk, window - rows, scale),
        grid=(heads // pair,),
        in_specs=[
            pl.BlockSpec((rows, wide), lambda i: (0, i)),
            pl.BlockSpec((rows, pair * ROPE), lambda i: (0, i)),
            pl.BlockSpec((window, wide), lambda i: (0, i)),
            pl.BlockSpec((window, ROPE), lambda i: (0, 0)),
            pl.BlockSpec((window, pair * VDIM), lambda i: (0, i)),
            pl.BlockSpec((rows, window), lambda i: (0, 0)),
        ],
        out_specs=pl.BlockSpec((rows, pair * VDIM), lambda i: (0, i)),
        out_shape=jax.ShapeDtypeStruct((rows, heads * VDIM), jnp.bfloat16),
        compiler_params=pltpu.CompilerParams(vmem_limit_bytes=40 * 1024 * 1024),
        cost_estimate=pl.CostEstimate(
            flops=16 * rows * window * heads * (NOPE + ROPE + VDIM),
            bytes_accessed=2 * (4 * rows * width + 2 * window * width),
            transcendentals=rows * window * heads,
        ),
    )(queries, turned, keys, rope_rows, values, bias)


def scatter_sum(terms, axis):
    count = lax.axis_size(axis)
    width = terms.shape[1] // count
    parts = jnp.stack([terms[:, i * width : (i + 1) * width] for i in range(count)])
    got = lax.all_to_all(parts.astype(jnp.bfloat16), axis, 0, 0)
    return jnp.sum(got.astype(jnp.float32), 0)


def finish(mixed, totals, gain_row, bias_row):
    row_mean = totals[0][:, None] / D
    row_power = totals[1][:, None] / D
    return (mixed - row_mean) * lax.rsqrt(
        row_power - row_mean * row_mean + norm_eps
    ) * gain_row.astype(jnp.float32) + bias_row.astype(jnp.float32)


def plain(
    residual,
    query_nope,
    query_rope,
    latent,
    rope_key,
    doc_ids,
    key_up,
    value_up,
    out_proj,
    norm1_gain,
    norm1_bias,
    ffn_gate,
    ffn_value,
    conv_gate,
    conv_value,
    ffn_down,
    norm2_gain,
    norm2_bias,
):
    row_count = latent.shape[0]
    head_count = query_nope.shape[1] // NOPE
    local_units = ffn_gate.shape[1]
    rim_rows = CONV - 1
    whole_gate = lax.all_gather(ffn_gate, "sp", axis=0, tiled=True)
    whole_value = lax.all_gather(ffn_value, "sp", axis=0, tiled=True)
    offset = lax.axis_index("sp") * row_count
    positions = offset + jnp.arange(row_count, dtype=jnp.int32)
    cosine, sine_table = tables(positions)
    turned_key = rotate(rope_key.astype(jnp.float32), cosine, sine_table).astype(jnp.bfloat16)
    turned_query = rotate(
        query_rope.astype(jnp.float32).reshape(row_count, head_count, ROPE),
        cosine[:, None],
        sine_table[:, None],
    ).astype(jnp.bfloat16)
    latent_width = latent.shape[1]
    packed = jnp.concatenate(
        [
            latent,
            turned_key,
            jnp.broadcast_to(doc_ids.astype(jnp.bfloat16)[:, None], (row_count, ROPE)),
        ],
        1,
    )
    parts = [passed_along(packed, "sp", shift_step) for shift_step in range(REACH, 0, -1)]
    pieces = jnp.concatenate(parts + [packed], 0)
    win_latent = pieces[:, :latent_width]
    win_key = pieces[:, latent_width : latent_width + ROPE]
    win_doc = pieces[:, latent_width + ROPE].astype(jnp.int32)
    down_blocks = ring_blocks(ffn_down, "sp")
    key_rows = jnp.dot(win_latent, key_up, preferred_element_type=jnp.float32).astype(jnp.bfloat16)
    values = jnp.dot(win_latent, value_up, preferred_element_type=jnp.float32).astype(jnp.bfloat16)
    window = key_rows.shape[0]
    key_pos = offset - REACH * row_count + jnp.arange(window, dtype=jnp.int32)
    allowed = (
        (key_pos[None, :] <= positions[:, None])
        & (key_pos[None, :] >= 0)
        & (win_doc[None, :] == doc_ids[:, None])
    )
    scale = (NOPE + ROPE) ** (-0.5)
    bias = jnp.where(allowed, 0.0, masked_score).astype(jnp.float32)
    attended = attend(
        query_nope,
        turned_query.reshape(row_count, head_count * ROPE),
        key_rows,
        win_key,
        values,
        bias,
        scale,
    )
    head_terms = jnp.dot(attended, out_proj, preferred_element_type=jnp.float32)
    projected = scatter_sum(head_terms, "tp")
    mixed_one = residual_scale * residual.astype(jnp.float32) + projected
    totals_one = lax.psum((jnp.sum(mixed_one, 1), jnp.sum(mixed_one * mixed_one, 1)), "tp")
    normed = finish(mixed_one, totals_one, norm1_gain, norm1_bias).astype(jnp.bfloat16)
    half = row_count // 2
    full_rows = jnp.concatenate(
        [
            lax.all_gather(normed[:half], "tp", axis=1, tiled=True),
            lax.all_gather(normed[half:], "tp", axis=1, tiled=True),
        ],
        0,
    )
    gate_sum = jnp.dot(full_rows, whole_gate, preferred_element_type=jnp.float32)
    value_sum = jnp.dot(full_rows, whole_value, preferred_element_type=jnp.float32)
    gate_pre = gate_sum.astype(jnp.bfloat16)
    value_pre = value_sum.astype(jnp.bfloat16)
    tail_gate, tail_value, tail_doc = passed_along(
        (
            gate_pre[row_count - rim_rows :],
            value_pre[row_count - rim_rows :],
            doc_ids[row_count - rim_rows :],
        ),
        "sp",
        1,
    )
    ext_gate = jnp.concatenate([tail_gate, gate_pre], 0)
    ext_value = jnp.concatenate([tail_value, value_pre], 0)
    ext_doc = jnp.concatenate([tail_doc, doc_ids], 0)
    gate_mix = jnp.zeros((row_count, local_units), jnp.float32)
    value_mix = jnp.zeros((row_count, local_units), jnp.float32)
    for tap_index in range(CONV):
        valid_tap = (
            (ext_doc[tap_index : tap_index + row_count] == doc_ids)
            & (positions - rim_rows + tap_index >= 0)
        ).astype(jnp.float32)[:, None]
        gate_mix = (
            gate_mix
            + conv_gate[tap_index].astype(jnp.float32)
            * ext_gate[tap_index : tap_index + row_count].astype(jnp.float32)
            * valid_tap
        )
        value_mix = (
            value_mix
            + conv_value[tap_index].astype(jnp.float32)
            * ext_value[tap_index : tap_index + row_count].astype(jnp.float32)
            * valid_tap
        )
    hidden = (value_mix * jax.nn.gelu(gate_mix)).astype(jnp.bfloat16)
    sp_count = lax.axis_size("sp")
    tp_count = lax.axis_size("tp")
    block_width = ffn_down.shape[1]
    unit_terms = jnp.zeros((sp_count, row_count, block_width), jnp.bfloat16)
    for owner, block in down_blocks:
        term = jnp.dot(hidden, block, preferred_element_type=jnp.float32).astype(jnp.bfloat16)
        unit_terms = lax.dynamic_update_slice(unit_terms, term[None], (owner, 0, 0))
    share = sp_count // tp_count
    got = lax.all_to_all(
        unit_terms.reshape(tp_count, share, row_count, block_width), "tp", 0, 0
    )
    ffn_blocks = jnp.sum(got.astype(jnp.float32), 0)
    ffn_out = jnp.concatenate([ffn_blocks[i] for i in range(share)], 1)
    mixed_two = residual_scale * normed.astype(jnp.float32) + ffn_out
    totals_two = lax.psum((jnp.sum(mixed_two, 1), jnp.sum(mixed_two * mixed_two, 1)), "tp")
    return finish(mixed_two, totals_two, norm2_gain, norm2_bias).astype(jnp.bfloat16)


LANES = 128
MESH = pl.DeviceIdType.MESH
log2_e = 1.4426950408889634


class Copies:
    def __init__(self, send_sems, recv_sems):
        self.send_sems, self.recv_sems = send_sems, recv_sems
        self.count = 0

    def ids(self, number=1):
        first = self.count
        self.count += number
        return first

    def make(self, index, source, target, sp, tp):
        return pltpu.make_async_remote_copy(
            src_ref=source,
            dst_ref=target,
            send_sem=self.send_sems.at[index],
            recv_sem=self.recv_sems.at[index],
            device_id={"sp": sp, "tp": tp},
            device_id_type=MESH,
        )


REMOTE = 160
LOCAL = 16


def flip(value, bits):
    for bit in range(bits.bit_length()):
        step = 1 << bit
        if bits & step:
            value = value + step - 2 * step * ((value // step) % 2)
    return value


def layer_kernel(
    sizes,
    q_in, t_in, latent_in, kup_in, vup_in, proj_in, resid_in, rope_in, doc_in, frequencies,
    gain1, bias1, gain2, bias2, conv_g, conv_v, gate_in, value_in, down_in,
    out_ref,
    cosine, sine, side_v, taps, win, q_v, t_v, kup, vup, proj, resid, keys, vals, ropes, bias, att,
    core_out, core_in, keep, y_out, y_in, mix, stat_own, stat_in, valid,
    rows_all, gate_w, value_w, down_w, ext, hid,
    part2, core_in2, y_out2, y_in2, z_out2, z_in2, stat_own2, stat_in2,
    send_sems, recv_sems, local_sems,
):
    n_sp, n_tp, R, reach, heads, wide, first, second = sizes
    C = LANES
    F = resid.shape[1]
    chunks = R // C
    window = (reach + 1) * R
    span = C + reach * R
    latent_width = kup.shape[0]
    gate_rows = gate_in.shape[0]
    down_cols = down_in.shape[1]
    bf16, f32 = jnp.bfloat16, jnp.float32
    me_sp, me_tp = lax.axis_index("sp"), lax.axis_index("tp")
    x, z = me_sp % 2, me_sp // 2
    odd = z % 2
    y, c = me_tp // 2, me_tp % 2
    x_peer = me_sp + 1 - 2 * x
    c_peer = me_tp + 1 - 2 * c
    y_peer = me_tp + 2 - 4 * y
    far_peer = 3 - me_tp
    nz = n_sp // 2
    z_sp = [2 * flip(z, d) + x for d in range(nz)]
    pair = z_sp[1]
    rc = Copies(send_sems, recv_sems)
    sent = []

    def start(copy, when=None):
        if when is None:
            copy.start()
        else:
            pl.when(when)(copy.start)
        sent.append((copy, when))

    barrier = pltpu.get_barrier_semaphore()
    for i in range(n_sp):
        for j in range(n_tp):
            if i or j:
                pl.semaphore_signal(
                    barrier, inc=1,
                    device_id={"sp": (me_sp + i) % n_sp, "tp": (me_tp + j) % n_tp},
                    device_id_type=MESH,
                )

    loads = {}

    def load(name, source, target):
        loads[name] = pltpu.make_async_copy(source, target, local_sems.at[len(loads)])
        loads[name].start()

    load("win", latent_in, win.at[pl.ds(reach * R, R), pl.ds(0, latent_width)])
    load("kup", kup_in, kup)
    load("vup", vup_in, vup)
    load("q", q_in, q_v)
    load("t", t_in, t_v)
    load("proj", proj_in, proj)
    load("resid", resid_in, resid)

    with jax.named_scope("barrier"):
        pl.semaphore_wait(barrier, n_sp * n_tp - 1)

    part = R // n_tp
    halo = rc.ids(reach)
    halo_ids = rc.ids(3 * reach)

    def quarter(k, tp):
        return win.at[pl.ds(pl.multiple_of((reach - k) * R + tp * part, 16), part)]

    halo_side = rc.ids(reach)
    own_part = pl.multiple_of(me_tp * part, 16)

    def halo_copy(k):
        return rc.make(
            halo + k - 1, latent_in.at[pl.ds(own_part, part)],
            quarter(k, me_tp).at[:, pl.ds(0, latent_width)], me_sp + k, me_tp,
        )

    def halo_side_copy(k):
        lanes = pl.ds(latent_width, LANES)
        return rc.make(
            halo_side + k - 1, win.at[pl.ds(reach * R + own_part, part), lanes],
            quarter(k, me_tp).at[:, lanes], me_sp + k, me_tp,
        )

    def halo_pass(k, kind, tp, tp_to):
        rows = quarter(k, tp)
        return rc.make(halo_ids + 3 * (k - 1) + kind, rows, rows, me_sp, tp_to)

    for k in range(1, reach + 1):
        start(halo_copy(k), me_sp + k < n_sp)

    place = lax.broadcasted_iota(jnp.int32, (R, LANES), 1)
    front = place % ROPE < ROPE // 2
    row_at = lax.broadcasted_iota(jnp.int32, (R, LANES), 0) + me_sp * R
    angles = row_at.astype(f32) * frequencies[...]
    cosine[...] = jnp.cos(angles)
    sine[...] = jnp.where(front, -1.0, 1.0) * jnp.sin(angles)

    def turn(vectors):
        vectors = vectors.astype(f32)
        swapped = jnp.where(
            front,
            pltpu.roll(vectors, LANES - ROPE // 2, 1),
            pltpu.roll(vectors, ROPE // 2, 1),
        )
        return vectors * cosine[...] + swapped * sine[...]

    own_rows = slice(reach * R, (reach + 1) * R)
    for r in range(chunks):
        docs = doc_in[pl.ds(r * C, C)].astype(f32)
        side_v[r * C : (r + 1) * C, 0:ROPE] = rope_in[:, r * C : (r + 1) * C].astype(f32).T
        side_v[r * C : (r + 1) * C, ROPE:] = jnp.broadcast_to(docs[None, :], (C, C)).T[:, ROPE:]
    win[own_rows, latent_width:] = jnp.where(
        place < ROPE, turn(side_v[...]), side_v[...]
    ).astype(bf16)
    for k in range(1, reach + 1):
        start(halo_side_copy(k), me_sp + k < n_sp)


    halves = ((0, first), (first, second))

    def half_in(w, parity):
        at, size = halves[parity]
        if w >= 2:
            return down_in.at[pl.ds(at + (w - 2) * (size // 2), size // 2), :]
        return (gate_in, value_in)[w].at[:, pl.ds(at, size)]

    def half_slot(w, parity, owner):
        size = halves[parity][1]
        if w >= 2:
            return down_w.at[owner, pl.ds((w - 2) * (size // 2), size // 2), :]
        rows = pl.ds(pl.multiple_of(owner * gate_rows, 16), gate_rows)
        return (gate_w, value_w)[w].at[rows, pl.ds(0, size)]

    def by_parity(parity, act):
        for p in range(2):
            pl.when(parity == p)(functools.partial(act, p))

    pieces = ((0,), (1,), (2, 3))
    z_ids = [rc.ids(nz) for _ in range(4)]
    x_ids = [rc.ids(nz) for _ in range(4)]
    own_ids = [len(loads) + w for w in range(4)]

    def own_weight(w, p):
        return pltpu.make_async_copy(half_in(w, p), half_slot(w, p, me_sp), local_sems.at[own_ids[w]])

    def z_weight(w, d, p):
        return rc.make(z_ids[w] + d, half_in(w, p), half_slot(w, p, me_sp), z_sp[d], me_tp)

    def z_landed(w, d, p):
        return rc.make(z_ids[w] + d, half_in(w, p), half_slot(w, p, z_sp[d]), z_sp[d], me_tp)

    def x_weight(w, d, p):
        source = half_in(w, p) if d == 0 else half_slot(w, p, z_sp[d])
        return rc.make(x_ids[w] + d, source, half_slot(w, p, z_sp[d]), x_peer, me_tp)

    def x_landed(w, d, p):
        slot = half_slot(w, p, z_sp[d] + 1 - 2 * x)
        return rc.make(x_ids[w] + d, slot, slot, x_peer, me_tp)

    def send_z(w, which):
        for d in which:
            def act(p, d=d):
                for piece in pieces[w]:
                    z_weight(piece, d, p).start()
            by_parity((odd + d) % 2, act)

    def send_x(w, d):
        def act(p):
            for piece in pieces[w]:
                if d:
                    z_landed(piece, d, p).wait_recv()
                x_weight(piece, d, p).start()
        by_parity(odd, act)

    def all_here(w):
        def act(p):
            own_weight(w, p).wait()
            for d in range(nz):
                x_landed(w, d, p).wait_recv()
        by_parity(odd, act)

    for w in range(4):
        by_parity(odd, lambda p, w=w: own_weight(w, p).start())
    middle, near = list(range(2, nz)), [1]
    rightward = 1 - z // (nz // 2)

    inner = odd == rightward
    outer = jnp.logical_not(inner)

    def first_weights(right):
        for w in range(2):
            pl.when((1 - odd) == right)(lambda w=w: send_z(w, near))
        pl.when((rightward == right) & outer)(lambda: send_z(0, middle))
        if not right:
            def inner_weights(turned):
                send_z(0, middle)
                send_z(1, middle)
                send_z(2, middle[: len(middle) - turned])
            for turned in range(2):
                pl.when(inner & (rightward == turned))(functools.partial(inner_weights, turned))

    send_x(0, 0)
    send_x(1, 0)
    first_weights(0)

    @pl.when(odd == 1)
    def _():
        blank = first - second
        if blank:
            gate_w[:, second:] = jnp.zeros((gate_w.shape[0], blank), bf16)
            value_w[:, second:] = jnp.zeros((gate_w.shape[0], blank), bf16)
            down_w[:, second:, :] = jnp.zeros((n_sp, blank, down_cols), bf16)

    for conv, at in ((conv_g, 0), (conv_v, 8)):
        def pick_taps(p, conv=conv, at=at):
            first_unit, size = halves[p]
            taps[at : at + CONV, 0:size] = conv[:, first_unit : first_unit + size].astype(f32)
            if size < first:
                taps[at : at + CONV, size:] = jnp.zeros((CONV, first - size), f32)
        by_parity(odd, pick_taps)

    loads["win"].wait()
    loads["kup"].wait()
    loads["vup"].wait()

    def raise_rows(block):
        rows = pl.ds(pl.multiple_of(block * R, LANES), R)
        source = win[rows, :latent_width]
        keys[rows, :] = jnp.dot(source, kup[...], preferred_element_type=f32).astype(bf16)
        vals[rows, :] = jnp.dot(source, vup[...], preferred_element_type=f32).astype(bf16)

    with jax.named_scope("own_kv"):
        raise_rows(reach)
    loads["q"].wait()
    loads["t"].wait()
    for duo in range(heads // 2):
        cut = slice(duo * LANES, (duo + 1) * LANES)
        t_v[:, cut] = turn(t_v[:, cut]).astype(bf16)
    for k in range(1, reach + 1):
        @pl.when(me_sp >= k)
        def _(k=k):
            with jax.named_scope("halo_wait"):
                halo_copy(k).wait_recv()
                halo_side_copy(k).wait_recv()
            halo_pass(k, 0, me_tp, y_peer).start()
            halo_pass(k, 1, me_tp, c_peer).start()

        @pl.when(me_sp < k)
        def _(k=k):
            win[(reach - k) * R : (reach - k + 1) * R, :] = jnp.zeros((R, win.shape[1]), bf16)
        sent.append((halo_pass(k, 0, me_tp, y_peer), me_sp >= k))
        sent.append((halo_pass(k, 1, me_tp, c_peer), me_sp >= k))
    for k in range(1, reach + 1):
        @pl.when(me_sp >= k)
        def _(k=k):
            with jax.named_scope("halo_y_wait"):
                halo_pass(k, 0, y_peer, y_peer).wait_recv()
            halo_pass(k, 2, y_peer, c_peer).start()
        sent.append((halo_pass(k, 2, y_peer, c_peer), me_sp >= k))
    for k in range(1, reach + 1):
        @pl.when(me_sp >= k)
        def _(k=k):
            with jax.named_scope("halo_core_wait"):
                halo_pass(k, 1, c_peer, c_peer).wait_recv()
                halo_pass(k, 2, far_peer, c_peer).wait_recv()
    first_weights(1)
    send_x(2, 0)

    with jax.named_scope("kv"):
        @pl.loop(0, reach)
        def _(block):
            raise_rows(block)

    side = win[:, latent_width:]
    side_f = side.astype(f32)
    lane = lax.broadcasted_iota(jnp.int32, (window, LANES), 1)
    low = lane < LANES // 2
    ropes[0] = jnp.where(low, side_f, 0.0).astype(bf16)
    ropes[1] = jnp.where(low, 0.0, pltpu.roll(side_f, LANES // 2, 1)).astype(bf16)
    pick = (
        (lax.broadcasted_iota(jnp.int32, (8, LANES), 1) == LANES // 2)
        .astype(f32)
        .astype(bf16)
    )
    key_doc = lax.dot_general(pick, side, (((1,), (1,)), ((), ())), preferred_element_type=f32)[0:1]
    for r in range(chunks):
        at = slice(r * C, (r + 1) * C)
        own_doc = side_f[reach * R + r * C : reach * R + (r + 1) * C, LANES // 2 : LANES // 2 + 1]
        key_at = lax.broadcasted_iota(jnp.int32, (C, window), 1) - reach * R
        row_at = lax.broadcasted_iota(jnp.int32, (C, window), 0) + r * C
        allowed = (key_at <= row_at) & (key_at + me_sp * R >= 0) & (key_doc == own_doc)
        bias[at, :] = jnp.where(allowed, 0.0, masked_score)

    tail = side_f[reach * R - 8 :]
    valid_id = rc.ids()
    row_no = lax.broadcasted_iota(jnp.int32, (R, LANES), 0) + me_sp * R
    here = tail[8:]
    back_one = (pltpu.roll(tail, 1, 0)[8:] == here) & (row_no >= 1)
    back_two = (pltpu.roll(tail, 2, 0)[8:] == here) & (row_no >= 2)
    lanes = lax.broadcasted_iota(jnp.int32, (R, LANES), 1)
    valid[odd] = jnp.where(
        lanes < 3 * LANES // 4, back_two.astype(f32), back_one.astype(f32)
    ).astype(bf16)
    start(rc.make(valid_id, valid.at[odd], valid.at[odd], pair, me_tp))

    scale = (NOPE + ROPE) ** (-0.5) * log2_e

    def attend_chunk(r):
        at, seen = slice(r * C, (r + 1) * C), slice(r * C, r * C + span)

        @pl.loop(0, heads // 2)
        def _(duo):
            turned = t_v[at, pl.ds(pl.multiple_of(duo * LANES, LANES), LANES)]
            for e in range(2):
                head = pl.ds(pl.multiple_of((2 * duo + e) * LANES, LANES), LANES)
                queries = jnp.concatenate([q_v[at, head], turned], 1)
                seen_keys = jnp.concatenate([keys[seen, head], ropes[e, seen, :]], 1)
                scores = lax.dot_general(
                    queries, seen_keys, (((1,), (1,)), ((), ())), preferred_element_type=f32
                )
                scores = scores * scale + bias[at, seen]
                weights = jnp.exp2(scores - jnp.max(scores, -1, keepdims=True))
                total = jnp.sum(weights, -1, keepdims=True)
                mixed = jnp.dot(weights.astype(bf16), vals[seen, head], preferred_element_type=f32)
                att[at, head] = (mixed * (1.0 / total)).astype(bf16)

    core_ids, y_ids = rc.ids(2 * chunks), rc.ids(chunks)
    stat_ids = rc.ids(3 * chunks)
    stat_ids2 = rc.ids(3 * chunks)
    gather_ids = rc.ids(8 * chunks)

    def to_core(r, i):
        return rc.make(core_ids + 2 * r + i, core_out.at[r, i], core_in.at[r, i], me_sp, c_peer)

    def to_y(r):
        return rc.make(y_ids + r, y_out.at[r], y_in.at[r], me_sp, y_peer)

    def features(tp):
        return pl.ds(pl.multiple_of(tp * F, LANES), F)

    def project(r):
        rows = att[r * C : (r + 1) * C, :]
        for i, yy in enumerate((1 - y, y)):
            core_out[r, i] = jnp.dot(
                rows, proj[:, features(2 * yy + 1 - c)], preferred_element_type=f32
            ).astype(bf16)
            start(to_core(r, i))
        for i, yy in enumerate((1 - y, y)):
            keep[r, i] = jnp.dot(
                rows, proj[:, features(2 * yy + c)], preferred_element_type=f32
            ).astype(bf16)
        to_core(r, 0).wait_recv()
        y_out[r] = (keep[r, 0].astype(f32) + core_in[r, 0].astype(f32)).astype(bf16)
        start(to_y(r))

    def stat_copy(ids, own, landed, r, i):
        return rc.make(ids + 3 * r + i, own.at[r], landed.at[r, i], me_sp, (c_peer, y_peer, far_peer)[i])

    def send_stats(values, ids, own, landed, r):
        one = jnp.sum(values, -1, keepdims=True)
        two = jnp.sum(values * values, -1, keepdims=True)
        lane = lax.broadcasted_iota(jnp.int32, (C, LANES), 1)
        own[r] = jnp.where(lane % 8 < 4, one, two).T[0:8]
        for i in (1, 2, 0):
            start(stat_copy(ids, own, landed, r, i))

    def norm(values, ids, own, landed, r, gain):
        for i in range(3):
            stat_copy(ids, own, landed, r, i).wait_recv()
        total = (own[r] + landed[r, 0]) + (landed[r, 1] + landed[r, 2])
        total = jnp.concatenate([total] * (LANES // 8), 0).T
        row_mean = total[:, 0:1] / wide
        row_power = total[:, 4:5] / wide
        scaled = (values - row_mean) * lax.rsqrt(row_power - row_mean * row_mean + norm_eps)
        return scaled * gain[0][...].astype(f32)[None, :] + gain[1][...].astype(f32)[None, :]

    def mix_one(r):
        at = slice(r * C, (r + 1) * C)
        to_core(r, 1).wait_recv()
        to_y(r).wait_recv()
        mixed = residual_scale * resid[at, :].astype(f32) + (
            keep[r, 1].astype(f32) + core_in[r, 1].astype(f32) + y_in[r].astype(f32)
        )
        mix[at, :] = mixed
        send_stats(mixed, stat_ids, stat_own, stat_in, r)

    def gathered(r, kind, slot, tp, sp_to, tp_to):
        spot = rows_all.at[slot, pl.ds(r * C, C), features(tp)]
        return rc.make(gather_ids + 8 * r + kind, spot, spot, sp_to, tp_to)

    def to_pair(r, slot):
        return gathered(r, 0, slot, me_tp, pair, me_tp)

    def core_gather(r, kind, slot, tp):
        return gathered(r, kind, slot, tp, me_sp, c_peer)

    def y_gather(r, kind, slot, tp):
        return gathered(r, kind, slot, tp, me_sp, y_peer)

    def norm_one(r):
        at = slice(r * C, (r + 1) * C)
        rows_all[odd, at, features(me_tp)] = norm(
            mix[at, :], stat_ids, stat_own, stat_in, r, (gain1, bias1)
        ).astype(bf16)
        start(to_pair(r, odd))
        start(y_gather(r, 1, odd, me_tp))
        start(core_gather(r, 2, odd, me_tp))

    def pass_pair(r):
        to_pair(r, 1 - odd).wait_recv()
        start(y_gather(r, 3, 1 - odd, me_tp))
        start(core_gather(r, 4, 1 - odd, me_tp))

    def pass_y(r):
        for kind, got, slot in ((5, 1, odd), (6, 3, 1 - odd)):
            y_gather(r, got, slot, y_peer).wait_recv()
            start(core_gather(r, kind, slot, y_peer))

    def rows_here(r):
        core_gather(r, 2, odd, c_peer).wait_recv()
        core_gather(r, 4, 1 - odd, c_peer).wait_recv()
        core_gather(r, 5, odd, far_peer).wait_recv()
        core_gather(r, 6, 1 - odd, far_peer).wait_recv()

    def z_left(w, d):
        by_parity((odd + d) % 2, lambda p: z_weight(w, d, p).wait_send())

    def forward(w, which):
        for d in which:
            with jax.named_scope("fwd%d_%d" % (w, d)):
                send_x(w, d)

    def attend_step(r):
        with jax.named_scope("att"):
            attend_chunk(r)
        if r == 0:
            loads["proj"].wait()
            loads["resid"].wait()
        else:
            with jax.named_scope("mix"):
                mix_one(r - 1)
        with jax.named_scope("proj"):
            project(r)
        if r:
            with jax.named_scope("norm"):
                norm_one(r - 1)

    for r in range(chunks):
        attend_step(r)
        if r == 0:
            pl.when(outer)(lambda: send_z(1, middle))
            forward(0, near)
        elif r == 1:
            forward(1, near)
    forward(0, middle)
    with jax.named_scope("mix"):
        mix_one(chunks - 1)
    with jax.named_scope("norm"):
        norm_one(chunks - 1)
    send_z(2, near)
    forward(1, middle[:-1])
    with jax.named_scope("pass_pair"):
        for r in range(chunks):
            pass_pair(r)
    with jax.named_scope("pass_y"):
        for r in range(chunks):
            pass_y(r)
    forward(1, middle[-1:])
    with jax.named_scope("rows_here"):
        for r in range(chunks):
            rows_here(r)

    tile = 2 * LANES
    mid = first

    def up(weights, base):
        @pl.loop(0, 2)
        def _(slot):
            @pl.loop(0, first // tile)
            def _(j):
                cols = pl.multiple_of(j * tile, LANES)
                ext[slot, 8:, pl.ds(base + cols, tile)] = (
                    jnp.dot(rows_all[slot], weights[:, pl.ds(cols, tile)], preferred_element_type=f32)
                    .astype(bf16)
                    .astype(f32)
                )

    pl.when(outer & (rightward == 0))(lambda: send_z(2, middle))
    with jax.named_scope("wait_g"):
        all_here(0)
    with jax.named_scope("up_g"):
        up(gate_w, 0)
    pl.when(outer & (rightward == 1))(lambda: send_z(2, middle[:-1]))
    forward(2, near)
    with jax.named_scope("wait_v"):
        all_here(1)
    with jax.named_scope("up_v"):
        up(value_w, mid)

    tail_ids = rc.ids(2)

    def tail_copy(slot, to_slot, sp):
        return rc.make(
            tail_ids + to_slot, ext.at[slot, pl.ds(R, 8)], ext.at[to_slot, pl.ds(0, 8)], sp, me_tp
        )

    last_pair = z >= nz - 2
    start(tail_copy(0, 0, x_peer), x == 0)
    start(tail_copy(1, 1, x_peer), x == 0)
    start(tail_copy(0, 1, x_peer), x == 1)
    start(tail_copy(1, 0, me_sp + 3), (x == 1) & (z < nz - 2))
    pl.when(rightward == 1)(lambda: send_z(2, middle[-1:]))

    @pl.when((x == 0) & (z < 2))
    def _():
        ext[0, 0:8, :] = jnp.zeros((8, ext.shape[2]), f32)

    deep = 64

    def convolve(first_step, steps):
        @pl.loop(0, 2)
        def _(slot):
            @pl.loop(first_step, first_step + steps)
            def _(i):
                at = pl.multiple_of(i * deep, 16)
                marks = valid[slot, pl.ds(at, deep), :].astype(f32)
                two, one = marks[:, LANES // 2 : LANES // 2 + 1], marks[:, LANES - 1 : LANES]

                @pl.loop(0, first // tile)
                def _(j):
                    cols = pl.multiple_of(j * tile, LANES)

                    def mixing(base, tap):
                        rows = ext[slot, pl.ds(at, deep + 8), pl.ds(base + cols, tile)]
                        weight = taps[pl.ds(tap, 8), pl.ds(cols, tile)]
                        return (
                            weight[0:1] * (pltpu.roll(rows, 2, 0)[8:] * two)
                            + weight[1:2] * (pltpu.roll(rows, 1, 0)[8:] * one)
                            + weight[2:3] * rows[8:]
                        )

                    hid[slot, pl.ds(at, deep), pl.ds(cols, tile)] = (
                        mixing(mid, 8) * jax.nn.gelu(mixing(0, 0))
                    ).astype(bf16)

    rc.make(valid_id, valid.at[1 - odd], valid.at[1 - odd], pair, me_tp).wait_recv()
    with jax.named_scope("conv"):
        convolve(1, R // deep - 1)
    forward(2, middle[:-1])
    with jax.named_scope("tails"):
        @pl.when((x == 1) | (z >= 2))
        def _():
            tail_copy(0, 0, x_peer).wait_recv()
        tail_copy(1, 1, x_peer).wait_recv()
    with jax.named_scope("conv_first"):
        convolve(0, 1)

    core_ids2, z_ids2, y_ids2 = rc.ids(4), rc.ids(2 * chunks), rc.ids(chunks)
    per = F // down_cols
    half_z = (z // 2) % 2
    slots = (1 - odd, odd)

    def to_core2(d, s):
        f = d // 2
        return rc.make(
            core_ids2 + 2 * f + s, part2.at[d, s], core_in2.at[f, s], me_sp, c_peer
        )

    def to_pair2(f, r):
        at = pl.ds(r * C, C)
        return rc.make(z_ids2 + chunks * f + r, z_out2.at[f, at], z_in2.at[f, at], pair, me_tp)

    def to_y2(r):
        at = pl.ds(r * C, C)
        return rc.make(y_ids2 + r, y_out2.at[at], y_in2.at[at], me_sp, y_peer)

    def down_block(d):
        f, block = d // 2, flip(z, d)
        with jax.named_scope("wait_d%d" % d):
            def act(p):
                for piece in pieces[2]:
                    if d == 0:
                        own_weight(piece, p).wait()
                    x_landed(piece, d, p).wait_recv()
            by_parity(odd, act)
        with jax.named_scope("down"):
            for s in range(2):
                for j in range(per):
                    part2[d, s, :, j * down_cols : (j + 1) * down_cols] = jnp.dot(
                        hid[slots[s]], down_w[per * block + j], preferred_element_type=f32
                    ).astype(bf16)
                start(to_core2(d, s), block % 2 != c)

    def pair_block(d):
        f, block = d // 2, flip(z, d)

        @pl.when(block % 2 == c)
        def _():
            with jax.named_scope("core2_wait"):
                to_core2(d, 0).wait_recv()
            for r in range(chunks):
                at = slice(r * C, (r + 1) * C)
                z_out2[f, at, :] = (
                    part2[d, 0, at, :].astype(f32) + core_in2[f, 0, at, :].astype(f32)
                ).astype(bf16)
                to_pair2(f, r).start()
            with jax.named_scope("core2_wait"):
                to_core2(d, 1).wait_recv()

    def mine_of(f):
        return 2 * f + (odd + c) % 2

    def pass_down(f):
        yy = half_z if f == 0 else 1 - half_z
        for r in range(chunks):
            at = slice(r * C, (r + 1) * C)
            with jax.named_scope("z2_wait"):
                to_pair2(f, r).wait_recv()
            sent.append((to_pair2(f, r), None))

            @pl.when(y != yy)
            def _():
                y_out2[at, :] = (
                    part2[mine_of(f), 1, pl.ds(r * C, C), :].astype(f32)
                    + core_in2[f, 1, at, :].astype(f32)
                    + z_in2[f, at, :].astype(f32)
                ).astype(bf16)
                to_y2(r).start()

    down_block(0)
    down_block(1)
    pair_block(0)
    pair_block(1)
    forward(2, middle[-1:])
    down_block(2)
    pair_block(2)
    down_block(3)
    pair_block(3)
    pass_down(0)
    pass_down(1)
    mine = (y + half_z) % 2
    for r in range(chunks):
        at = slice(r * C, (r + 1) * C)
        rows = pl.ds(r * C, C)
        with jax.named_scope("y2_wait"):
            to_y2(r).wait_recv()
        sent.append((to_y2(r), None))
        mixed = residual_scale * rows_all[odd, at, features(me_tp)].astype(f32) + (
            part2[mine_of(mine), 1, rows, :].astype(f32)
            + core_in2[mine, 1, rows, :].astype(f32)
            + z_in2[mine, rows, :].astype(f32)
            + y_in2[at, :].astype(f32)
        )
        mix[at, :] = mixed
        send_stats(mixed, stat_ids2, stat_own2, stat_in2, r)
    with jax.named_scope("norm2"):
        for r in range(chunks):
            at = slice(r * C, (r + 1) * C)
            out_ref[at, :] = norm(mix[at, :], stat_ids2, stat_own2, stat_in2, r, (gain2, bias2)).astype(bf16)

    for copy, when in sent:
        if when is None:
            copy.wait_send()
        else:
            pl.when(when)(copy.wait_send)
    for w in range(4):
        for d in range(nz):
            if d:
                z_left(w, d)
            by_parity(odd, lambda p, d=d, w=w: x_weight(w, d, p).wait_send())
    assert rc.count <= REMOTE, rc.count


def fused(
    residual, query_nope, query_rope, latent, rope_key, doc_ids, key_up, value_up, out_proj,
    norm1_gain, norm1_bias, ffn_gate, ffn_value, conv_gate, conv_value, ffn_down, norm2_gain, norm2_bias,
):
    n_sp, n_tp = lax.axis_size("sp"), lax.axis_size("tp")
    R, F = residual.shape
    heads = query_nope.shape[1] // NOPE
    units = ffn_gate.shape[1]
    first = -(-units // (2 * LANES)) * LANES
    second = units - first
    window = (REACH + 1) * R
    chunks = R // LANES
    f32, bf16 = jnp.float32, jnp.bfloat16
    half = ROPE // 2
    place = np.arange(LANES) % half
    frequencies = jnp.asarray((rope_base_freq ** (-2.0 * place / ROPE))[None, :], f32)
    hbm = pl.BlockSpec(memory_space=pl.ANY)
    vmem = pl.BlockSpec(memory_space=pltpu.VMEM)
    sizes = (n_sp, n_tp, R, REACH, heads, n_tp * F, first, second)

    def v(*shape, dtype=bf16):
        return pltpu.VMEM(shape, dtype)

    C = LANES
    return pl.pallas_call(
        functools.partial(layer_kernel, sizes),
        in_specs=[hbm] * 7 + [vmem] * 9 + [hbm] * 3,
        out_specs=vmem,
        out_shape=jax.ShapeDtypeStruct((R, F), bf16),
        scratch_shapes=[
            v(R, LANES, dtype=f32), v(R, LANES, dtype=f32), v(R, LANES, dtype=f32), v(16, first, dtype=f32), v(window, latent.shape[1] + LANES), v(R, heads * NOPE), v(R, heads * ROPE),
            v(*key_up.shape), v(*value_up.shape), v(*out_proj.shape), v(R, F),
            v(window, heads * NOPE), v(window, heads * VDIM), v(2, window, LANES),
            v(R, window, dtype=f32), v(R, heads * VDIM),
            v(chunks, 2, C, F), v(chunks, 2, C, F), v(chunks, 2, C, F), v(chunks, C, F), v(chunks, C, F),
            v(R, F, dtype=f32), v(chunks, 8, LANES, dtype=f32), v(chunks, 3, 8, LANES, dtype=f32),
            v(2, R, LANES),
            v(2, R, n_tp * F), v(n_sp * ffn_gate.shape[0], first), v(n_sp * ffn_gate.shape[0], first),
            v(n_sp, first, ffn_down.shape[1]), v(2, R + 8, 2 * first, dtype=f32), v(2, R, first),
            v(4, 2, R, F), v(2, 2, R, F), v(R, F), v(R, F), v(2, R, F), v(2, R, F),
            v(chunks, 8, LANES, dtype=f32), v(chunks, 3, 8, LANES, dtype=f32),
            pltpu.SemaphoreType.DMA((REMOTE,)), pltpu.SemaphoreType.DMA((REMOTE,)),
            pltpu.SemaphoreType.DMA((LOCAL,)),
        ],
        compiler_params=pltpu.CompilerParams(
            collective_id=0, has_side_effects=True, vmem_limit_bytes=64 * 1024 * 1024 - 65536
        ),
    )(
        query_nope, query_rope, latent, key_up, value_up, out_proj, residual, rope_key.T, doc_ids, frequencies,
        norm1_gain, norm1_bias, norm2_gain, norm2_bias,
        conv_gate, conv_value, ffn_gate, ffn_value, ffn_down,
    )


def local(*arrays):
    rows, features = arrays[0].shape
    down_cols = arrays[15].shape[1]
    n_sp, n_tp = lax.axis_size("sp"), lax.axis_size("tp")
    paired = n_sp // 2
    fits = n_tp == 4 and paired == n_tp
    tiled = rows % LANES == 0 and down_cols % LANES == 0 and features == 2 * down_cols
    return (fused if fits and tiled else plain)(*arrays)


def solution(mesh):
    placed = (
        P("sp", "tp"),
        P("sp", "tp"),
        P("sp", "tp"),
        P("sp", None),
        P("sp", None),
        P("sp"),
        P(None, "tp"),
        P(None, "tp"),
        P("tp", None),
        P("tp"),
        P("tp"),
        P("sp", "tp"),
        P("sp", "tp"),
        P(None, "tp"),
        P(None, "tp"),
        P("tp", "sp"),
        P("tp"),
        P("tp"),
    )
    return jax.shard_map(
        local, mesh=mesh, in_specs=placed, out_specs=P("sp", "tp"), check_vma=False
    )
```

```python
import functools

import jax
import jax.numpy as jnp
import numpy as np
from jax import lax
from jax.experimental import pallas as pl
from jax.experimental.pallas import tpu as pltpu
from jax.sharding import PartitionSpec as P

D = 2048
NOPE = 128
ROPE = 64
VDIM = 128
CONV = 3
REACH = 3


norm_eps = 1e-05
residual_scale = 8.0**0.25
rope_base_freq = 10000.0
masked_score = -1e30


def passed_along(value, axis, by):
    count = lax.axis_size(axis)
    pairs = [(i, i + by) for i in range(count) if 0 <= i + by < count]
    return lax.ppermute(value, axis, pairs)


def tables(positions):
    frequencies = 1.0 / rope_base_freq ** (jnp.arange(0, ROPE, 2, dtype=jnp.float32) / ROPE)
    angles = positions.astype(jnp.float32)[:, None] * frequencies[None, :]
    return (jnp.cos(angles), jnp.sin(angles))


def rotate(vectors, cosine, sine_table):
    half_width = vectors.shape[-1] // 2
    front_half = vectors[..., :half_width]
    back_half = vectors[..., half_width:]
    return jnp.concatenate(
        [
            front_half * cosine - back_half * sine_table,
            front_half * sine_table + back_half * cosine,
        ],
        axis=-1,
    )


def ring_blocks(block, axis):
    count = lax.axis_size(axis)
    order = list(range(0, count, 2)) + list(range(1, count, 2))[::-1]
    place = [order.index(i) for i in range(count)]
    me = lax.axis_index(axis)
    found = [(me, block)]
    ahead = count // 2
    for turn, steps in ((1, ahead), (-1, count - 1 - ahead)):
        pairs = [(order[p], order[(p + turn) % count]) for p in range(count)]
        moving = block
        for step in range(1, steps + 1):
            moving = lax.ppermute(moving, axis, pairs)
            owners = [order[(place[i] - turn * step) % count] for i in range(count)]
            found.append((jnp.asarray(owners, jnp.int32)[me], moving))
    return found


def attend_kernel(chunk, reach_rows, scale, q_ref, turned_ref, k_ref, rope_ref, v_ref, bias_ref, out_ref):
    rows = q_ref.shape[0]
    span = chunk + reach_rows
    rope_rows = rope_ref[...]
    for head in range(q_ref.shape[1] // NOPE):
        nope = slice(head * NOPE, (head + 1) * NOPE)
        rope = slice(head * ROPE, (head + 1) * ROPE)
        queries = jnp.concatenate([q_ref[:, nope], turned_ref[:, rope]], 1)
        keys = jnp.concatenate([k_ref[:, nope], rope_rows], 1)
        for start in range(0, rows, chunk):
            cut = slice(start, start + chunk)
            seen = slice(start, start + span)
            scores = lax.dot_general(
                queries[cut], keys[seen], (((1,), (1,)), ((), ())), preferred_element_type=jnp.float32
            )
            scores = scores * scale + bias_ref[cut, seen]
            weights = jnp.exp(scores - jnp.max(scores, -1, keepdims=True))
            weights = weights * (1.0 / jnp.sum(weights, -1, keepdims=True))
            out_ref[cut, nope] = jnp.dot(
                weights.astype(jnp.bfloat16), v_ref[seen, nope], preferred_element_type=jnp.float32
            ).astype(jnp.bfloat16)


def attend(queries, turned, keys, rope_rows, values, bias, scale):
    rows, width = queries.shape
    window = keys.shape[0]
    chunk = 128 if rows % 128 == 0 else rows
    pair = 2
    wide = pair * NOPE
    heads = width // NOPE
    return pl.pallas_call(
        functools.partial(attend_kernel, chunk, window - rows, scale),
        grid=(heads // pair,),
        in_specs=[
            pl.BlockSpec((rows, wide), lambda i: (0, i)),
            pl.BlockSpec((rows, pair * ROPE), lambda i: (0, i)),
            pl.BlockSpec((window, wide), lambda i: (0, i)),
            pl.BlockSpec((window, ROPE), lambda i: (0, 0)),
            pl.BlockSpec((window, pair * VDIM), lambda i: (0, i)),
            pl.BlockSpec((rows, window), lambda i: (0, 0)),
        ],
        out_specs=pl.BlockSpec((rows, pair * VDIM), lambda i: (0, i)),
        out_shape=jax.ShapeDtypeStruct((rows, heads * VDIM), jnp.bfloat16),
        compiler_params=pltpu.CompilerParams(vmem_limit_bytes=40 * 1024 * 1024),
        cost_estimate=pl.CostEstimate(
            flops=16 * rows * window * heads * (NOPE + ROPE + VDIM),
            bytes_accessed=2 * (4 * rows * width + 2 * window * width),
            transcendentals=rows * window * heads,
        ),
    )(queries, turned, keys, rope_rows, values, bias)


def scatter_sum(terms, axis):
    count = lax.axis_size(axis)
    width = terms.shape[1] // count
    parts = jnp.stack([terms[:, i * width : (i + 1) * width] for i in range(count)])
    got = lax.all_to_all(parts.astype(jnp.bfloat16), axis, 0, 0)
    return jnp.sum(got.astype(jnp.float32), 0)


def finish(mixed, totals, gain_row, bias_row):
    row_mean = totals[0][:, None] / D
    row_power = totals[1][:, None] / D
    return (mixed - row_mean) * lax.rsqrt(
        row_power - row_mean * row_mean + norm_eps
    ) * gain_row.astype(jnp.float32) + bias_row.astype(jnp.float32)


def plain(
    residual,
    query_nope,
    query_rope,
    latent,
    rope_key,
    doc_ids,
    key_up,
    value_up,
    out_proj,
    norm1_gain,
    norm1_bias,
    ffn_gate,
    ffn_value,
    conv_gate,
    conv_value,
    ffn_down,
    norm2_gain,
    norm2_bias,
):
    row_count = latent.shape[0]
    head_count = query_nope.shape[1] // NOPE
    local_units = ffn_gate.shape[1]
    rim_rows = CONV - 1
    whole_gate = lax.all_gather(ffn_gate, "sp", axis=0, tiled=True)
    whole_value = lax.all_gather(ffn_value, "sp", axis=0, tiled=True)
    offset = lax.axis_index("sp") * row_count
    positions = offset + jnp.arange(row_count, dtype=jnp.int32)
    cosine, sine_table = tables(positions)
    turned_key = rotate(rope_key.astype(jnp.float32), cosine, sine_table).astype(jnp.bfloat16)
    turned_query = rotate(
        query_rope.astype(jnp.float32).reshape(row_count, head_count, ROPE),
        cosine[:, None],
        sine_table[:, None],
    ).astype(jnp.bfloat16)
    latent_width = latent.shape[1]
    packed = jnp.concatenate(
        [
            latent,
            turned_key,
            jnp.broadcast_to(doc_ids.astype(jnp.bfloat16)[:, None], (row_count, ROPE)),
        ],
        1,
    )
    parts = [passed_along(packed, "sp", shift_step) for shift_step in range(REACH, 0, -1)]
    pieces = jnp.concatenate(parts + [packed], 0)
    win_latent = pieces[:, :latent_width]
    win_key = pieces[:, latent_width : latent_width + ROPE]
    win_doc = pieces[:, latent_width + ROPE].astype(jnp.int32)
    down_blocks = ring_blocks(ffn_down, "sp")
    key_rows = jnp.dot(win_latent, key_up, preferred_element_type=jnp.float32).astype(jnp.bfloat16)
    values = jnp.dot(win_latent, value_up, preferred_element_type=jnp.float32).astype(jnp.bfloat16)
    window = key_rows.shape[0]
    key_pos = offset - REACH * row_count + jnp.arange(window, dtype=jnp.int32)
    allowed = (
        (key_pos[None, :] <= positions[:, None])
        & (key_pos[None, :] >= 0)
        & (win_doc[None, :] == doc_ids[:, None])
    )
    scale = (NOPE + ROPE) ** (-0.5)
    bias = jnp.where(allowed, 0.0, masked_score).astype(jnp.float32)
    attended = attend(
        query_nope,
        turned_query.reshape(row_count, head_count * ROPE),
        key_rows,
        win_key,
        values,
        bias,
        scale,
    )
    head_terms = jnp.dot(attended, out_proj, preferred_element_type=jnp.float32)
    projected = scatter_sum(head_terms, "tp")
    mixed_one = residual_scale * residual.astype(jnp.float32) + projected
    totals_one = lax.psum((jnp.sum(mixed_one, 1), jnp.sum(mixed_one * mixed_one, 1)), "tp")
    normed = finish(mixed_one, totals_one, norm1_gain, norm1_bias).astype(jnp.bfloat16)
    half = row_count // 2
    full_rows = jnp.concatenate(
        [
            lax.all_gather(normed[:half], "tp", axis=1, tiled=True),
            lax.all_gather(normed[half:], "tp", axis=1, tiled=True),
        ],
        0,
    )
    gate_sum = jnp.dot(full_rows, whole_gate, preferred_element_type=jnp.float32)
    value_sum = jnp.dot(full_rows, whole_value, preferred_element_type=jnp.float32)
    gate_pre = gate_sum.astype(jnp.bfloat16)
    value_pre = value_sum.astype(jnp.bfloat16)
    tail_gate, tail_value, tail_doc = passed_along(
        (
            gate_pre[row_count - rim_rows :],
            value_pre[row_count - rim_rows :],
            doc_ids[row_count - rim_rows :],
        ),
        "sp",
        1,
    )
    ext_gate = jnp.concatenate([tail_gate, gate_pre], 0)
    ext_value = jnp.concatenate([tail_value, value_pre], 0)
    ext_doc = jnp.concatenate([tail_doc, doc_ids], 0)
    gate_mix = jnp.zeros((row_count, local_units), jnp.float32)
    value_mix = jnp.zeros((row_count, local_units), jnp.float32)
    for tap_index in range(CONV):
        valid_tap = (
            (ext_doc[tap_index : tap_index + row_count] == doc_ids)
            & (positions - rim_rows + tap_index >= 0)
        ).astype(jnp.float32)[:, None]
        gate_mix = (
            gate_mix
            + conv_gate[tap_index].astype(jnp.float32)
            * ext_gate[tap_index : tap_index + row_count].astype(jnp.float32)
            * valid_tap
        )
        value_mix = (
            value_mix
            + conv_value[tap_index].astype(jnp.float32)
            * ext_value[tap_index : tap_index + row_count].astype(jnp.float32)
            * valid_tap
        )
    hidden = (value_mix * jax.nn.gelu(gate_mix)).astype(jnp.bfloat16)
    sp_count = lax.axis_size("sp")
    tp_count = lax.axis_size("tp")
    block_width = ffn_down.shape[1]
    unit_terms = jnp.zeros((sp_count, row_count, block_width), jnp.bfloat16)
    for owner, block in down_blocks:
        term = jnp.dot(hidden, block, preferred_element_type=jnp.float32).astype(jnp.bfloat16)
        unit_terms = lax.dynamic_update_slice(unit_terms, term[None], (owner, 0, 0))
    share = sp_count // tp_count
    got = lax.all_to_all(
        unit_terms.reshape(tp_count, share, row_count, block_width), "tp", 0, 0
    )
    ffn_blocks = jnp.sum(got.astype(jnp.float32), 0)
    ffn_out = jnp.concatenate([ffn_blocks[i] for i in range(share)], 1)
    mixed_two = residual_scale * normed.astype(jnp.float32) + ffn_out
    totals_two = lax.psum((jnp.sum(mixed_two, 1), jnp.sum(mixed_two * mixed_two, 1)), "tp")
    return finish(mixed_two, totals_two, norm2_gain, norm2_bias).astype(jnp.bfloat16)


LANES = 128
MESH = pl.DeviceIdType.MESH
log2_e = 1.4426950408889634


class Copies:
    def __init__(self, send_sems, recv_sems):
        self.send_sems, self.recv_sems = send_sems, recv_sems
        self.count = 0

    def ids(self, number=1):
        first = self.count
        self.count += number
        return first

    def make(self, index, source, target, sp, tp):
        return pltpu.make_async_remote_copy(
            src_ref=source,
            dst_ref=target,
            send_sem=self.send_sems.at[index],
            recv_sem=self.recv_sems.at[index],
            device_id={"sp": sp, "tp": tp},
            device_id_type=MESH,
        )


REMOTE = 160
LOCAL = 16


def flip(value, bits):
    for bit in range(bits.bit_length()):
        step = 1 << bit
        if bits & step:
            value = value + step - 2 * step * ((value // step) % 2)
    return value


def layer_kernel(
    sizes,
    q_in, t_in, latent_in, kup_in, vup_in, proj_in, resid_in, rope_in, doc_in, frequencies,
    gain1, bias1, gain2, bias2, conv_g, conv_v, gate_in, value_in, down_in,
    out_ref,
    cosine, sine, side_v, taps, win, q_v, t_v, kup, vup, proj, resid, keys, vals, ropes, bias, att,
    core_out, core_in, keep, y_out, y_in, mix, stat_own, stat_in, valid,
    rows_all, gate_w, value_w, down_w, ext, hid,
    part2, core_in2, y_out2, y_in2, z_out2, z_in2, stat_own2, stat_in2,
    send_sems, recv_sems, local_sems,
):
    n_sp, n_tp, R, reach, heads, wide, first, second = sizes
    C = LANES
    F = resid.shape[1]
    chunks = R // C
    window = (reach + 1) * R
    span = C + reach * R
    latent_width = kup.shape[0]
    gate_rows = gate_in.shape[0]
    down_cols = down_in.shape[1]
    bf16, f32 = jnp.bfloat16, jnp.float32
    me_sp, me_tp = lax.axis_index("sp"), lax.axis_index("tp")
    x, z = me_sp % 2, me_sp // 2
    odd = z % 2
    y, c = me_tp // 2, me_tp % 2
    x_peer = me_sp + 1 - 2 * x
    c_peer = me_tp + 1 - 2 * c
    y_peer = me_tp + 2 - 4 * y
    far_peer = 3 - me_tp
    nz = n_sp // 2
    z_sp = [2 * flip(z, d) + x for d in range(nz)]
    pair = z_sp[1]
    rc = Copies(send_sems, recv_sems)
    sent = []

    def start(copy, when=None):
        if when is None:
            copy.start()
        else:
            pl.when(when)(copy.start)
        sent.append((copy, when))

    barrier = pltpu.get_barrier_semaphore()
    for i in range(n_sp):
        for j in range(n_tp):
            if i or j:
                pl.semaphore_signal(
                    barrier, inc=1,
                    device_id={"sp": (me_sp + i) % n_sp, "tp": (me_tp + j) % n_tp},
                    device_id_type=MESH,
                )

    loads = {}

    def load(name, source, target):
        loads[name] = pltpu.make_async_copy(source, target, local_sems.at[len(loads)])
        loads[name].start()

    load("win", latent_in, win.at[pl.ds(reach * R, R), pl.ds(0, latent_width)])
    load("kup", kup_in, kup)
    load("vup", vup_in, vup)
    load("q", q_in, q_v)
    load("t", t_in, t_v)
    load("proj", proj_in, proj)
    load("resid", resid_in, resid)

    with jax.named_scope("barrier"):
        pl.semaphore_wait(barrier, n_sp * n_tp - 1)

    part = R // n_tp
    halo = rc.ids(reach)
    halo_ids = rc.ids(3 * reach)

    def quarter(k, tp):
        return win.at[pl.ds(pl.multiple_of((reach - k) * R + tp * part, 16), part)]

    halo_side = rc.ids(reach)
    own_part = pl.multiple_of(me_tp * part, 16)

    def halo_copy(k):
        return rc.make(
            halo + k - 1, latent_in.at[pl.ds(own_part, part)],
            quarter(k, me_tp).at[:, pl.ds(0, latent_width)], me_sp + k, me_tp,
        )

    def halo_side_copy(k):
        lanes = pl.ds(latent_width, LANES)
        return rc.make(
            halo_side + k - 1, win.at[pl.ds(reach * R + own_part, part), lanes],
            quarter(k, me_tp).at[:, lanes], me_sp + k, me_tp,
        )

    def halo_pass(k, kind, tp, tp_to):
        rows = quarter(k, tp)
        return rc.make(halo_ids + 3 * (k - 1) + kind, rows, rows, me_sp, tp_to)

    for k in range(1, reach + 1):
        start(halo_copy(k), me_sp + k < n_sp)

    place = lax.broadcasted_iota(jnp.int32, (R, LANES), 1)
    front = place % ROPE < ROPE // 2
    row_at = lax.broadcasted_iota(jnp.int32, (R, LANES), 0) + me_sp * R
    angles = row_at.astype(f32) * frequencies[...]
    cosine[...] = jnp.cos(angles)
    sine[...] = jnp.where(front, -1.0, 1.0) * jnp.sin(angles)

    def turn(vectors):
        vectors = vectors.astype(f32)
        swapped = jnp.where(
            front,
            pltpu.roll(vectors, LANES - ROPE // 2, 1),
            pltpu.roll(vectors, ROPE // 2, 1),
        )
        return vectors * cosine[...] + swapped * sine[...]

    own_rows = slice(reach * R, (reach + 1) * R)
    for r in range(chunks):
        docs = doc_in[pl.ds(r * C, C)].astype(f32)
        side_v[r * C : (r + 1) * C, 0:ROPE] = rope_in[:, r * C : (r + 1) * C].astype(f32).T
        side_v[r * C : (r + 1) * C, ROPE:] = jnp.broadcast_to(docs[None, :], (C, C)).T[:, ROPE:]
    win[own_rows, latent_width:] = jnp.where(
        place < ROPE, turn(side_v[...]), side_v[...]
    ).astype(bf16)
    for k in range(1, reach + 1):
        start(halo_side_copy(k), me_sp + k < n_sp)


    halves = ((0, first), (first, second))

    def half_in(w, parity):
        at, size = halves[parity]
        if w >= 2:
            return down_in.at[pl.ds(at + (w - 2) * (size // 2), size // 2), :]
        return (gate_in, value_in)[w].at[:, pl.ds(at, size)]

    def half_slot(w, parity, owner):
        size = halves[parity][1]
        if w >= 2:
            return down_w.at[owner, pl.ds((w - 2) * (size // 2), size // 2), :]
        rows = pl.ds(pl.multiple_of(owner * gate_rows, 16), gate_rows)
        return (gate_w, value_w)[w].at[rows, pl.ds(0, size)]

    def by_parity(parity, act):
        for p in range(2):
            pl.when(parity == p)(functools.partial(act, p))

    pieces = ((0,), (1,), (2, 3))
    z_ids = [rc.ids(nz) for _ in range(4)]
    x_ids = [rc.ids(nz) for _ in range(4)]
    own_ids = [len(loads) + w for w in range(4)]

    def own_weight(w, p):
        return pltpu.make_async_copy(half_in(w, p), half_slot(w, p, me_sp), local_sems.at[own_ids[w]])

    def z_weight(w, d, p):
        return rc.make(z_ids[w] + d, half_in(w, p), half_slot(w, p, me_sp), z_sp[d], me_tp)

    def z_landed(w, d, p):
        return rc.make(z_ids[w] + d, half_in(w, p), half_slot(w, p, z_sp[d]), z_sp[d], me_tp)

    def x_weight(w, d, p):
        source = half_in(w, p) if d == 0 else half_slot(w, p, z_sp[d])
        return rc.make(x_ids[w] + d, source, half_slot(w, p, z_sp[d]), x_peer, me_tp)

    def x_landed(w, d, p):
        slot = half_slot(w, p, z_sp[d] + 1 - 2 * x)
        return rc.make(x_ids[w] + d, slot, slot, x_peer, me_tp)

    def send_z(w, which):
        for d in which:
            def act(p, d=d):
                for piece in pieces[w]:
                    z_weight(piece, d, p).start()
            by_parity((odd + d) % 2, act)

    def send_x(w, d):
        def act(p):
            for piece in pieces[w]:
                if d:
                    z_landed(piece, d, p).wait_recv()
                x_weight(piece, d, p).start()
        by_parity(odd, act)

    def all_here(w):
        def act(p):
            own_weight(w, p).wait()
            for d in range(nz):
                x_landed(w, d, p).wait_recv()
        by_parity(odd, act)

    for w in range(4):
        by_parity(odd, lambda p, w=w: own_weight(w, p).start())
    middle, near = list(range(2, nz)), [1]
    rightward = 1 - z // (nz // 2)

    inner = odd == rightward
    outer = jnp.logical_not(inner)

    def first_weights(right):
        for w in range(2):
            pl.when((1 - odd) == right)(lambda w=w: send_z(w, near))
        pl.when((rightward == right) & outer)(lambda: send_z(0, middle))
        if not right:
            def inner_weights(turned):
                send_z(0, middle)
                send_z(1, middle)
                send_z(2, middle[: len(middle) - turned])
            for turned in range(2):
                held = rightward * x
                pl.when(inner & (held == turned))(functools.partial(inner_weights, turned))

    send_x(0, 0)
    send_x(1, 0)
    first_weights(0)

    @pl.when(odd == 1)
    def _():
        blank = first - second
        if blank:
            gate_w[:, second:] = jnp.zeros((gate_w.shape[0], blank), bf16)
            value_w[:, second:] = jnp.zeros((gate_w.shape[0], blank), bf16)
            down_w[:, second:, :] = jnp.zeros((n_sp, blank, down_cols), bf16)

    for conv, at in ((conv_g, 0), (conv_v, 8)):
        def pick_taps(p, conv=conv, at=at):
            first_unit, size = halves[p]
            taps[at : at + CONV, 0:size] = conv[:, first_unit : first_unit + size].astype(f32)
            if size < first:
                taps[at : at + CONV, size:] = jnp.zeros((CONV, first - size), f32)
        by_parity(odd, pick_taps)

    loads["win"].wait()
    loads["kup"].wait()
    loads["vup"].wait()

    def raise_rows(block):
        rows = pl.ds(pl.multiple_of(block * R, LANES), R)
        source = win[rows, :latent_width]
        keys[rows, :] = jnp.dot(source, kup[...], preferred_element_type=f32).astype(bf16)
        vals[rows, :] = jnp.dot(source, vup[...], preferred_element_type=f32).astype(bf16)

    with jax.named_scope("own_kv"):
        raise_rows(reach)
    loads["q"].wait()
    loads["t"].wait()
    for duo in range(heads // 2):
        cut = slice(duo * LANES, (duo + 1) * LANES)
        t_v[:, cut] = turn(t_v[:, cut]).astype(bf16)
    for k in range(1, reach + 1):
        @pl.when(me_sp >= k)
        def _(k=k):
            with jax.named_scope("halo_wait"):
                halo_copy(k).wait_recv()
                halo_side_copy(k).wait_recv()
            halo_pass(k, 0, me_tp, y_peer).start()
            halo_pass(k, 1, me_tp, c_peer).start()

        @pl.when(me_sp < k)
        def _(k=k):
            win[(reach - k) * R : (reach - k + 1) * R, :] = jnp.zeros((R, win.shape[1]), bf16)
        sent.append((halo_pass(k, 0, me_tp, y_peer), me_sp >= k))
        sent.append((halo_pass(k, 1, me_tp, c_peer), me_sp >= k))
    for k in range(1, reach + 1):
        @pl.when(me_sp >= k)
        def _(k=k):
            with jax.named_scope("halo_y_wait"):
                halo_pass(k, 0, y_peer, y_peer).wait_recv()
            halo_pass(k, 2, y_peer, c_peer).start()
        sent.append((halo_pass(k, 2, y_peer, c_peer), me_sp >= k))
    for k in range(1, reach + 1):
        @pl.when(me_sp >= k)
        def _(k=k):
            with jax.named_scope("halo_core_wait"):
                halo_pass(k, 1, c_peer, c_peer).wait_recv()
                halo_pass(k, 2, far_peer, c_peer).wait_recv()
    first_weights(1)
    send_x(2, 0)

    with jax.named_scope("kv"):
        @pl.loop(0, reach)
        def _(block):
            raise_rows(block)

    side = win[:, latent_width:]
    side_f = side.astype(f32)
    lane = lax.broadcasted_iota(jnp.int32, (window, LANES), 1)
    low = lane < LANES // 2
    ropes[0] = jnp.where(low, side_f, 0.0).astype(bf16)
    ropes[1] = jnp.where(low, 0.0, pltpu.roll(side_f, LANES // 2, 1)).astype(bf16)
    pick = (
        (lax.broadcasted_iota(jnp.int32, (8, LANES), 1) == LANES // 2)
        .astype(f32)
        .astype(bf16)
    )
    key_doc = lax.dot_general(pick, side, (((1,), (1,)), ((), ())), preferred_element_type=f32)[0:1]
    for r in range(chunks):
        at = slice(r * C, (r + 1) * C)
        own_doc = side_f[reach * R + r * C : reach * R + (r + 1) * C, LANES // 2 : LANES // 2 + 1]
        key_at = lax.broadcasted_iota(jnp.int32, (C, window), 1) - reach * R
        row_at = lax.broadcasted_iota(jnp.int32, (C, window), 0) + r * C
        allowed = (key_at <= row_at) & (key_at + me_sp * R >= 0) & (key_doc == own_doc)
        bias[at, :] = jnp.where(allowed, 0.0, masked_score)

    tail = side_f[reach * R - 8 :]
    valid_id = rc.ids()
    row_no = lax.broadcasted_iota(jnp.int32, (R, LANES), 0) + me_sp * R
    here = tail[8:]
    back_one = (pltpu.roll(tail, 1, 0)[8:] == here) & (row_no >= 1)
    back_two = (pltpu.roll(tail, 2, 0)[8:] == here) & (row_no >= 2)
    lanes = lax.broadcasted_iota(jnp.int32, (R, LANES), 1)
    valid[odd] = jnp.where(
        lanes < 3 * LANES // 4, back_two.astype(f32), back_one.astype(f32)
    ).astype(bf16)
    start(rc.make(valid_id, valid.at[odd], valid.at[odd], pair, me_tp))

    scale = (NOPE + ROPE) ** (-0.5) * log2_e

    def attend_chunk(r):
        at, seen = slice(r * C, (r + 1) * C), slice(r * C, r * C + span)

        @pl.loop(0, heads // 2)
        def _(duo):
            turned = t_v[at, pl.ds(pl.multiple_of(duo * LANES, LANES), LANES)]
            for e in range(2):
                head = pl.ds(pl.multiple_of((2 * duo + e) * LANES, LANES), LANES)
                queries = jnp.concatenate([q_v[at, head], turned], 1)
                seen_keys = jnp.concatenate([keys[seen, head], ropes[e, seen, :]], 1)
                scores = lax.dot_general(
                    queries, seen_keys, (((1,), (1,)), ((), ())), preferred_element_type=f32
                )
                scores = scores * scale + bias[at, seen]
                weights = jnp.exp2(scores - jnp.max(scores, -1, keepdims=True))
                total = jnp.sum(weights, -1, keepdims=True)
                mixed = jnp.dot(weights.astype(bf16), vals[seen, head], preferred_element_type=f32)
                att[at, head] = (mixed * (1.0 / total)).astype(bf16)

    core_ids, y_ids = rc.ids(2 * chunks), rc.ids(chunks)
    stat_ids = rc.ids(3 * chunks)
    stat_ids2 = rc.ids(3 * chunks)
    gather_ids = rc.ids(8 * chunks)

    def to_core(r, i):
        return rc.make(core_ids + 2 * r + i, core_out.at[r, i], core_in.at[r, i], me_sp, c_peer)

    def to_y(r):
        return rc.make(y_ids + r, y_out.at[r], y_in.at[r], me_sp, y_peer)

    def features(tp):
        return pl.ds(pl.multiple_of(tp * F, LANES), F)

    def project(r):
        rows = att[r * C : (r + 1) * C, :]
        for i, yy in enumerate((1 - y, y)):
            core_out[r, i] = jnp.dot(
                rows, proj[:, features(2 * yy + 1 - c)], preferred_element_type=f32
            ).astype(bf16)
            start(to_core(r, i))
        for i, yy in enumerate((1 - y, y)):
            keep[r, i] = jnp.dot(
                rows, proj[:, features(2 * yy + c)], preferred_element_type=f32
            ).astype(bf16)
        to_core(r, 0).wait_recv()
        y_out[r] = (keep[r, 0].astype(f32) + core_in[r, 0].astype(f32)).astype(bf16)
        start(to_y(r))

    def stat_copy(ids, own, landed, r, i):
        return rc.make(ids + 3 * r + i, own.at[r], landed.at[r, i], me_sp, (c_peer, y_peer, far_peer)[i])

    def send_stats(values, ids, own, landed, r):
        one = jnp.sum(values, -1, keepdims=True)
        two = jnp.sum(values * values, -1, keepdims=True)
        lane = lax.broadcasted_iota(jnp.int32, (C, LANES), 1)
        own[r] = jnp.where(lane % 8 < 4, one, two).T[0:8]
        for i in (1, 2, 0):
            start(stat_copy(ids, own, landed, r, i))

    def norm(values, ids, own, landed, r, gain):
        for i in range(3):
            stat_copy(ids, own, landed, r, i).wait_recv()
        total = (own[r] + landed[r, 0]) + (landed[r, 1] + landed[r, 2])
        total = jnp.concatenate([total] * (LANES // 8), 0).T
        row_mean = total[:, 0:1] / wide
        row_power = total[:, 4:5] / wide
        scaled = (values - row_mean) * lax.rsqrt(row_power - row_mean * row_mean + norm_eps)
        return scaled * gain[0][...].astype(f32)[None, :] + gain[1][...].astype(f32)[None, :]

    def mix_one(r):
        at = slice(r * C, (r + 1) * C)
        to_core(r, 1).wait_recv()
        to_y(r).wait_recv()
        mixed = residual_scale * resid[at, :].astype(f32) + (
            keep[r, 1].astype(f32) + core_in[r, 1].astype(f32) + y_in[r].astype(f32)
        )
        mix[at, :] = mixed
        send_stats(mixed, stat_ids, stat_own, stat_in, r)

    def gathered(r, kind, slot, tp, sp_to, tp_to):
        spot = rows_all.at[slot, pl.ds(r * C, C), features(tp)]
        return rc.make(gather_ids + 8 * r + kind, spot, spot, sp_to, tp_to)

    def to_pair(r, slot):
        return gathered(r, 0, slot, me_tp, pair, me_tp)

    def core_gather(r, kind, slot, tp):
        return gathered(r, kind, slot, tp, me_sp, c_peer)

    def y_gather(r, kind, slot, tp):
        return gathered(r, kind, slot, tp, me_sp, y_peer)

    def norm_one(r):
        at = slice(r * C, (r + 1) * C)
        rows_all[odd, at, features(me_tp)] = norm(
            mix[at, :], stat_ids, stat_own, stat_in, r, (gain1, bias1)
        ).astype(bf16)
        start(to_pair(r, odd))
        start(y_gather(r, 1, odd, me_tp))
        start(core_gather(r, 2, odd, me_tp))

    def pass_pair(r):
        to_pair(r, 1 - odd).wait_recv()
        start(y_gather(r, 3, 1 - odd, me_tp))
        start(core_gather(r, 4, 1 - odd, me_tp))

    def pass_y(r):
        for kind, got, slot in ((5, 1, odd), (6, 3, 1 - odd)):
            y_gather(r, got, slot, y_peer).wait_recv()
            start(core_gather(r, kind, slot, y_peer))

    def rows_here(r):
        core_gather(r, 2, odd, c_peer).wait_recv()
        core_gather(r, 4, 1 - odd, c_peer).wait_recv()
        core_gather(r, 5, odd, far_peer).wait_recv()
        core_gather(r, 6, 1 - odd, far_peer).wait_recv()

    def z_left(w, d):
        by_parity((odd + d) % 2, lambda p: z_weight(w, d, p).wait_send())

    def forward(w, which):
        for d in which:
            with jax.named_scope("fwd%d_%d" % (w, d)):
                send_x(w, d)

    def attend_step(r):
        with jax.named_scope("att"):
            attend_chunk(r)
        if r == 0:
            loads["proj"].wait()
            loads["resid"].wait()
        else:
            with jax.named_scope("mix"):
                mix_one(r - 1)
        with jax.named_scope("proj"):
            project(r)
        if r:
            with jax.named_scope("norm"):
                norm_one(r - 1)

    for r in range(chunks):
        attend_step(r)
        if r == 0:
            pl.when(outer)(lambda: send_z(1, middle))
            forward(0, near)
        elif r == 1:
            forward(1, near)
    forward(0, middle)
    with jax.named_scope("mix"):
        mix_one(chunks - 1)
    with jax.named_scope("norm"):
        norm_one(chunks - 1)
    send_z(2, near)
    forward(1, middle[:-1])
    with jax.named_scope("pass_pair"):
        for r in range(chunks):
            pass_pair(r)
    with jax.named_scope("pass_y"):
        for r in range(chunks):
            pass_y(r)
    forward(1, middle[-1:])
    with jax.named_scope("rows_here"):
        for r in range(chunks):
            rows_here(r)

    tile = 2 * LANES
    mid = first

    def up(weights, base):
        @pl.loop(0, 2)
        def _(slot):
            @pl.loop(0, first // tile)
            def _(j):
                cols = pl.multiple_of(j * tile, LANES)
                ext[slot, 8:, pl.ds(base + cols, tile)] = (
                    jnp.dot(rows_all[slot], weights[:, pl.ds(cols, tile)], preferred_element_type=f32)
                    .astype(bf16)
                    .astype(f32)
                )

    pl.when(outer & (rightward == 0))(lambda: send_z(2, middle))
    with jax.named_scope("wait_g"):
        all_here(0)
    with jax.named_scope("up_g"):
        up(gate_w, 0)
    pl.when(outer & (rightward == 1))(lambda: send_z(2, middle[:-1]))
    forward(2, near)
    with jax.named_scope("wait_v"):
        all_here(1)
    with jax.named_scope("up_v"):
        up(value_w, mid)

    tail_ids = rc.ids(2)

    def tail_copy(slot, to_slot, sp):
        return rc.make(
            tail_ids + to_slot, ext.at[slot, pl.ds(R, 8)], ext.at[to_slot, pl.ds(0, 8)], sp, me_tp
        )

    last_pair = z >= nz - 2
    start(tail_copy(0, 0, x_peer), x == 0)
    start(tail_copy(1, 1, x_peer), x == 0)
    start(tail_copy(0, 1, x_peer), x == 1)
    start(tail_copy(1, 0, me_sp + 3), (x == 1) & (z < nz - 2))
    pl.when((rightward == 1) & (outer | (x == 1)))(lambda: send_z(2, middle[-1:]))

    @pl.when((x == 0) & (z < 2))
    def _():
        ext[0, 0:8, :] = jnp.zeros((8, ext.shape[2]), f32)

    deep = 64

    def convolve(first_step, steps):
        @pl.loop(0, 2)
        def _(slot):
            @pl.loop(first_step, first_step + steps)
            def _(i):
                at = pl.multiple_of(i * deep, 16)
                marks = valid[slot, pl.ds(at, deep), :].astype(f32)
                two, one = marks[:, LANES // 2 : LANES // 2 + 1], marks[:, LANES - 1 : LANES]

                @pl.loop(0, first // tile)
                def _(j):
                    cols = pl.multiple_of(j * tile, LANES)

                    def mixing(base, tap):
                        rows = ext[slot, pl.ds(at, deep + 8), pl.ds(base + cols, tile)]
                        weight = taps[pl.ds(tap, 8), pl.ds(cols, tile)]
                        return (
                            weight[0:1] * (pltpu.roll(rows, 2, 0)[8:] * two)
                            + weight[1:2] * (pltpu.roll(rows, 1, 0)[8:] * one)
                            + weight[2:3] * rows[8:]
                        )

                    hid[slot, pl.ds(at, deep), pl.ds(cols, tile)] = (
                        mixing(mid, 8) * jax.nn.gelu(mixing(0, 0))
                    ).astype(bf16)

    rc.make(valid_id, valid.at[1 - odd], valid.at[1 - odd], pair, me_tp).wait_recv()
    with jax.named_scope("conv"):
        convolve(1, R // deep - 1)
    forward(2, middle[:-1])
    with jax.named_scope("tails"):
        @pl.when((x == 1) | (z >= 2))
        def _():
            tail_copy(0, 0, x_peer).wait_recv()
        tail_copy(1, 1, x_peer).wait_recv()
    with jax.named_scope("conv_first"):
        convolve(0, 1)

    core_ids2, z_ids2, y_ids2 = rc.ids(4), rc.ids(2 * chunks), rc.ids(chunks)
    per = F // down_cols
    half_z = (z // 2) % 2
    slots = (1 - odd, odd)

    def to_core2(d, s):
        f = d // 2
        return rc.make(
            core_ids2 + 2 * f + s, part2.at[d, s], core_in2.at[f, s], me_sp, c_peer
        )

    def to_pair2(f, r):
        at = pl.ds(r * C, C)
        return rc.make(z_ids2 + chunks * f + r, z_out2.at[f, at], z_in2.at[f, at], pair, me_tp)

    def to_y2(r):
        at = pl.ds(r * C, C)
        return rc.make(y_ids2 + r, y_out2.at[at], y_in2.at[at], me_sp, y_peer)

    def down_block(d):
        f, block = d // 2, flip(z, d)
        with jax.named_scope("wait_d%d" % d):
            def act(p):
                for piece in pieces[2]:
                    if d == 0:
                        own_weight(piece, p).wait()
                    x_landed(piece, d, p).wait_recv()
            by_parity(odd, act)
        with jax.named_scope("down"):
            for s in range(2):
                for j in range(per):
                    part2[d, s, :, j * down_cols : (j + 1) * down_cols] = jnp.dot(
                        hid[slots[s]], down_w[per * block + j], preferred_element_type=f32
                    ).astype(bf16)
                start(to_core2(d, s), block % 2 != c)

    def pair_block(d):
        f, block = d // 2, flip(z, d)

        @pl.when(block % 2 == c)
        def _():
            with jax.named_scope("core2_wait"):
                to_core2(d, 0).wait_recv()
            for r in range(chunks):
                at = slice(r * C, (r + 1) * C)
                z_out2[f, at, :] = (
                    part2[d, 0, at, :].astype(f32) + core_in2[f, 0, at, :].astype(f32)
                ).astype(bf16)
                to_pair2(f, r).start()
            with jax.named_scope("core2_wait"):
                to_core2(d, 1).wait_recv()

    def mine_of(f):
        return 2 * f + (odd + c) % 2

    def pass_down(f):
        yy = half_z if f == 0 else 1 - half_z
        for r in range(chunks):
            at = slice(r * C, (r + 1) * C)
            with jax.named_scope("z2_wait"):
                to_pair2(f, r).wait_recv()
            sent.append((to_pair2(f, r), None))

            @pl.when(y != yy)
            def _():
                y_out2[at, :] = (
                    part2[mine_of(f), 1, pl.ds(r * C, C), :].astype(f32)
                    + core_in2[f, 1, at, :].astype(f32)
                    + z_in2[f, at, :].astype(f32)
                ).astype(bf16)
                to_y2(r).start()

    down_block(0)
    down_block(1)
    pair_block(0)
    pair_block(1)
    forward(2, middle[-1:])
    down_block(2)
    pair_block(2)
    down_block(3)
    pair_block(3)
    pass_down(0)
    pass_down(1)
    mine = (y + half_z) % 2
    for r in range(chunks):
        at = slice(r * C, (r + 1) * C)
        rows = pl.ds(r * C, C)
        with jax.named_scope("y2_wait"):
            to_y2(r).wait_recv()
        sent.append((to_y2(r), None))
        mixed = residual_scale * rows_all[odd, at, features(me_tp)].astype(f32) + (
            part2[mine_of(mine), 1, rows, :].astype(f32)
            + core_in2[mine, 1, rows, :].astype(f32)
            + z_in2[mine, rows, :].astype(f32)
            + y_in2[at, :].astype(f32)
        )
        mix[at, :] = mixed
        send_stats(mixed, stat_ids2, stat_own2, stat_in2, r)
    with jax.named_scope("norm2"):
        for r in range(chunks):
            at = slice(r * C, (r + 1) * C)
            out_ref[at, :] = norm(mix[at, :], stat_ids2, stat_own2, stat_in2, r, (gain2, bias2)).astype(bf16)

    for copy, when in sent:
        if when is None:
            copy.wait_send()
        else:
            pl.when(when)(copy.wait_send)
    for w in range(4):
        for d in range(nz):
            if d:
                z_left(w, d)
            by_parity(odd, lambda p, d=d, w=w: x_weight(w, d, p).wait_send())
    assert rc.count <= REMOTE, rc.count


def fused(
    residual, query_nope, query_rope, latent, rope_key, doc_ids, key_up, value_up, out_proj,
    norm1_gain, norm1_bias, ffn_gate, ffn_value, conv_gate, conv_value, ffn_down, norm2_gain, norm2_bias,
):
    n_sp, n_tp = lax.axis_size("sp"), lax.axis_size("tp")
    R, F = residual.shape
    heads = query_nope.shape[1] // NOPE
    units = ffn_gate.shape[1]
    first = -(-units // (2 * LANES)) * LANES
    second = units - first
    window = (REACH + 1) * R
    chunks = R // LANES
    f32, bf16 = jnp.float32, jnp.bfloat16
    half = ROPE // 2
    place = np.arange(LANES) % half
    frequencies = jnp.asarray((rope_base_freq ** (-2.0 * place / ROPE))[None, :], f32)
    hbm = pl.BlockSpec(memory_space=pl.ANY)
    vmem = pl.BlockSpec(memory_space=pltpu.VMEM)
    sizes = (n_sp, n_tp, R, REACH, heads, n_tp * F, first, second)

    def v(*shape, dtype=bf16):
        return pltpu.VMEM(shape, dtype)

    C = LANES
    return pl.pallas_call(
        functools.partial(layer_kernel, sizes),
        in_specs=[hbm] * 7 + [vmem] * 9 + [hbm] * 3,
        out_specs=vmem,
        out_shape=jax.ShapeDtypeStruct((R, F), bf16),
        scratch_shapes=[
            v(R, LANES, dtype=f32), v(R, LANES, dtype=f32), v(R, LANES, dtype=f32), v(16, first, dtype=f32), v(window, latent.shape[1] + LANES), v(R, heads * NOPE), v(R, heads * ROPE),
            v(*key_up.shape), v(*value_up.shape), v(*out_proj.shape), v(R, F),
            v(window, heads * NOPE), v(window, heads * VDIM), v(2, window, LANES),
            v(R, window, dtype=f32), v(R, heads * VDIM),
            v(chunks, 2, C, F), v(chunks, 2, C, F), v(chunks, 2, C, F), v(chunks, C, F), v(chunks, C, F),
            v(R, F, dtype=f32), v(chunks, 8, LANES, dtype=f32), v(chunks, 3, 8, LANES, dtype=f32),
            v(2, R, LANES),
            v(2, R, n_tp * F), v(n_sp * ffn_gate.shape[0], first), v(n_sp * ffn_gate.shape[0], first),
            v(n_sp, first, ffn_down.shape[1]), v(2, R + 8, 2 * first, dtype=f32), v(2, R, first),
            v(4, 2, R, F), v(2, 2, R, F), v(R, F), v(R, F), v(2, R, F), v(2, R, F),
            v(chunks, 8, LANES, dtype=f32), v(chunks, 3, 8, LANES, dtype=f32),
            pltpu.SemaphoreType.DMA((REMOTE,)), pltpu.SemaphoreType.DMA((REMOTE,)),
            pltpu.SemaphoreType.DMA((LOCAL,)),
        ],
        compiler_params=pltpu.CompilerParams(
            collective_id=0, has_side_effects=True, vmem_limit_bytes=64 * 1024 * 1024 - 65536
        ),
    )(
        query_nope, query_rope, latent, key_up, value_up, out_proj, residual, rope_key.T, doc_ids, frequencies,
        norm1_gain, norm1_bias, norm2_gain, norm2_bias,
        conv_gate, conv_value, ffn_gate, ffn_value, ffn_down,
    )


def local(*arrays):
    rows, features = arrays[0].shape
    down_cols = arrays[15].shape[1]
    n_sp, n_tp = lax.axis_size("sp"), lax.axis_size("tp")
    paired = n_sp // 2
    fits = n_tp == 4 and paired == n_tp
    tiled = rows % LANES == 0 and down_cols % LANES == 0 and features == 2 * down_cols
    return (fused if fits and tiled else plain)(*arrays)


def solution(mesh):
    placed = (
        P("sp", "tp"),
        P("sp", "tp"),
        P("sp", "tp"),
        P("sp", None),
        P("sp", None),
        P("sp"),
        P(None, "tp"),
        P(None, "tp"),
        P("tp", None),
        P("tp"),
        P("tp"),
        P("sp", "tp"),
        P("sp", "tp"),
        P(None, "tp"),
        P(None, "tp"),
        P("tp", "sp"),
        P("tp"),
        P("tp"),
    )
    return jax.shard_map(
        local, mesh=mesh, in_specs=placed, out_specs=P("sp", "tp"), check_vma=False
    )
```
